32 devices in a mesh: grp: 2 (over y), tp: 4 (over z), dp: 4 (over x, core).
Axes of the slice: x: 2, y: 2, z: 4, core: 2. Of those that a mesh axis runs over, the one named last changes fastest.
Arguments:
- hidden_in: bfloat16 [96, 4096], P(('grp', 'tp'), 'dp'), parts along dimension 0, may hold values from -40 to 40
- input_norm_gain: float32 [2, 4096], P(None, 'dp'), may hold values from 0.1 to 1.9
- w_query: bfloat16 [2, 4096, 2048], P(None, 'dp', 'tp'), may hold values from -0.09375 to 0.09375
- w_key: bfloat16 [2, 4096, 2048], P(None, 'dp', 'tp'), may hold values from -0.09375 to 0.09375
- w_decay: bfloat16 [2, 4096, 2048], P(None, 'dp', 'tp'), may hold values from -0.375 to 0.375
- w_value: bfloat16 [2, 4096, 4096], P(None, 'dp', 'tp'), may hold values from -0.09375 to 0.09375
- w_gate: bfloat16 [2, 4096, 4096], P(None, 'dp', 'tp'), may hold values from -0.09375 to 0.09375
- out_gain: float32 [2, 4096], P(None, 'tp'), may hold values from 0.1 to 1.9
- w_out: bfloat16 [2, 4096, 4096], P(None, 'tp', 'dp'), may hold values from -0.09375 to 0.09375
- decay_offset: float32 [2, 96, 2048], P(None, ('grp', 'dp'), 'tp'), parts along dimension 1, may hold values from -0.7 to 0
- state: float32 [2, 96, 32, 64, 128], P(None, ('grp', 'dp'), 'tp'), parts along dimension 1, may hold values from -3 to 3
Outputs:
- hidden_out: bfloat16 [96, 4096], P(('grp', 'tp'), 'dp'), parts along dimension 0
- new_state: float32 [2, 96, 32, 64, 128], P(None, ('grp', 'dp'), 'tp'), parts along dimension 1
The draws below stay inside these ranges and needn't reach their ends.
There are 2 independent parts, one for each index of `grp`. The reference program is written for one: setup_inputs(seed, part) draws one part's arguments, and reference() takes and returns one part's arrays. A program takes and returns all parts, laid end to end along the dimension named above; an argument that names none is the same for every part. Nothing has to cross between parts.
All inputs are finite; a program needn't handle non-finite values.
Results may differ from the reference program's by a relative error of at most 0.017.
Values may be sent and summed in bfloat16 or wider, within the bound.
A program may use at most 64 MiB of HBM per device.

```python
import jax
import jax.numpy as jnp
from jax import lax

D = 4096
HEADS = 32
HEAD_KEY = 64
VALUE_CHANNELS = 128
LAYERS = 2
BATCH = 48
KEY_W = 2048
VAL_W = 4096
N_DP = 4


def draw_hidden_in(key, part):
    base_key, column_key, row_key = jax.random.split(key, 3)
    column = jnp.arange(D, dtype=jnp.float32) / (D - 1)
    column_scale = jnp.exp(jnp.log(3.0) * column + jax.random.uniform(column_key, (D,), jnp.float32, -0.5, 0.5))
    values = jnp.clip(jax.random.normal(base_key, (BATCH, D), jnp.float32), -4.0, 4.0)
    row_scale = jnp.exp(jax.random.uniform(row_key, (BATCH, 1), jnp.float32, -0.7, 0.7))
    return (values * row_scale * column_scale[None, :]).astype(jnp.bfloat16)


def level_of(own_key, extent, shards, low, largest):
    level = 1.0
    for position, blocks in shards:
        steps = jax.random.uniform(jax.random.fold_in(jax.random.fold_in(own_key, 6), position), (blocks,), jnp.float32, low / len(shards), largest / len(shards))
        level = level * jnp.repeat(jnp.exp(steps), extent[position] // blocks).reshape((-1,) + (1,) * (len(extent) - 1 - position))
    return level


def bell_draw(stream_key, dims, scale, bound, cuts=(), kind=jnp.bfloat16):
    result = scale * jax.random.normal(stream_key, dims, jnp.float32)
    if cuts:
        result = result * level_of(stream_key, dims, cuts, -0.22, 0.18)
    return jnp.clip(result, -bound, bound).astype(kind)


def setup_inputs(seed: int = 0, part: int = 0) -> dict:
    arg_keys = jax.random.split(jax.random.key(seed), 12)
    part_keys = jax.random.split(jax.random.fold_in(arg_keys[11], part), 12)
    hidden_in = draw_hidden_in(jax.random.fold_in(jax.random.fold_in(arg_keys[11], part), 71), part)
    input_norm_gain = jnp.clip(1.0 + 0.18 * jax.random.normal(arg_keys[1], (LAYERS, D), jnp.float32), 0.1, 1.9)
    w_query = bell_draw(arg_keys[2], (LAYERS, D, KEY_W), D ** -0.5, 0.09375, ((1, 4), (2, 4)))
    w_key = bell_draw(arg_keys[3], (LAYERS, D, KEY_W), D ** -0.5, 0.09375, ((1, 4), (2, 4)))
    w_decay = bell_draw(arg_keys[4], (LAYERS, D, KEY_W), (D // 16) ** -0.5, 0.375, ((1, 4), (2, 4)))
    w_value = bell_draw(arg_keys[5], (LAYERS, D, VAL_W), D ** -0.5, 0.09375, ((1, 4), (2, 4)))
    w_gate = bell_draw(arg_keys[6], (LAYERS, D, VAL_W), D ** -0.5, 0.09375, ((1, 4), (2, 4)))
    out_gain = jnp.clip(1.0 + 0.18 * jax.random.normal(arg_keys[7], (LAYERS, VAL_W), jnp.float32), 0.1, 1.9)
    w_out = bell_draw(arg_keys[8], (LAYERS, VAL_W, D), VAL_W ** -0.5, 0.09375, ((1, 4), (2, 4)))
    decay_offset = jnp.clip(-0.7 + 0.7 * jax.random.uniform(part_keys[9], (LAYERS, BATCH, KEY_W), jnp.float32) ** level_of(part_keys[9], (LAYERS, BATCH, KEY_W), ((1, 4), (2, 4)), -0.2, 0.2), -0.7, 0.0)
    state = bell_draw(part_keys[10], (LAYERS, BATCH, HEADS, HEAD_KEY, VALUE_CHANNELS), 0.5, 3.0, ((1, 4), (2, 4)), jnp.float32)
    return dict(hidden_in=hidden_in, input_norm_gain=input_norm_gain, w_query=w_query, w_key=w_key, w_decay=w_decay, w_value=w_value, w_gate=w_gate, out_gain=out_gain, w_out=w_out, decay_offset=decay_offset, state=state)


epsilon = 1e-06
softness_factor = 16.0

def reference(hidden_in, input_norm_gain, w_query, w_key, w_decay, w_value, w_gate, out_gain, w_out, decay_offset, state):
    hidden = hidden_in
    states = []
    for index_of_block in range(LAYERS):
        widened = hidden.astype(jnp.float32)
        squares = lax.optimization_barrier(jnp.sum(widened * widened, axis=1))
        scaled_query = (widened * input_norm_gain[index_of_block][None, :]).astype(jnp.bfloat16)
        groups = scaled_query.astype(jnp.float32).reshape(BATCH, N_DP, D // N_DP)
        pieces = []
        for matrix in (w_query, w_key, w_decay, w_value, w_gate):
            blocks = matrix[index_of_block].astype(jnp.float32).reshape(N_DP, D // N_DP, matrix.shape[2])
            partial_value = jnp.einsum('bnr,nrc->nbc', groups, blocks, precision=lax.Precision.HIGHEST)
            rounded = lax.optimization_barrier(partial_value.astype(jnp.bfloat16))
            pieces.append(lax.optimization_barrier(jnp.sum(rounded.astype(jnp.float32), axis=0)))
        inverse = lax.rsqrt(squares / D + epsilon)[:, None]
        query_rows = (pieces[0] * inverse).reshape(BATCH, HEADS, HEAD_KEY)
        key_rows = (pieces[1] * inverse).reshape(BATCH, HEADS, HEAD_KEY) * HEAD_KEY ** (-0.5)
        decay_logits = pieces[2] * inverse
        value_rows = (pieces[3] * inverse).reshape(BATCH, HEADS, VALUE_CHANNELS)
        gate_rows = (pieces[4] * inverse).reshape(BATCH, HEADS, VALUE_CHANNELS)
        decay_logarithm = jax.nn.log_sigmoid(decay_logits) / softness_factor + decay_offset[index_of_block]
        decay_rate = jnp.exp(decay_logarithm).reshape(BATCH, HEADS, HEAD_KEY)
        fresh = decay_rate[:, :, :, None] * state[index_of_block] + key_rows[:, :, :, None] * value_rows[:, :, None, :]
        readout = lax.optimization_barrier(jnp.sum(query_rows[:, :, :, None] * fresh, axis=2))
        normed = readout * lax.rsqrt(lax.optimization_barrier(jnp.mean(readout * readout, axis=2, keepdims=True)) + epsilon)
        normed = normed * out_gain[index_of_block].reshape(HEADS, VALUE_CHANNELS)[None]
        gated_out = (normed * jax.nn.silu(gate_rows)).reshape(BATCH, VAL_W).astype(jnp.bfloat16)
        mixed = jnp.dot(gated_out, w_out[index_of_block], preferred_element_type=jnp.float32)
        hidden = (widened + mixed).astype(jnp.bfloat16)
        states.append(fresh)
    return (hidden, jnp.stack(states))
```

```python
import functools

import jax
import jax.numpy as jnp
from jax import lax
from jax.experimental import pallas as pl
from jax.experimental.pallas import tpu as pltpu
from jax.sharding import PartitionSpec as P

EPSILON = 1e-06
SOFTNESS = 16.0
F32 = jnp.float32
BF16 = jnp.bfloat16


def swap(tiles):
    return pltpu.roll(tiles, 4, 0)


def first_half(shape):
    return lax.broadcasted_iota(jnp.int32, shape, 0) < 4


def fold(upper, lower, second):
    even = jnp.concatenate([lower[:, :128], lower[:, 256:384]], axis=1)
    odd = jnp.concatenate([lower[:, 128:256], lower[:, 384:]], axis=1)
    top = first_half(even.shape)
    first_form = jnp.where(top, even, swap(odd))
    second_form = jnp.where(top, swap(even), odd)
    if isinstance(second, int):
        folded = second_form if second else first_form
    else:
        folded = jnp.where(second == 1, second_form, first_form)
    return jnp.concatenate(
        [
            jnp.concatenate([upper[:, :256], folded[:, :128]], axis=1),
            jnp.concatenate([upper[:, 256:], folded[:, 128:]], axis=1),
        ],
        axis=0,
    )


def unfold(block):
    upper = jnp.concatenate([block[:8, :256], block[8:, :256]], axis=1)
    left, right = block[:8, 256:], block[8:, 256:]
    lower = jnp.concatenate([left, swap(left), right, swap(right)], axis=1)
    return upper, lower


def unfold_rows(block):
    upper, lower = unfold(block)
    return jnp.concatenate([upper, jnp.where(first_half(lower.shape), lower, 0.0)], axis=0)


def stack_groups(blocks):
    rows = []
    for core in range(2):
        one, two = blocks[core], blocks[2 + core]
        upper_one = jnp.concatenate([one[:8, :256], one[8:, :256]], axis=1)
        upper_two = jnp.concatenate([two[:8, :256], two[8:, :256]], axis=1)
        lower = []
        for half in range(2):
            a, b = one[8 * half : 8 * half + 8, 256:], two[8 * half : 8 * half + 8, 256:]
            top = first_half(a.shape)
            lower += [jnp.where(top, a, swap(b)), jnp.where(top, swap(a), b)]
        rows += [upper_one, upper_two, jnp.concatenate(lower, axis=1)]
    return jnp.concatenate(rows, axis=0)


def group_of(stacked, s):
    chip, core = divmod(s, 2)
    base = 24 * core
    upper = stacked[base + 8 * chip : base + 8 * chip + 8]
    return fold(upper, stacked[base + 16 : base + 24], chip)


def block_kernel(
    n_tp, n_dp, d_model, head_key, value_channels, piece,
    hidden_hbm, gain_hbm, out_gain_hbm, offset_hbm,
    wq_hbm, wk_hbm, wd_hbm, wv_hbm, wg_hbm, wo_hbm, state_hbm,
    hidden_out_ref, new_state_ref,
    hidden, gain, out_gain, offset, proj, wo, state,
    gathered, product, partial, near, own, cross, far,
    sq_part, sq_near, sq_cross, sq_far,
    expand, values, fresh_columns, readout,
    gated_all, mix_part, mix_send, mix_recv,
    small_sem, proj_sem, wo_sem, state_sem,
    gather_recv, near_recv, far_recv, sq_recv, gated_recv, mix_recv_sem, send_sem,
):
    layers, rows, heads = state.shape[0], state.shape[1], state.shape[2]
    pad = 16
    mix_pieces = mix_send.shape[1]
    pieces = proj.shape[1]
    key_cols = heads * head_key
    value_cols = heads * value_channels
    halves = value_cols // piece
    half_heads = heads // halves
    tp = lax.axis_index("tp")
    dp = lax.axis_index("dp")
    chip, core = dp // 2, lax.rem(dp, 2)
    other_core = 1 - core
    other_chip = 1 - chip
    partner = 2 * chip + other_core
    across = 2 * other_chip + core
    mesh_id = pl.DeviceIdType.MESH

    barrier = pltpu.get_barrier_semaphore()
    for j in range(1, n_tp):
        pl.semaphore_signal(
            barrier, inc=1, device_id={"tp": lax.rem(tp + j, n_tp)}, device_id_type=mesh_id
        )
    for j in range(1, n_dp):
        pl.semaphore_signal(
            barrier, inc=1, device_id={"dp": lax.rem(dp + j, n_dp)}, device_id_type=mesh_id
        )

    small = [
        pltpu.make_async_copy(source, target, small_sem.at[index])
        for index, (source, target) in enumerate(
            ((hidden_hbm, hidden), (gain_hbm, gain), (out_gain_hbm, out_gain), (offset_hbm, offset))
        )
    ]

    def load_proj(layer, i):
        if i < 3:
            source = (wq_hbm, wk_hbm, wd_hbm)[i].at[layer]
        else:
            half, which = divmod(i - 3, 2)
            source = (wv_hbm, wg_hbm)[which].at[layer, :, pl.ds(half * piece, piece)]
        return pltpu.make_async_copy(source, proj.at[layer, i], proj_sem.at[layer, i])

    def load_wo(layer):
        return pltpu.make_async_copy(wo_hbm.at[layer], wo.at[layer], wo_sem.at[layer])

    def load_state(layer):
        return pltpu.make_async_copy(state_hbm.at[layer], state.at[layer], state_sem.at[layer])

    for copy in small:
        copy.start()

    row_of = lax.broadcasted_iota(jnp.int32, (4 * pad, 2 * value_channels), 0)
    lane_of = lax.broadcasted_iota(jnp.int32, (4 * pad, 2 * value_channels), 1)
    for second in range(2):
        for pair in range(rows // 2):
            picked = pair * 2 + lane_of // value_channels
            inside = (row_of >= second * 2 * pad) & (row_of < (second + 1) * 2 * pad)
            hit = inside & (lax.rem(row_of, pad) == picked)
            expand[second, pair] = jnp.where(hit, 1.0, 0.0).astype(BF16)

    for copy in small:
        copy.wait()
    for layer in range(layers):
        for i in range(pieces):
            load_proj(layer, i).start()
        load_state(layer).start()
        load_wo(layer).start()

    upper = hidden[pl.ds(0, 8), :].astype(F32)
    lower = hidden[pl.ds(8, 4), :].astype(F32)
    lower = jnp.concatenate([lower, lower], axis=0)
    for p in range(mix_pieces):
        span = slice(p * piece, (p + 1) * piece)
        gathered[0, p, tp] = fold(upper[:, span], lower[:, span], 0).astype(BF16)
    pl.semaphore_wait(barrier, n_tp + n_dp - 2)

    def remote(src, dst, send, recv, axis, target):
        copy = pltpu.make_async_remote_copy(
            src_ref=src, dst_ref=dst, send_sem=send, recv_sem=recv,
            device_id={axis: target}, device_id_type=mesh_id,
        )
        copy.start()

    def await_bytes(ref, sem):
        pltpu.make_async_copy(ref, ref, sem).wait()

    above = tp // (n_tp // 2)

    def tp_step(j):
        return j + above * (n_tp - 2 * j)

    def send_features(layer, p):
        for j in range(n_tp - 1, 0, -1):
            remote(
                gathered.at[layer, p, tp], gathered.at[layer, p, tp],
                send_sem.at[layer, 0], gather_recv.at[layer, p],
                "tp", lax.rem(tp + tp_step(j), n_tp),
            )

    def split(block):
        high = block.astype(BF16).astype(F32)
        return [high, block - high]

    def columns_of(parts):
        return jnp.concatenate(parts, axis=0).T.astype(BF16)

    for p in range(mix_pieces):
        send_features(0, p)

    for layer in range(layers):
        squares = jnp.zeros((n_tp * rows, 128), F32)
        for p in range(mix_pieces):
            await_bytes(gathered.at[layer, p, pl.ds(0, n_tp - 1)], gather_recv.at[layer, p])
            widened = stack_groups([gathered[layer, p, s].astype(F32) for s in range(n_tp)])
            span = pl.ds(p * piece, piece)
            scaled = (widened * gain[layer, span][None, :]).astype(BF16)
            for lane in range(0, piece, 128):
                tile = widened[:, lane : lane + 128]
                squares = squares + tile * tile
            if p == mix_pieces - 1:
                for c in range(2):
                    sq_part[layer, c] = squares[24 * c : 24 * c + 24]
                remote(
                    sq_part.at[layer, other_core], sq_near.at[layer],
                    send_sem.at[layer, 1], sq_recv.at[layer, 0], "dp", partner,
                )
            for i in range(pieces):
                if p == 0:
                    load_proj(layer, i).wait()
                result = jnp.dot(scaled, proj[layer, i, span, :], preferred_element_type=F32)
                if p > 0:
                    result = result + product[i]
                if p < mix_pieces - 1:
                    product[i] = result
                    continue
                for c in range(2):
                    block = result[24 * c : 24 * c + 24]
                    tail = jnp.concatenate([block[16:, :256], block[16:, 256:]], axis=0)
                    partial[layer, i, c] = jnp.concatenate([block[:16], tail], axis=1).astype(BF16)
                remote(
                    partial.at[layer, i, other_core], near.at[layer, i],
                    send_sem.at[layer, 2], near_recv.at[layer, i], "dp", partner,
                )

        await_bytes(sq_near.at[layer], sq_recv.at[layer, 0])
        chip_squares = sq_part[layer, core] + sq_near[layer]
        sq_cross[layer] = jnp.concatenate(
            [jnp.where(chip == 0, chip_squares[8:16], chip_squares[:8]), chip_squares[16:]], axis=0
        )
        remote(
            sq_cross.at[layer], sq_far.at[layer],
            send_sem.at[layer, 6], sq_recv.at[layer, 1], "dp", across,
        )
        for i in range(pieces):
            await_bytes(near.at[layer, i], near_recv.at[layer, i])
            both = partial[layer, i, core].astype(F32) + near[layer, i].astype(F32)
            tail = jnp.concatenate([both[:8, piece:], both[8:, piece:]], axis=1)
            zero, one = both[:8, :piece], both[8:, :piece]
            cross[layer, i] = fold(jnp.where(chip == 0, one, zero), tail, other_chip).astype(BF16)
            remote(
                cross.at[layer, i], far.at[layer, i],
                send_sem.at[layer, 3], far_recv.at[layer, i], "dp", across,
            )
            own[i] = fold(jnp.where(chip == 0, zero, one), tail, chip)

        await_bytes(sq_far.at[layer], sq_recv.at[layer, 1])
        last = chip_squares[16:] + sq_far[layer, pl.ds(8, 8), :]
        total_squares = jnp.concatenate(
            [
                jnp.where(chip == 0, chip_squares[:8], chip_squares[8:16])
                + sq_far[layer, pl.ds(0, 8), :],
                jnp.where(chip == 0, last, swap(last)),
            ],
            axis=0,
        )
        inverse = lax.rsqrt(jnp.sum(total_squares, axis=1, keepdims=True) / d_model + EPSILON)

        def projected(i):
            await_bytes(far.at[layer, i], far_recv.at[layer, i])
            return unfold_rows(own[i] + far[layer, i].astype(F32)) * inverse

        query = projected(0)
        key = projected(1) * head_key ** (-0.5)
        logits = projected(2)
        log_sigmoid = jnp.minimum(logits, 0.0) - jnp.log(1.0 + jnp.exp(-jnp.abs(logits)))
        log_decay = log_sigmoid[:rows] / SOFTNESS + offset[:, layer, :]
        decay = jnp.exp(jnp.concatenate([log_decay, jnp.zeros((pad - rows, key_cols), F32)], axis=0))
        read_columns = columns_of(split(query * decay))
        both = query * key
        products = [
            jnp.sum(both[:, h * head_key : (h + 1) * head_key], axis=1, keepdims=True)
            for h in range(heads)
        ]
        load_state(layer).wait()
        for pair in range(rows // 2):
            factors = jnp.dot(
                read_columns, expand[0, pair, pl.ds(0, 2 * pad), :], preferred_element_type=F32
            )
            for k in range(2):
                b = 2 * pair + k
                for h in range(heads):
                    factor = factors[
                        h * head_key : (h + 1) * head_key,
                        k * value_channels : (k + 1) * value_channels,
                    ]
                    readout[h, pl.ds(b, 1), :] = jnp.sum(
                        factor * state[layer, b, h], axis=0, keepdims=True
                    )

        for half in range(halves):
            value = projected(3 + 2 * half)
            gate_all = projected(4 + 2 * half)
            values[:, pl.ds(half * piece, piece)] = value
            gated_heads = []
            for hh in range(half_heads):
                h = half * half_heads + hh
                span = slice(hh * value_channels, (hh + 1) * value_channels)
                got = readout[h] + products[h] * value[:, span]
                gate = gate_all[:, span]
                normed = got * lax.rsqrt(jnp.mean(got * got, axis=1, keepdims=True) + EPSILON)
                whole = pl.ds(h * value_channels, value_channels)
                normed = normed * out_gain[layer, whole][None, :]
                gated_heads.append(normed * (gate / (1.0 + jnp.exp(-gate))))
            gated = jnp.concatenate(gated_heads, axis=1)
            gated_all[layer, half, dp] = fold(gated[:8], gated[8:], 0).astype(BF16)
            for j in range(1, n_dp):
                remote(
                    gated_all.at[layer, half, dp], gated_all.at[layer, half, dp],
                    send_sem.at[layer, 4], gated_recv.at[layer, half],
                    "dp", lax.rem(dp + j, n_dp),
                )

        fresh_columns[...] = columns_of(split(key) + split(decay))
        for pair in range(rows // 2):
            adds = jnp.dot(fresh_columns[...], expand[0, pair], preferred_element_type=F32)
            keeps = jnp.dot(fresh_columns[...], expand[1, pair], preferred_element_type=F32)
            for k in range(2):
                b = 2 * pair + k
                lanes = slice(k * value_channels, (k + 1) * value_channels)
                for h in range(heads):
                    part = slice(h * head_key, (h + 1) * head_key)
                    row = values[pl.ds(b, 1), pl.ds(h * value_channels, value_channels)]
                    new_state_ref[layer, b, h] = (
                        keeps[part, lanes] * state[layer, b, h] + adds[part, lanes] * row
                    )

        load_wo(layer).wait()
        for half in range(halves):
            await_bytes(gated_all.at[layer, half, pl.ds(0, n_dp - 1)], gated_recv.at[layer, half])
            gated = stack_groups(
                [gated_all[layer, half, s].astype(F32) for s in range(n_dp)]
            ).astype(BF16)
            for p in range(mix_pieces):
                columns = pl.ds(p * piece, piece)
                result = jnp.dot(
                    gated, wo[layer, pl.ds(half * piece, piece), columns],
                    preferred_element_type=F32,
                )
                if half > 0:
                    result = result + mix_part[p]
                if half < halves - 1:
                    mix_part[p] = result
                    continue
                for s in range(n_tp):
                    mix_send[layer, p, s] = group_of(result, s).astype(BF16)
                for j in range(n_tp - 1, 0, -1):
                    step = tp_step(j)
                    to = lax.rem(tp + step, n_tp)
                    remote(
                        mix_send.at[layer, p, to], mix_recv.at[layer, p, step - 1],
                        send_sem.at[layer, 5], mix_recv_sem.at[layer, p], "tp", to,
                    )

        await_bytes(gathered.at[layer, :, pl.ds(0, n_tp - 1)], send_sem.at[layer, 0])
        await_bytes(sq_near.at[layer], send_sem.at[layer, 1])
        await_bytes(sq_far.at[layer], send_sem.at[layer, 6])
        await_bytes(near.at[layer], send_sem.at[layer, 2])
        await_bytes(far.at[layer], send_sem.at[layer, 3])
        await_bytes(gated_all.at[layer, :, pl.ds(0, n_dp - 1)], send_sem.at[layer, 4])

        for p in range(mix_pieces):
            await_bytes(mix_recv.at[layer, p], mix_recv_sem.at[layer, p])
            total = mix_send[layer, p, tp].astype(F32)
            for j in range(1, n_tp):
                total = total + mix_recv[layer, p, j - 1].astype(F32)
            result = (gathered[layer, p, tp].astype(F32) + total).astype(BF16)
            if layer + 1 < layers:
                gathered[layer + 1, p, tp] = result
                send_features(layer + 1, p)
            else:
                span = slice(p * piece, (p + 1) * piece)
                hidden_out_ref[:, span] = unfold_rows(result.astype(F32))[:rows].astype(BF16)
        await_bytes(mix_recv.at[layer], send_sem.at[layer, 5])


def store_kernel(hidden_ref, state_ref, hidden_out, state_out, hidden_sem, state_sem):
    layers, rows = state_ref.shape[:2]
    copies = [
        pltpu.make_async_copy(state_ref.at[layer, b], state_out.at[layer, b], state_sem.at[layer, b])
        for layer in range(layers)
        for b in range(rows)
    ]
    copies.append(pltpu.make_async_copy(hidden_ref, hidden_out, hidden_sem))
    for copy in copies:
        copy.start()
    for copy in copies:
        copy.wait()


def fused(
    n_tp, n_dp, hidden_in, input_norm_gain, w_query, w_key, w_decay, w_value, w_gate,
    out_gain, w_out, decay_offset, state,
):
    layers, rows, heads, head_key, value_channels = state.shape
    width = hidden_in.shape[1]
    key_cols, value_cols = w_query.shape[2], w_value.shape[2]
    piece = key_cols
    halves = value_cols // piece
    pieces = 3 + 2 * halves
    mix_pieces = width // piece
    block = (16, piece // 4 * 3)
    vmem = pl.BlockSpec(memory_space=pltpu.VMEM)
    hbm = pl.BlockSpec(memory_space=pl.ANY)
    offsets = decay_offset.transpose(1, 0, 2)
    hidden, fresh = pl.pallas_call(
        functools.partial(
            block_kernel, n_tp, n_dp, width * n_dp, head_key, value_channels, piece
        ),
        out_shape=(
            pltpu.VMEM(hidden_in.shape, BF16),
            pltpu.VMEM(state.shape, F32),
        ),
        in_specs=[hbm] * 11,
        out_specs=(vmem, vmem),
        scratch_shapes=[
            pltpu.VMEM(hidden_in.shape, BF16),
            pltpu.VMEM(input_norm_gain.shape, F32),
            pltpu.VMEM(out_gain.shape, F32),
            pltpu.VMEM(offsets.shape, F32),
            pltpu.VMEM((layers, pieces, width, piece), BF16),
            pltpu.VMEM(w_out.shape, BF16),
            pltpu.VMEM(state.shape, F32),
            pltpu.VMEM((layers, mix_pieces, n_tp) + block, BF16),
            pltpu.VMEM((pieces, n_tp * rows, piece), F32),
            pltpu.VMEM((layers, pieces, 2, 16, piece // 2 * 3), BF16),
            pltpu.VMEM((layers, pieces, 16, piece // 2 * 3), BF16),
            pltpu.VMEM((pieces,) + block, F32),
            pltpu.VMEM((layers, pieces) + block, BF16),
            pltpu.VMEM((layers, pieces) + block, BF16),
            pltpu.VMEM((layers, 2, 2 * rows, 128), F32),
            pltpu.VMEM((layers, 2 * rows, 128), F32),
            pltpu.VMEM((layers, 16, 128), F32),
            pltpu.VMEM((layers, 16, 128), F32),
            pltpu.VMEM((2, rows // 2, 64, 2 * value_channels), BF16),
            pltpu.VMEM((16, value_cols), F32),
            pltpu.VMEM((key_cols, 64), BF16),
            pltpu.VMEM((heads, 16, value_channels), F32),
            pltpu.VMEM((layers, halves, n_dp) + block, BF16),
            pltpu.VMEM((mix_pieces, n_tp * rows, piece), F32),
            pltpu.VMEM((layers, mix_pieces, n_tp) + block, BF16),
            pltpu.VMEM((layers, mix_pieces, n_tp - 1) + block, BF16),
            pltpu.SemaphoreType.DMA((4,)),
            pltpu.SemaphoreType.DMA((layers, pieces)),
            pltpu.SemaphoreType.DMA((layers,)),
            pltpu.SemaphoreType.DMA((layers,)),
            pltpu.SemaphoreType.DMA((layers, mix_pieces)),
            pltpu.SemaphoreType.DMA((layers, pieces)),
            pltpu.SemaphoreType.DMA((layers, pieces)),
            pltpu.SemaphoreType.DMA((layers, 2)),
            pltpu.SemaphoreType.DMA((layers, halves)),
            pltpu.SemaphoreType.DMA((layers, mix_pieces)),
            pltpu.SemaphoreType.DMA((layers, 7)),
        ],
        compiler_params=pltpu.CompilerParams(
            collective_id=0, has_side_effects=True, vmem_limit_bytes=48 * 1024 * 1024
        ),
    )(
        hidden_in, input_norm_gain, out_gain, offsets,
        w_query, w_key, w_decay, w_value, w_gate, w_out, state,
    )
    return pl.pallas_call(
        store_kernel,
        out_shape=(
            jax.ShapeDtypeStruct(hidden_in.shape, BF16),
            jax.ShapeDtypeStruct(state.shape, F32),
        ),
        in_specs=[vmem] * 2,
        out_specs=(hbm, hbm),
        scratch_shapes=[
            pltpu.SemaphoreType.DMA,
            pltpu.SemaphoreType.DMA((layers, rows)),
        ],
        compiler_params=pltpu.CompilerParams(vmem_limit_bytes=1024 * 1024),
    )(hidden, fresh)


def plain(
    hidden_in, input_norm_gain, w_query, w_key, w_decay, w_value, w_gate,
    out_gain, w_out, decay_offset, state,
):
    layers, rows, heads, head_key, value_channels = state.shape
    key_cols, value_cols = w_query.shape[2], w_value.shape[2]
    d_model = hidden_in.shape[1] * lax.axis_size("dp")
    first = lax.axis_index("dp") * rows
    current, states = hidden_in, []
    for layer in range(layers):
        widened = lax.all_gather(current, "tp", axis=0, tiled=True).astype(F32)
        squares = lax.psum(jnp.sum(widened * widened, axis=1), "dp")
        scaled = (widened * input_norm_gain[layer][None, :]).astype(BF16)
        partial = jnp.concatenate(
            [
                jnp.dot(scaled, matrix[layer], preferred_element_type=F32)
                for matrix in (w_query, w_key, w_decay, w_value, w_gate)
            ],
            axis=1,
        ).astype(BF16)
        summed = lax.psum_scatter(partial, "dp", scatter_dimension=0, tiled=True).astype(F32)
        own = lax.dynamic_slice_in_dim(squares, first, rows)
        projected = summed * lax.rsqrt(own / d_model + EPSILON)[:, None]
        query, key, logits, value, gate = jnp.split(
            projected,
            [key_cols, 2 * key_cols, 3 * key_cols, 3 * key_cols + value_cols],
            axis=1,
        )
        decay = jnp.exp(jax.nn.log_sigmoid(logits) / SOFTNESS + decay_offset[layer])
        per_key, per_value = (rows, heads, head_key), (rows, heads, value_channels)
        fresh = (
            decay.reshape(per_key)[..., None] * state[layer]
            + (key * head_key ** (-0.5)).reshape(per_key)[..., None]
            * value.reshape(per_value)[:, :, None, :]
        )
        got = jnp.sum(query.reshape(per_key)[..., None] * fresh, axis=2)
        got = got * lax.rsqrt(jnp.mean(got * got, axis=2, keepdims=True) + EPSILON)
        got = got * out_gain[layer].reshape(heads, value_channels)[None]
        gated = (got * jax.nn.silu(gate.reshape(per_value))).reshape(rows, value_cols).astype(BF16)
        mixed = jnp.dot(
            lax.all_gather(gated, "dp", axis=0, tiled=True), w_out[layer],
            preferred_element_type=F32,
        ).astype(BF16)
        mine = lax.psum_scatter(mixed, "tp", scatter_dimension=0, tiled=True).astype(F32)
        current = (current.astype(F32) + mine).astype(BF16)
        states.append(fresh)
    return current, jnp.stack(states)


def solution(mesh):
    n_tp, n_dp = mesh.shape["tp"], mesh.shape["dp"]

    def per_device(hidden_in, *rest):
        state = rest[-1]
        width, key_cols, value_cols = hidden_in.shape[1], rest[1].shape[2], rest[4].shape[2]
        rows, heads = state.shape[1], state.shape[2]
        sized = key_cols == 512 and width % key_cols == 0 and value_cols % key_cols == 0
        shaped = hidden_in.shape[0] == rows == 12 and state.shape[4] == 128
        if n_tp == 4 and n_dp == 4 and sized and shaped and heads % (value_cols // key_cols) == 0:
            return fused(n_tp, n_dp, hidden_in, *rest)
        return plain(hidden_in, *rest)

    return jax.shard_map(
        per_device,
        mesh=mesh,
        in_specs=(
            P(("grp", "tp"), "dp"),
            P(None, "dp"),
            P(None, "dp", "tp"),
            P(None, "dp", "tp"),
            P(None, "dp", "tp"),
            P(None, "dp", "tp"),
            P(None, "dp", "tp"),
            P(None, "tp"),
            P(None, "tp", "dp"),
            P(None, ("grp", "dp"), "tp"),
            P(None, ("grp", "dp"), "tp", None, None),
        ),
        out_specs=(P(("grp", "tp"), "dp"), P(None, ("grp", "dp"), "tp", None, None)),
        check_vma=False,
    )
```

```python
import functools

import jax
import jax.numpy as jnp
from jax import lax
from jax.experimental import pallas as pl
from jax.experimental.pallas import tpu as pltpu
from jax.sharding import PartitionSpec as P

EPSILON = 1e-06
SOFTNESS = 16.0
F32 = jnp.float32
BF16 = jnp.bfloat16


def swap(tiles):
    return pltpu.roll(tiles, 4, 0)


def first_half(shape):
    return lax.broadcasted_iota(jnp.int32, shape, 0) < 4


def fold(upper, lower, second):
    even = jnp.concatenate([lower[:, :128], lower[:, 256:384]], axis=1)
    odd = jnp.concatenate([lower[:, 128:256], lower[:, 384:]], axis=1)
    top = first_half(even.shape)
    first_form = jnp.where(top, even, swap(odd))
    second_form = jnp.where(top, swap(even), odd)
    if isinstance(second, int):
        folded = second_form if second else first_form
    else:
        folded = jnp.where(second == 1, second_form, first_form)
    return jnp.concatenate(
        [
            jnp.concatenate([upper[:, :256], folded[:, :128]], axis=1),
            jnp.concatenate([upper[:, 256:], folded[:, 128:]], axis=1),
        ],
        axis=0,
    )


def unfold(block):
    upper = jnp.concatenate([block[:8, :256], block[8:, :256]], axis=1)
    left, right = block[:8, 256:], block[8:, 256:]
    lower = jnp.concatenate([left, swap(left), right, swap(right)], axis=1)
    return upper, lower


def unfold_rows(block):
    upper, lower = unfold(block)
    return jnp.concatenate([upper, jnp.where(first_half(lower.shape), lower, 0.0)], axis=0)


def stack_groups(blocks):
    rows = []
    for core in range(2):
        one, two = blocks[core], blocks[2 + core]
        upper_one = jnp.concatenate([one[:8, :256], one[8:, :256]], axis=1)
        upper_two = jnp.concatenate([two[:8, :256], two[8:, :256]], axis=1)
        lower = []
        for half in range(2):
            a, b = one[8 * half : 8 * half + 8, 256:], two[8 * half : 8 * half + 8, 256:]
            top = first_half(a.shape)
            lower += [jnp.where(top, a, swap(b)), jnp.where(top, swap(a), b)]
        rows += [upper_one, upper_two, jnp.concatenate(lower, axis=1)]
    return jnp.concatenate(rows, axis=0)


def group_of(stacked, s):
    chip, core = divmod(s, 2)
    base = 24 * core
    upper = stacked[base + 8 * chip : base + 8 * chip + 8]
    return fold(upper, stacked[base + 16 : base + 24], chip)


def block_kernel(
    n_tp, n_dp, d_model, head_key, value_channels, piece,
    hidden_hbm, gain_hbm, out_gain_hbm, offset_hbm,
    wq_hbm, wk_hbm, wd_hbm, wv_hbm, wg_hbm, wo_hbm, state_hbm,
    hidden_out_ref, new_state_ref,
    hidden, gain, out_gain, offset, proj, wo, state,
    gathered, product, partial, near, own, cross, far,
    sq_part, sq_near, sq_cross, sq_far,
    expand, values, fresh_columns, readout,
    gated_all, mix_part, mix_send, mix_recv, mix_last,
    small_sem, proj_sem, wo_sem, state_sem,
    gather_recv, near_recv, far_recv, sq_recv, gated_recv, mix_recv_sem, send_sem,
):
    layers, rows, heads = state.shape[0], state.shape[1], state.shape[2]
    pad = 16
    mix_pieces = mix_send.shape[1]
    pieces = proj.shape[1]
    key_cols = heads * head_key
    value_cols = heads * value_channels
    halves = value_cols // piece
    half_heads = heads // halves
    groups = ((0, 3), (3, pieces - 3))
    parcels = ((0, 1), (1, 1), (2, 1)) + tuple((3 + 2 * half, 2) for half in range(halves))
    tp = lax.axis_index("tp")
    dp = lax.axis_index("dp")
    chip, core = dp // 2, lax.rem(dp, 2)
    other_core = 1 - core
    other_chip = 1 - chip
    partner = 2 * chip + other_core
    across = 2 * other_chip + core
    mesh_id = pl.DeviceIdType.MESH

    barrier = pltpu.get_barrier_semaphore()
    for j in range(1, n_tp):
        pl.semaphore_signal(
            barrier, inc=1, device_id={"tp": lax.rem(tp + j, n_tp)}, device_id_type=mesh_id
        )
    for j in range(1, n_dp):
        pl.semaphore_signal(
            barrier, inc=1, device_id={"dp": lax.rem(dp + j, n_dp)}, device_id_type=mesh_id
        )

    small = [
        pltpu.make_async_copy(source, target, small_sem.at[index])
        for index, (source, target) in enumerate(
            ((hidden_hbm, hidden), (gain_hbm, gain), (out_gain_hbm, out_gain), (offset_hbm, offset))
        )
    ]

    def load_proj(layer, i):
        if i < 3:
            source = (wd_hbm, wq_hbm, wk_hbm)[i].at[layer]
        else:
            half, which = divmod(i - 3, 2)
            source = (wv_hbm, wg_hbm)[which].at[layer, :, pl.ds(half * piece, piece)]
        return pltpu.make_async_copy(source, proj.at[layer, i], proj_sem.at[layer])

    def load_wo(layer):
        return pltpu.make_async_copy(wo_hbm.at[layer], wo.at[layer], wo_sem)

    def load_state(layer):
        return pltpu.make_async_copy(state_hbm.at[layer], state.at[layer], state_sem)

    for copy in small:
        copy.start()

    row_of = lax.broadcasted_iota(jnp.int32, (4 * pad, 2 * value_channels), 0)
    lane_of = lax.broadcasted_iota(jnp.int32, (4 * pad, 2 * value_channels), 1)
    for second in range(2):
        for pair in range(rows // 2):
            picked = pair * 2 + lane_of // value_channels
            inside = (row_of >= second * 2 * pad) & (row_of < (second + 1) * 2 * pad)
            hit = inside & (lax.rem(row_of, pad) == picked)
            expand[second, pair] = jnp.where(hit, 1.0, 0.0).astype(BF16)

    for copy in small:
        copy.wait()
    for layer in range(layers):
        for i in range(pieces):
            load_proj(layer, i).start()
        load_state(layer).start()
        load_wo(layer).start()

    upper = hidden[pl.ds(0, 8), :].astype(F32)
    lower = hidden[pl.ds(8, 4), :].astype(F32)
    lower = jnp.concatenate([lower, lower], axis=0)
    for p in range(mix_pieces):
        span = slice(p * piece, (p + 1) * piece)
        gathered[0, p, tp] = fold(upper[:, span], lower[:, span], 0).astype(BF16)
    pl.semaphore_wait(barrier, n_tp + n_dp - 2)

    def remote(src, dst, send, recv, axis, target):
        copy = pltpu.make_async_remote_copy(
            src_ref=src, dst_ref=dst, send_sem=send, recv_sem=recv,
            device_id={axis: target}, device_id_type=mesh_id,
        )
        copy.start()

    def await_bytes(ref, sem):
        pltpu.make_async_copy(ref, ref, sem).wait()

    above = tp // 2
    is_owner = (tp == 1) | (tp == 2)

    def tp_step(j):
        return j + above * (n_tp - 2 * j)

    def send_features(layer, p):
        for j in range(n_tp - 1, 0, -1):
            remote(
                gathered.at[layer, p, tp], gathered.at[layer, p, tp],
                send_sem.at[0], gather_recv.at[p],
                "tp", lax.rem(tp + tp_step(j), n_tp),
            )

    def await_features(layer, p):
        if layer == 0:
            await_bytes(gathered.at[layer, p, pl.ds(0, n_tp - 1)], gather_recv.at[p])
            return

        @pl.when(is_owner)
        def _():
            await_bytes(gathered.at[layer, p, pl.ds(0, 2)], gather_recv.at[p])

        @pl.when(jnp.logical_not(is_owner))
        def _():
            await_bytes(gathered.at[layer, p], gather_recv.at[p])

    def await_feature_sends(layer):
        if layer == 0:
            await_bytes(gathered.at[layer, :, pl.ds(0, n_tp - 1)], send_sem.at[0])
            return

        @pl.when(is_owner)
        def _():
            await_bytes(mix_recv.at[layer - 1], send_sem.at[0])

    def send_mixed(layer, p):
        for k in range(2):

            def send_to(owner):
                remote(
                    mix_send.at[layer, p, 2 * (owner - 1) + k],
                    mix_recv.at[layer, p, k, tp - above],
                    send_sem.at[5], mix_recv_sem.at[p, k], "tp", owner,
                )

            send_to(2 - above)

            @pl.when(jnp.logical_not(is_owner))
            def _():
                send_to(1 + above)

    lowest = tp == 0
    last_order = (
        jnp.where(lowest, 3, 0),
        jnp.where(lowest, 2, 1 + lax.rem(tp, 3)),
        jnp.where(lowest, 1, 1 + lax.rem(tp + 1, 3)),
    )

    def send_last(layer, p, to):
        remote(
            mix_send.at[layer, p, to], mix_last.at[p, lax.rem(tp - to + n_tp - 1, n_tp)],
            send_sem.at[5], mix_recv_sem.at[p, 0], "tp", to,
        )

    def await_mixed_sends(layer):
        if layer == layers - 1:
            await_bytes(mix_last, send_sem.at[5])
            return

        @pl.when(is_owner)
        def _():
            await_bytes(mix_send.at[layer, :, pl.ds(0, 2)], send_sem.at[5])

        @pl.when(jnp.logical_not(is_owner))
        def _():
            await_bytes(mix_send.at[layer], send_sem.at[5])

    def finish_middle(layer):
        for p in range(mix_pieces):
            for k in range(2):
                await_bytes(mix_recv.at[layer, p, k], mix_recv_sem.at[p, k])
                mine = 2 * (tp - 1) + k
                total = mix_send[layer, p, mine].astype(F32)
                for j in range(n_tp - 1):
                    total = total + mix_recv[layer, p, k, j].astype(F32)
                gathered[layer + 1, p, mine] = (
                    gathered[layer, p, mine].astype(F32) + total
                ).astype(BF16)
                block = gathered.at[layer + 1, p, mine]
                for to in (3 * (2 - tp), 3 - tp, 3 * (tp - 1)):
                    remote(block, block, send_sem.at[0], gather_recv.at[p], "tp", to)

    def split(block):
        high = block.astype(BF16).astype(F32)
        return [high, block - high]

    def columns_of(parts):
        return jnp.concatenate(parts, axis=0).T.astype(BF16)

    for p in range(mix_pieces):
        send_features(0, p)

    for layer in range(layers):
        squares = jnp.zeros((n_tp * rows, 128), F32)
        for p in range(mix_pieces):
            await_features(layer, p)
            widened = stack_groups([gathered[layer, p, s].astype(F32) for s in range(n_tp)])
            span = pl.ds(p * piece, piece)
            scaled = (widened * gain[layer, span][None, :]).astype(BF16)
            for lane in range(0, piece, 128):
                tile = widened[:, lane : lane + 128]
                squares = squares + tile * tile
            if p == mix_pieces - 1:
                for c in range(2):
                    sq_part[layer, c] = squares[24 * c : 24 * c + 24]
                remote(
                    sq_part.at[layer, other_core], sq_near.at[layer],
                    send_sem.at[1], sq_recv.at[0], "dp", partner,
                )
            if p == 0:
                await_bytes(proj.at[layer], proj_sem.at[layer])
            for first, count in groups:
                for i in range(first, first + count):
                    result = jnp.dot(scaled, proj[layer, i, span, :], preferred_element_type=F32)
                    if p > 0:
                        result = result + product[i]
                    if p < mix_pieces - 1:
                        product[i] = result
                        continue
                    for c in range(2):
                        block = result[24 * c : 24 * c + 24]
                        tail = jnp.concatenate([block[16:, :256], block[16:, 256:]], axis=0)
                        partial[layer, c, i] = jnp.concatenate(
                            [block[:16], tail], axis=1
                        ).astype(BF16)
                if p == mix_pieces - 1:
                    these = pl.ds(first, count)
                    remote(
                        partial.at[layer, other_core, these], near.at[layer, these],
                        send_sem.at[2], near_recv.at[min(first, 1)], "dp", partner,
                    )

        await_bytes(sq_near.at[layer], sq_recv.at[0])
        chip_squares = sq_part[layer, core] + sq_near[layer]
        sq_cross[layer] = jnp.concatenate(
            [jnp.where(chip == 0, chip_squares[8:16], chip_squares[:8]), chip_squares[16:]], axis=0
        )
        remote(
            sq_cross.at[layer], sq_far.at[layer],
            send_sem.at[6], sq_recv.at[1], "dp", across,
        )
        for i in range(pieces):
            for first, count in groups:
                if i == first:
                    await_bytes(near.at[layer, pl.ds(first, count)], near_recv.at[min(first, 1)])
            both = partial[layer, core, i].astype(F32) + near[layer, i].astype(F32)
            tail = jnp.concatenate([both[:8, piece:], both[8:, piece:]], axis=1)
            zero, one = both[:8, :piece], both[8:, :piece]
            cross[layer, i] = fold(jnp.where(chip == 0, one, zero), tail, other_chip).astype(BF16)
            for number, (first, count) in enumerate(parcels):
                if i == first + count - 1:
                    these = pl.ds(first, count)
                    remote(
                        cross.at[layer, these], far.at[layer, these],
                        send_sem.at[3], far_recv.at[number], "dp", across,
                    )
            own[i] = fold(jnp.where(chip == 0, zero, one), tail, chip)

        await_bytes(sq_far.at[layer], sq_recv.at[1])
        last = chip_squares[16:] + sq_far[layer, pl.ds(8, 8), :]
        total_squares = jnp.concatenate(
            [
                jnp.where(chip == 0, chip_squares[:8], chip_squares[8:16])
                + sq_far[layer, pl.ds(0, 8), :],
                jnp.where(chip == 0, last, swap(last)),
            ],
            axis=0,
        )
        inverse = lax.rsqrt(jnp.sum(total_squares, axis=1, keepdims=True) / d_model + EPSILON)

        def projected(i):
            for number, (first, count) in enumerate(parcels):
                if i == first:
                    await_bytes(far.at[layer, pl.ds(first, count)], far_recv.at[number])
            return unfold_rows(own[i] + far[layer, i].astype(F32)) * inverse

        if layer == 0:
            await_bytes(state, state_sem)
        logits = projected(0)
        log_sigmoid = jnp.minimum(logits, 0.0) - jnp.log(1.0 + jnp.exp(-jnp.abs(logits)))
        log_decay = log_sigmoid[:rows] / SOFTNESS + offset[:, layer, :]
        decay = jnp.exp(jnp.concatenate([log_decay, jnp.zeros((pad - rows, key_cols), F32)], axis=0))
        query = projected(1)
        read_columns = columns_of(split(query * decay))
        key = projected(2) * head_key ** (-0.5)
        both = query * key
        products = [
            jnp.sum(both[:, h * head_key : (h + 1) * head_key], axis=1, keepdims=True)
            for h in range(heads)
        ]

        for half in range(halves):
            base = half * half_heads
            columns = read_columns[base * head_key : (base + half_heads) * head_key]
            for pair in range(rows // 2):
                factors = jnp.dot(
                    columns, expand[0, pair, pl.ds(0, 2 * pad), :], preferred_element_type=F32
                )
                for k in range(2):
                    b = 2 * pair + k
                    for hh in range(half_heads):
                        factor = factors[
                            hh * head_key : (hh + 1) * head_key,
                            k * value_channels : (k + 1) * value_channels,
                        ]
                        readout[base + hh, pl.ds(b, 1), :] = jnp.sum(
                            factor * state[layer, b, base + hh], axis=0, keepdims=True
                        )
            value = projected(3 + 2 * half)
            gate_all = projected(4 + 2 * half)
            values[:, pl.ds(half * piece, piece)] = value
            gated_heads = []
            for hh in range(half_heads):
                h = base + hh
                span = slice(hh * value_channels, (hh + 1) * value_channels)
                got = readout[h] + products[h] * value[:, span]
                gate = gate_all[:, span]
                normed = got * lax.rsqrt(jnp.mean(got * got, axis=1, keepdims=True) + EPSILON)
                whole = pl.ds(h * value_channels, value_channels)
                normed = normed * out_gain[layer, whole][None, :]
                gated_heads.append(normed * (gate / (1.0 + jnp.exp(-gate))))
            gated = jnp.concatenate(gated_heads, axis=1)
            gated_all[layer, half, dp] = fold(gated[:8], gated[8:], 0).astype(BF16)
            for j in range(1, n_dp):
                remote(
                    gated_all.at[layer, half, dp], gated_all.at[layer, half, dp],
                    send_sem.at[4], gated_recv.at[half],
                    "dp", lax.rem(dp + j, n_dp),
                )

        fresh_columns[...] = columns_of(split(key) + split(decay))
        for pair in range(rows // 2):
            adds = jnp.dot(fresh_columns[...], expand[0, pair], preferred_element_type=F32)
            keeps = jnp.dot(fresh_columns[...], expand[1, pair], preferred_element_type=F32)
            for k in range(2):
                b = 2 * pair + k
                lanes = slice(k * value_channels, (k + 1) * value_channels)
                for h in range(heads):
                    part = slice(h * head_key, (h + 1) * head_key)
                    row = values[pl.ds(b, 1), pl.ds(h * value_channels, value_channels)]
                    new_state_ref[layer, b, h] = (
                        keeps[part, lanes] * state[layer, b, h] + adds[part, lanes] * row
                    )

        if layer == 0:
            await_bytes(wo, wo_sem)
        for half in range(halves):
            await_bytes(gated_all.at[layer, half, pl.ds(0, n_dp - 1)], gated_recv.at[half])
            gated = stack_groups(
                [gated_all[layer, half, s].astype(F32) for s in range(n_dp)]
            ).astype(BF16)
            for p in range(mix_pieces):
                columns = pl.ds(p * piece, piece)
                result = jnp.dot(
                    gated, wo[layer, pl.ds(half * piece, piece), columns],
                    preferred_element_type=F32,
                )
                if half > 0:
                    result = result + mix_part[p]
                if half < halves - 1:
                    mix_part[p] = result
                    continue
                for s in range(n_tp):
                    mix_send[layer, p, s] = group_of(result, s).astype(BF16)
                if layer < layers - 1:
                    send_mixed(layer, p)
                else:
                    send_last(layer, p, last_order[0])

        if layer == layers - 1:
            for to in last_order[1:]:
                for p in range(mix_pieces):
                    send_last(layer, p, to)

        await_feature_sends(layer)
        await_bytes(sq_near.at[layer], send_sem.at[1])
        await_bytes(sq_far.at[layer], send_sem.at[6])
        await_bytes(near.at[layer], send_sem.at[2])
        await_bytes(far.at[layer], send_sem.at[3])
        await_bytes(gated_all.at[layer, :, pl.ds(0, n_dp - 1)], send_sem.at[4])

        if layer + 1 < layers:
            pl.when(is_owner)(functools.partial(finish_middle, layer))
        else:
            for p in range(mix_pieces):
                await_bytes(mix_last.at[p], mix_recv_sem.at[p, 0])
                total = mix_send[layer, p, tp].astype(F32)
                for j in range(n_tp - 1):
                    total = total + mix_last[p, j].astype(F32)
                result = (gathered[layer, p, tp].astype(F32) + total).astype(BF16)
                span = slice(p * piece, (p + 1) * piece)
                hidden_out_ref[:, span] = unfold_rows(result.astype(F32))[:rows].astype(BF16)
        await_mixed_sends(layer)


def store_kernel(hidden_ref, state_ref, hidden_out, state_out, hidden_sem, state_sem):
    layers, rows, heads = state_ref.shape[:3]
    for layer in range(layers):
        for b in range(rows):
            for half in range(2):
                part = (layer, b, pl.ds(half * (heads // 2), heads // 2))
                pltpu.make_async_copy(state_ref.at[part], state_out.at[part], state_sem).start()
    store_hidden = pltpu.make_async_copy(hidden_ref, hidden_out, hidden_sem)
    store_hidden.start()
    store_hidden.wait()
    pltpu.make_async_copy(state_ref, state_out, state_sem).wait()


def fused(
    n_tp, n_dp, hidden_in, input_norm_gain, w_query, w_key, w_decay, w_value, w_gate,
    out_gain, w_out, decay_offset, state,
):
    layers, rows, heads, head_key, value_channels = state.shape
    width = hidden_in.shape[1]
    key_cols, value_cols = w_query.shape[2], w_value.shape[2]
    piece = key_cols
    halves = value_cols // piece
    pieces = 3 + 2 * halves
    mix_pieces = width // piece
    block = (16, piece // 4 * 3)
    vmem = pl.BlockSpec(memory_space=pltpu.VMEM)
    hbm = pl.BlockSpec(memory_space=pl.ANY)
    offsets = decay_offset.transpose(1, 0, 2)
    hidden, fresh = pl.pallas_call(
        functools.partial(
            block_kernel, n_tp, n_dp, width * n_dp, head_key, value_channels, piece
        ),
        out_shape=(
            pltpu.VMEM(hidden_in.shape, BF16),
            pltpu.VMEM(state.shape, F32),
        ),
        in_specs=[hbm] * 11,
        out_specs=(vmem, vmem),
        scratch_shapes=[
            pltpu.VMEM(hidden_in.shape, BF16),
            pltpu.VMEM(input_norm_gain.shape, F32),
            pltpu.VMEM(out_gain.shape, F32),
            pltpu.VMEM(offsets.shape, F32),
            pltpu.VMEM((layers, pieces, width, piece), BF16),
            pltpu.VMEM(w_out.shape, BF16),
            pltpu.VMEM(state.shape, F32),
            pltpu.VMEM((layers, mix_pieces, n_tp) + block, BF16),
            pltpu.VMEM((pieces, n_tp * rows, piece), F32),
            pltpu.VMEM((layers, 2, pieces, 16, piece // 2 * 3), BF16),
            pltpu.VMEM((layers, pieces, 16, piece // 2 * 3), BF16),
            pltpu.VMEM((pieces,) + block, F32),
            pltpu.VMEM((layers, pieces) + block, BF16),
            pltpu.VMEM((layers, pieces) + block, BF16),
            pltpu.VMEM((layers, 2, 2 * rows, 128), F32),
            pltpu.VMEM((layers, 2 * rows, 128), F32),
            pltpu.VMEM((layers, 16, 128), F32),
            pltpu.VMEM((layers, 16, 128), F32),
            pltpu.VMEM((2, rows // 2, 64, 2 * value_channels), BF16),
            pltpu.VMEM((16, value_cols), F32),
            pltpu.VMEM((key_cols, 64), BF16),
            pltpu.VMEM((heads, 16, value_channels), F32),
            pltpu.VMEM((layers, halves, n_dp) + block, BF16),
            pltpu.VMEM((mix_pieces, n_tp * rows, piece), F32),
            pltpu.VMEM((layers, mix_pieces, n_tp) + block, BF16),
            pltpu.VMEM((layers - 1, mix_pieces, 2, n_tp - 1) + block, BF16),
            pltpu.VMEM((mix_pieces, n_tp - 1) + block, BF16),
            pltpu.SemaphoreType.DMA((4,)),
            pltpu.SemaphoreType.DMA((layers,)),
            pltpu.SemaphoreType.DMA,
            pltpu.SemaphoreType.DMA,
            pltpu.SemaphoreType.DMA((mix_pieces,)),
            pltpu.SemaphoreType.DMA((2,)),
            pltpu.SemaphoreType.DMA((3 + halves,)),
            pltpu.SemaphoreType.DMA((2,)),
            pltpu.SemaphoreType.DMA((halves,)),
            pltpu.SemaphoreType.DMA((mix_pieces, 2)),
            pltpu.SemaphoreType.DMA((7,)),
        ],
        compiler_params=pltpu.CompilerParams(
            collective_id=0, has_side_effects=True, vmem_limit_bytes=48 * 1024 * 1024
        ),
    )(
        hidden_in, input_norm_gain, out_gain, offsets,
        w_query, w_key, w_decay, w_value, w_gate, w_out, state,
    )
    return pl.pallas_call(
        store_kernel,
        out_shape=(
            jax.ShapeDtypeStruct(hidden_in.shape, BF16),
            jax.ShapeDtypeStruct(state.shape, F32),
        ),
        in_specs=[vmem] * 2,
        out_specs=(hbm, hbm),
        scratch_shapes=[
            pltpu.SemaphoreType.DMA,
            pltpu.SemaphoreType.DMA,
        ],
        compiler_params=pltpu.CompilerParams(vmem_limit_bytes=1024 * 1024),
    )(hidden, fresh)


def plain(
    hidden_in, input_norm_gain, w_query, w_key, w_decay, w_value, w_gate,
    out_gain, w_out, decay_offset, state,
):
    layers, rows, heads, head_key, value_channels = state.shape
    key_cols, value_cols = w_query.shape[2], w_value.shape[2]
    d_model = hidden_in.shape[1] * lax.axis_size("dp")
    first = lax.axis_index("dp") * rows
    current, states = hidden_in, []
    for layer in range(layers):
        widened = lax.all_gather(current, "tp", axis=0, tiled=True).astype(F32)
        squares = lax.psum(jnp.sum(widened * widened, axis=1), "dp")
        scaled = (widened * input_norm_gain[layer][None, :]).astype(BF16)
        partial = jnp.concatenate(
            [
                jnp.dot(scaled, matrix[layer], preferred_element_type=F32)
                for matrix in (w_query, w_key, w_decay, w_value, w_gate)
            ],
            axis=1,
        ).astype(BF16)
        summed = lax.psum_scatter(partial, "dp", scatter_dimension=0, tiled=True).astype(F32)
        own = lax.dynamic_slice_in_dim(squares, first, rows)
        projected = summed * lax.rsqrt(own / d_model + EPSILON)[:, None]
        query, key, logits, value, gate = jnp.split(
            projected,
            [key_cols, 2 * key_cols, 3 * key_cols, 3 * key_cols + value_cols],
            axis=1,
        )
        decay = jnp.exp(jax.nn.log_sigmoid(logits) / SOFTNESS + decay_offset[layer])
        per_key, per_value = (rows, heads, head_key), (rows, heads, value_channels)
        fresh = (
            decay.reshape(per_key)[..., None] * state[layer]
            + (key * head_key ** (-0.5)).reshape(per_key)[..., None]
            * value.reshape(per_value)[:, :, None, :]
        )
        got = jnp.sum(query.reshape(per_key)[..., None] * fresh, axis=2)
        got = got * lax.rsqrt(jnp.mean(got * got, axis=2, keepdims=True) + EPSILON)
        got = got * out_gain[layer].reshape(heads, value_channels)[None]
        gated = (got * jax.nn.silu(gate.reshape(per_value))).reshape(rows, value_cols).astype(BF16)
        mixed = jnp.dot(
            lax.all_gather(gated, "dp", axis=0, tiled=True), w_out[layer],
            preferred_element_type=F32,
        ).astype(BF16)
        mine = lax.psum_scatter(mixed, "tp", scatter_dimension=0, tiled=True).astype(F32)
        current = (current.astype(F32) + mine).astype(BF16)
        states.append(fresh)
    return current, jnp.stack(states)


def solution(mesh):
    n_tp, n_dp = mesh.shape["tp"], mesh.shape["dp"]

    def per_device(hidden_in, *rest):
        state = rest[-1]
        width, key_cols, value_cols = hidden_in.shape[1], rest[1].shape[2], rest[4].shape[2]
        layers, rows, heads = state.shape[:3]
        sized = key_cols == 512 and width % key_cols == 0 and value_cols % key_cols == 0
        shaped = hidden_in.shape[0] == rows == 12 and state.shape[4] == 128
        if n_tp == 4 and n_dp == 4 and layers > 1 and sized and shaped and heads % (value_cols // key_cols) == 0:
            return fused(n_tp, n_dp, hidden_in, *rest)
        return plain(hidden_in, *rest)

    return jax.shard_map(
        per_device,
        mesh=mesh,
        in_specs=(
            P(("grp", "tp"), "dp"),
            P(None, "dp"),
            P(None, "dp", "tp"),
            P(None, "dp", "tp"),
            P(None, "dp", "tp"),
            P(None, "dp", "tp"),
            P(None, "dp", "tp"),
            P(None, "tp"),
            P(None, "tp", "dp"),
            P(None, ("grp", "dp"), "tp"),
            P(None, ("grp", "dp"), "tp", None, None),
        ),
        out_specs=(P(("grp", "tp"), "dp"), P(None, ("grp", "dp"), "tp", None, None)),
        check_vma=False,
    )
```

```python
import functools

import jax
import jax.numpy as jnp
from jax import lax
from jax.experimental import pallas as pl
from jax.experimental.pallas import tpu as pltpu
from jax.sharding import PartitionSpec as P

EPSILON = 1e-06
SOFTNESS = 16.0
F32 = jnp.float32
BF16 = jnp.bfloat16


def swap(tiles):
    return pltpu.roll(tiles, 4, 0)


def first_half(shape):
    return lax.broadcasted_iota(jnp.int32, shape, 0) < 4


def fold(upper, lower, second):
    even = jnp.concatenate([lower[:, :128], lower[:, 256:384]], axis=1)
    odd = jnp.concatenate([lower[:, 128:256], lower[:, 384:]], axis=1)
    top = first_half(even.shape)
    first_form = jnp.where(top, even, swap(odd))
    second_form = jnp.where(top, swap(even), odd)
    if isinstance(second, int):
        folded = second_form if second else first_form
    else:
        folded = jnp.where(second == 1, second_form, first_form)
    return jnp.concatenate(
        [
            jnp.concatenate([upper[:, :256], folded[:, :128]], axis=1),
            jnp.concatenate([upper[:, 256:], folded[:, 128:]], axis=1),
        ],
        axis=0,
    )


def unfold(block):
    upper = jnp.concatenate([block[:8, :256], block[8:, :256]], axis=1)
    left, right = block[:8, 256:], block[8:, 256:]
    lower = jnp.concatenate([left, swap(left), right, swap(right)], axis=1)
    return upper, lower


def unfold_rows(block):
    upper, lower = unfold(block)
    return jnp.concatenate([upper, jnp.where(first_half(lower.shape), lower, 0.0)], axis=0)


def stack_groups(blocks):
    rows = []
    for core in range(2):
        one, two = blocks[core], blocks[2 + core]
        upper_one = jnp.concatenate([one[:8, :256], one[8:, :256]], axis=1)
        upper_two = jnp.concatenate([two[:8, :256], two[8:, :256]], axis=1)
        lower = []
        for half in range(2):
            a, b = one[8 * half : 8 * half + 8, 256:], two[8 * half : 8 * half + 8, 256:]
            top = first_half(a.shape)
            lower += [jnp.where(top, a, swap(b)), jnp.where(top, swap(a), b)]
        rows += [upper_one, upper_two, jnp.concatenate(lower, axis=1)]
    return jnp.concatenate(rows, axis=0)


def group_of(stacked, s):
    chip, core = divmod(s, 2)
    base = 24 * core
    upper = stacked[base + 8 * chip : base + 8 * chip + 8]
    return fold(upper, stacked[base + 16 : base + 24], chip)


def block_kernel(
    n_tp, n_dp, d_model, head_key, value_channels, piece,
    hidden_hbm, gain_hbm, out_gain_hbm, offset_hbm,
    wq_hbm, wk_hbm, wd_hbm, wv_hbm, wg_hbm, wo_hbm, state_hbm,
    hidden_out_ref, new_state_ref,
    hidden, gain, out_gain, offset, proj, wo, state,
    gathered, product, partial, near, own, cross, far,
    sq_part, sq_near, sq_cross, sq_far,
    expand, values, fresh_columns, readout,
    gated_all, mix_part, mix_send, mix_recv, mix_last,
    small_sem, proj_sem, wo_sem, state_sem,
    gather_recv, near_recv, far_recv, sq_recv, gated_recv, mix_recv_sem, send_sem,
):
    layers, rows, heads = state.shape[0], state.shape[1], state.shape[2]
    pad = 16
    mix_pieces = mix_send.shape[1]
    pieces = proj.shape[1]
    key_cols = heads * head_key
    value_cols = heads * value_channels
    halves = value_cols // piece
    half_heads = heads // halves
    pairs = tuple((3 + 2 * half, 2) for half in range(halves))
    groups = ((0, 3),) + pairs
    parcels = ((0, 1), (1, 1), (2, 1)) + pairs
    tp = lax.axis_index("tp")
    dp = lax.axis_index("dp")
    chip, core = dp // 2, lax.rem(dp, 2)
    other_core = 1 - core
    other_chip = 1 - chip
    partner = 2 * chip + other_core
    across = 2 * other_chip + core
    mesh_id = pl.DeviceIdType.MESH

    barrier = pltpu.get_barrier_semaphore()
    for j in range(1, n_tp):
        pl.semaphore_signal(
            barrier, inc=1, device_id={"tp": lax.rem(tp + j, n_tp)}, device_id_type=mesh_id
        )
    for j in range(1, n_dp):
        pl.semaphore_signal(
            barrier, inc=1, device_id={"dp": lax.rem(dp + j, n_dp)}, device_id_type=mesh_id
        )

    small = [
        pltpu.make_async_copy(source, target, small_sem.at[index])
        for index, (source, target) in enumerate(
            ((hidden_hbm, hidden), (gain_hbm, gain), (out_gain_hbm, out_gain), (offset_hbm, offset))
        )
    ]

    def load_proj(layer, i):
        if i < 3:
            source = (wd_hbm, wq_hbm, wk_hbm)[i].at[layer]
        else:
            half, which = divmod(i - 3, 2)
            source = (wv_hbm, wg_hbm)[which].at[layer, :, pl.ds(half * piece, piece)]
        return pltpu.make_async_copy(source, proj.at[layer, i], proj_sem.at[layer])

    def load_wo(layer):
        return pltpu.make_async_copy(wo_hbm.at[layer], wo.at[layer], wo_sem)

    def load_state(layer):
        return pltpu.make_async_copy(state_hbm.at[layer], state.at[layer], state_sem)

    for copy in small:
        copy.start()

    row_of = lax.broadcasted_iota(jnp.int32, (4 * pad, 2 * value_channels), 0)
    lane_of = lax.broadcasted_iota(jnp.int32, (4 * pad, 2 * value_channels), 1)
    for second in range(2):
        for pair in range(rows // 2):
            picked = pair * 2 + lane_of // value_channels
            inside = (row_of >= second * 2 * pad) & (row_of < (second + 1) * 2 * pad)
            hit = inside & (lax.rem(row_of, pad) == picked)
            expand[second, pair] = jnp.where(hit, 1.0, 0.0).astype(BF16)

    for copy in small:
        copy.wait()
    for layer in range(layers):
        for i in range(pieces):
            load_proj(layer, i).start()
        load_state(layer).start()
        load_wo(layer).start()

    upper = hidden[pl.ds(0, 8), :].astype(F32)
    lower = hidden[pl.ds(8, 4), :].astype(F32)
    lower = jnp.concatenate([lower, lower], axis=0)
    for p in range(mix_pieces):
        span = slice(p * piece, (p + 1) * piece)
        gathered[0, p, tp] = fold(upper[:, span], lower[:, span], 0).astype(BF16)
    pl.semaphore_wait(barrier, n_tp + n_dp - 2)

    def remote(src, dst, send, recv, axis, target):
        copy = pltpu.make_async_remote_copy(
            src_ref=src, dst_ref=dst, send_sem=send, recv_sem=recv,
            device_id={axis: target}, device_id_type=mesh_id,
        )
        copy.start()

    def await_bytes(ref, sem):
        pltpu.make_async_copy(ref, ref, sem).wait()

    above = tp // 2
    is_owner = (tp == 1) | (tp == 2)

    def tp_step(j):
        return j + above * (n_tp - 2 * j)

    def send_features(layer, p):
        for j in range(n_tp - 1, 0, -1):
            remote(
                gathered.at[layer, p, tp], gathered.at[layer, p, tp],
                send_sem.at[0], gather_recv.at[p],
                "tp", lax.rem(tp + tp_step(j), n_tp),
            )

    def await_features(layer, p):
        if layer == 0:
            await_bytes(gathered.at[layer, p, pl.ds(0, n_tp - 1)], gather_recv.at[p])
            return

        @pl.when(is_owner)
        def _():
            await_bytes(gathered.at[layer, p, pl.ds(0, 2)], gather_recv.at[p])

        @pl.when(jnp.logical_not(is_owner))
        def _():
            await_bytes(gathered.at[layer, p], gather_recv.at[p])

    def await_feature_sends(layer):
        if layer == 0:
            await_bytes(gathered.at[layer, :, pl.ds(0, n_tp - 1)], send_sem.at[0])
            return

        @pl.when(is_owner)
        def _():
            await_bytes(mix_recv.at[layer - 1], send_sem.at[0])

    def send_mixed(layer, p):
        for k in range(2):

            def send_to(owner):
                remote(
                    mix_send.at[layer, p, 2 * (owner - 1) + k],
                    mix_recv.at[layer, p, k, tp - above],
                    send_sem.at[5], mix_recv_sem.at[p, k], "tp", owner,
                )

            send_to(2 - above)

            @pl.when(jnp.logical_not(is_owner))
            def _():
                send_to(1 + above)

    lowest = tp == 0
    last_order = (
        jnp.where(lowest, 3, 0),
        jnp.where(lowest, 2, 1 + lax.rem(tp, 3)),
        jnp.where(lowest, 1, 1 + lax.rem(tp + 1, 3)),
    )

    def send_last(layer, p, to):
        remote(
            mix_send.at[layer, p, to], mix_last.at[p, lax.rem(tp - to + n_tp - 1, n_tp)],
            send_sem.at[5], mix_recv_sem.at[p, 0], "tp", to,
        )

    def await_mixed_sends(layer):
        if layer == layers - 1:
            await_bytes(mix_last, send_sem.at[5])
            return

        @pl.when(is_owner)
        def _():
            await_bytes(mix_send.at[layer, :, pl.ds(0, 2)], send_sem.at[5])

        @pl.when(jnp.logical_not(is_owner))
        def _():
            await_bytes(mix_send.at[layer], send_sem.at[5])

    def finish_middle(layer):
        for p in range(mix_pieces):
            for k in range(2):
                await_bytes(mix_recv.at[layer, p, k], mix_recv_sem.at[p, k])
                mine = 2 * (tp - 1) + k
                total = mix_send[layer, p, mine].astype(F32)
                for j in range(n_tp - 1):
                    total = total + mix_recv[layer, p, k, j].astype(F32)
                gathered[layer + 1, p, mine] = (
                    gathered[layer, p, mine].astype(F32) + total
                ).astype(BF16)
                block = gathered.at[layer + 1, p, mine]
                for to in (3 * (2 - tp), 3 - tp, 3 * (tp - 1)):
                    remote(block, block, send_sem.at[0], gather_recv.at[p], "tp", to)

    def store_partial(layer, i, result):
        for c in range(2):
            block = result[24 * c : 24 * c + 24]
            tail = jnp.concatenate([block[16:, :256], block[16:, 256:]], axis=0)
            partial[layer, c, i] = jnp.concatenate([block[:16], tail], axis=1).astype(BF16)

    def send_group(layer, number):
        these = pl.ds(*groups[number])
        remote(
            partial.at[layer, other_core, these], near.at[layer, these],
            send_sem.at[2], near_recv.at[number], "dp", partner,
        )

    def cross_first(layer):
        await_bytes(sq_near.at[layer], sq_recv.at[0])
        chip_squares = sq_part[layer, core] + sq_near[layer]
        sq_part[layer, core] = chip_squares
        sq_cross[layer] = jnp.concatenate(
            [jnp.where(chip == 0, chip_squares[8:16], chip_squares[:8]), chip_squares[16:]], axis=0
        )
        remote(
            sq_cross.at[layer], sq_far.at[layer], send_sem.at[6], sq_recv.at[1], "dp", across
        )
        cross_group(layer, 0)

    def cross_group(layer, number):
        begin, amount = groups[number]
        await_bytes(near.at[layer, pl.ds(begin, amount)], near_recv.at[number])
        for i in range(begin, begin + amount):
            both = partial[layer, core, i].astype(F32) + near[layer, i].astype(F32)
            tail = jnp.concatenate([both[:8, piece:], both[8:, piece:]], axis=1)
            zero, one = both[:8, :piece], both[8:, :piece]
            cross[layer, i] = fold(jnp.where(chip == 0, one, zero), tail, other_chip).astype(BF16)
            for parcel, (first, count) in enumerate(parcels):
                if i == first + count - 1:
                    these = pl.ds(first, count)
                    remote(
                        cross.at[layer, these], far.at[layer, these],
                        send_sem.at[3], far_recv.at[parcel], "dp", across,
                    )
            own[i] = fold(jnp.where(chip == 0, zero, one), tail, chip)

    def split(block):
        high = block.astype(BF16).astype(F32)
        return [high, block - high]

    def columns_of(parts):
        return jnp.concatenate(parts, axis=0).T.astype(BF16)

    for p in range(mix_pieces):
        send_features(0, p)

    for layer in range(layers):
        squares = jnp.zeros((n_tp * rows, 128), F32)
        scaled = []
        first, count = groups[0]
        for p in range(mix_pieces):
            await_features(layer, p)
            widened = stack_groups([gathered[layer, p, s].astype(F32) for s in range(n_tp)])
            span = pl.ds(p * piece, piece)
            scaled.append((widened * gain[layer, span][None, :]).astype(BF16))
            for lane in range(0, piece, 128):
                tile = widened[:, lane : lane + 128]
                squares = squares + tile * tile
            if p == 0:
                await_bytes(proj.at[layer], proj_sem.at[layer])
            if p == mix_pieces - 1:
                for c in range(2):
                    sq_part[layer, c] = squares[24 * c : 24 * c + 24]
                remote(
                    sq_part.at[layer, other_core], sq_near.at[layer],
                    send_sem.at[1], sq_recv.at[0], "dp", partner,
                )
            for i in range(first, first + count):
                result = jnp.dot(scaled[p], proj[layer, i, span, :], preferred_element_type=F32)
                if p > 0:
                    result = result + product[i]
                if p < mix_pieces - 1:
                    product[i] = result
                else:
                    store_partial(layer, i, result)
        send_group(layer, 0)
        pl.when(core == 0)(functools.partial(cross_first, layer))
        whole_rows = jnp.concatenate(scaled, axis=1)
        for number in range(1, len(groups)):
            first, count = groups[number]
            for i in range(first, first + count):
                store_partial(
                    layer, i, jnp.dot(whole_rows, proj[layer, i], preferred_element_type=F32)
                )
            send_group(layer, number)
        pl.when(core != 0)(functools.partial(cross_first, layer))
        for number in range(1, len(groups)):
            cross_group(layer, number)

        await_bytes(sq_far.at[layer], sq_recv.at[1])
        chip_squares = sq_part[layer, core]
        last = chip_squares[16:] + sq_far[layer, pl.ds(8, 8), :]
        total_squares = jnp.concatenate(
            [
                jnp.where(chip == 0, chip_squares[:8], chip_squares[8:16])
                + sq_far[layer, pl.ds(0, 8), :],
                jnp.where(chip == 0, last, swap(last)),
            ],
            axis=0,
        )
        inverse = lax.rsqrt(jnp.sum(total_squares, axis=1, keepdims=True) / d_model + EPSILON)

        def projected(i):
            for number, (first, count) in enumerate(parcels):
                if i == first:
                    await_bytes(far.at[layer, pl.ds(first, count)], far_recv.at[number])
            return unfold_rows(own[i] + far[layer, i].astype(F32)) * inverse

        if layer == 0:
            await_bytes(state, state_sem)
        logits = projected(0)
        log_sigmoid = jnp.minimum(logits, 0.0) - jnp.log(1.0 + jnp.exp(-jnp.abs(logits)))
        log_decay = log_sigmoid[:rows] / SOFTNESS + offset[:, layer, :]
        decay = jnp.exp(jnp.concatenate([log_decay, jnp.zeros((pad - rows, key_cols), F32)], axis=0))
        query = projected(1)
        read_columns = columns_of(split(query * decay))
        key = projected(2) * head_key ** (-0.5)
        both = query * key
        products = [
            jnp.sum(both[:, h * head_key : (h + 1) * head_key], axis=1, keepdims=True)
            for h in range(heads)
        ]

        for half in range(halves):
            base = half * half_heads
            columns = read_columns[base * head_key : (base + half_heads) * head_key]
            for pair in range(rows // 2):
                factors = jnp.dot(
                    columns, expand[0, pair, pl.ds(0, 2 * pad), :], preferred_element_type=F32
                )
                for k in range(2):
                    b = 2 * pair + k
                    for hh in range(half_heads):
                        factor = factors[
                            hh * head_key : (hh + 1) * head_key,
                            k * value_channels : (k + 1) * value_channels,
                        ]
                        readout[base + hh, pl.ds(b, 1), :] = jnp.sum(
                            factor * state[layer, b, base + hh], axis=0, keepdims=True
                        )
            value = projected(3 + 2 * half)
            gate_all = projected(4 + 2 * half)
            values[:, pl.ds(half * piece, piece)] = value
            gated_heads = []
            for hh in range(half_heads):
                h = base + hh
                span = slice(hh * value_channels, (hh + 1) * value_channels)
                got = readout[h] + products[h] * value[:, span]
                gate = gate_all[:, span]
                normed = got * lax.rsqrt(jnp.mean(got * got, axis=1, keepdims=True) + EPSILON)
                whole = pl.ds(h * value_channels, value_channels)
                normed = normed * out_gain[layer, whole][None, :]
                gated_heads.append(normed * (gate / (1.0 + jnp.exp(-gate))))
            gated = jnp.concatenate(gated_heads, axis=1)
            gated_all[layer, half, dp] = fold(gated[:8], gated[8:], 0).astype(BF16)
            for j in range(1, n_dp):
                remote(
                    gated_all.at[layer, half, dp], gated_all.at[layer, half, dp],
                    send_sem.at[4], gated_recv.at[half],
                    "dp", lax.rem(dp + j, n_dp),
                )

        fresh_columns[...] = columns_of(split(key) + split(decay))
        for pair in range(rows // 2):
            adds = jnp.dot(fresh_columns[...], expand[0, pair], preferred_element_type=F32)
            keeps = jnp.dot(fresh_columns[...], expand[1, pair], preferred_element_type=F32)
            for k in range(2):
                b = 2 * pair + k
                lanes = slice(k * value_channels, (k + 1) * value_channels)
                for h in range(heads):
                    part = slice(h * head_key, (h + 1) * head_key)
                    row = values[pl.ds(b, 1), pl.ds(h * value_channels, value_channels)]
                    new_state_ref[layer, b, h] = (
                        keeps[part, lanes] * state[layer, b, h] + adds[part, lanes] * row
                    )

        if layer == 0:
            await_bytes(wo, wo_sem)
        for half in range(halves):
            await_bytes(gated_all.at[layer, half, pl.ds(0, n_dp - 1)], gated_recv.at[half])
            gated = stack_groups(
                [gated_all[layer, half, s].astype(F32) for s in range(n_dp)]
            ).astype(BF16)
            for p in range(mix_pieces):
                columns = pl.ds(p * piece, piece)
                result = jnp.dot(
                    gated, wo[layer, pl.ds(half * piece, piece), columns],
                    preferred_element_type=F32,
                )
                if half > 0:
                    result = result + mix_part[p]
                if half < halves - 1:
                    mix_part[p] = result
                    continue
                for s in range(n_tp):
                    mix_send[layer, p, s] = group_of(result, s).astype(BF16)
                if layer < layers - 1:
                    send_mixed(layer, p)
                else:
                    send_last(layer, p, last_order[0])

        if layer == layers - 1:
            for to in last_order[1:]:
                for p in range(mix_pieces):
                    send_last(layer, p, to)

        await_feature_sends(layer)
        await_bytes(sq_near.at[layer], send_sem.at[1])
        await_bytes(sq_far.at[layer], send_sem.at[6])
        await_bytes(near.at[layer], send_sem.at[2])
        await_bytes(far.at[layer], send_sem.at[3])
        await_bytes(gated_all.at[layer, :, pl.ds(0, n_dp - 1)], send_sem.at[4])

        if layer + 1 < layers:
            pl.when(is_owner)(functools.partial(finish_middle, layer))
        else:
            for p in range(mix_pieces):
                await_bytes(mix_last.at[p], mix_recv_sem.at[p, 0])
                total = mix_send[layer, p, tp].astype(F32)
                for j in range(n_tp - 1):
                    total = total + mix_last[p, j].astype(F32)
                result = (gathered[layer, p, tp].astype(F32) + total).astype(BF16)
                span = slice(p * piece, (p + 1) * piece)
                hidden_out_ref[:, span] = unfold_rows(result.astype(F32))[:rows].astype(BF16)
        await_mixed_sends(layer)


def store_kernel(hidden_ref, state_ref, hidden_out, state_out, hidden_sem, state_sem):
    layers, rows, heads = state_ref.shape[:3]
    for layer in range(layers):
        for b in range(rows):
            for half in range(2):
                part = (layer, b, pl.ds(half * (heads // 2), heads // 2))
                pltpu.make_async_copy(state_ref.at[part], state_out.at[part], state_sem).start()
    store_hidden = pltpu.make_async_copy(hidden_ref, hidden_out, hidden_sem)
    store_hidden.start()
    store_hidden.wait()
    pltpu.make_async_copy(state_ref, state_out, state_sem).wait()


def fused(
    n_tp, n_dp, hidden_in, input_norm_gain, w_query, w_key, w_decay, w_value, w_gate,
    out_gain, w_out, decay_offset, state,
):
    layers, rows, heads, head_key, value_channels = state.shape
    width = hidden_in.shape[1]
    key_cols, value_cols = w_query.shape[2], w_value.shape[2]
    piece = key_cols
    halves = value_cols // piece
    pieces = 3 + 2 * halves
    mix_pieces = width // piece
    block = (16, piece // 4 * 3)
    vmem = pl.BlockSpec(memory_space=pltpu.VMEM)
    hbm = pl.BlockSpec(memory_space=pl.ANY)
    offsets = decay_offset.transpose(1, 0, 2)
    hidden, fresh = pl.pallas_call(
        functools.partial(
            block_kernel, n_tp, n_dp, width * n_dp, head_key, value_channels, piece
        ),
        out_shape=(
            pltpu.VMEM(hidden_in.shape, BF16),
            pltpu.VMEM(state.shape, F32),
        ),
        in_specs=[hbm] * 11,
        out_specs=(vmem, vmem),
        scratch_shapes=[
            pltpu.VMEM(hidden_in.shape, BF16),
            pltpu.VMEM(input_norm_gain.shape, F32),
            pltpu.VMEM(out_gain.shape, F32),
            pltpu.VMEM(offsets.shape, F32),
            pltpu.VMEM((layers, pieces, width, piece), BF16),
            pltpu.VMEM(w_out.shape, BF16),
            pltpu.VMEM(state.shape, F32),
            pltpu.VMEM((layers, mix_pieces, n_tp) + block, BF16),
            pltpu.VMEM((3, n_tp * rows, piece), F32),
            pltpu.VMEM((layers, 2, pieces, 16, piece // 2 * 3), BF16),
            pltpu.VMEM((layers, pieces, 16, piece // 2 * 3), BF16),
            pltpu.VMEM((pieces,) + block, F32),
            pltpu.VMEM((layers, pieces) + block, BF16),
            pltpu.VMEM((layers, pieces) + block, BF16),
            pltpu.VMEM((layers, 2, 2 * rows, 128), F32),
            pltpu.VMEM((layers, 2 * rows, 128), F32),
            pltpu.VMEM((layers, 16, 128), F32),
            pltpu.VMEM((layers, 16, 128), F32),
            pltpu.VMEM((2, rows // 2, 64, 2 * value_channels), BF16),
            pltpu.VMEM((16, value_cols), F32),
            pltpu.VMEM((key_cols, 64), BF16),
            pltpu.VMEM((heads, 16, value_channels), F32),
            pltpu.VMEM((layers, halves, n_dp) + block, BF16),
            pltpu.VMEM((mix_pieces, n_tp * rows, piece), F32),
            pltpu.VMEM((layers, mix_pieces, n_tp) + block, BF16),
            pltpu.VMEM((layers - 1, mix_pieces, 2, n_tp - 1) + block, BF16),
            pltpu.VMEM((mix_pieces, n_tp - 1) + block, BF16),
            pltpu.SemaphoreType.DMA((4,)),
            pltpu.SemaphoreType.DMA((layers,)),
            pltpu.SemaphoreType.DMA,
            pltpu.SemaphoreType.DMA,
            pltpu.SemaphoreType.DMA((mix_pieces,)),
            pltpu.SemaphoreType.DMA((1 + halves,)),
            pltpu.SemaphoreType.DMA((3 + halves,)),
            pltpu.SemaphoreType.DMA((2,)),
            pltpu.SemaphoreType.DMA((halves,)),
            pltpu.SemaphoreType.DMA((mix_pieces, 2)),
            pltpu.SemaphoreType.DMA((7,)),
        ],
        compiler_params=pltpu.CompilerParams(
            collective_id=0, has_side_effects=True, vmem_limit_bytes=48 * 1024 * 1024
        ),
    )(
        hidden_in, input_norm_gain, out_gain, offsets,
        w_query, w_key, w_decay, w_value, w_gate, w_out, state,
    )
    return pl.pallas_call(
        store_kernel,
        out_shape=(
            jax.ShapeDtypeStruct(hidden_in.shape, BF16),
            jax.ShapeDtypeStruct(state.shape, F32),
        ),
        in_specs=[vmem] * 2,
        out_specs=(hbm, hbm),
        scratch_shapes=[
            pltpu.SemaphoreType.DMA,
            pltpu.SemaphoreType.DMA,
        ],
        compiler_params=pltpu.CompilerParams(vmem_limit_bytes=1024 * 1024),
    )(hidden, fresh)


def plain(
    hidden_in, input_norm_gain, w_query, w_key, w_decay, w_value, w_gate,
    out_gain, w_out, decay_offset, state,
):
    layers, rows, heads, head_key, value_channels = state.shape
    key_cols, value_cols = w_query.shape[2], w_value.shape[2]
    d_model = hidden_in.shape[1] * lax.axis_size("dp")
    first = lax.axis_index("dp") * rows
    current, states = hidden_in, []
    for layer in range(layers):
        widened = lax.all_gather(current, "tp", axis=0, tiled=True).astype(F32)
        squares = lax.psum(jnp.sum(widened * widened, axis=1), "dp")
        scaled = (widened * input_norm_gain[layer][None, :]).astype(BF16)
        partial = jnp.concatenate(
            [
                jnp.dot(scaled, matrix[layer], preferred_element_type=F32)
                for matrix in (w_query, w_key, w_decay, w_value, w_gate)
            ],
            axis=1,
        ).astype(BF16)
        summed = lax.psum_scatter(partial, "dp", scatter_dimension=0, tiled=True).astype(F32)
        own = lax.dynamic_slice_in_dim(squares, first, rows)
        projected = summed * lax.rsqrt(own / d_model + EPSILON)[:, None]
        query, key, logits, value, gate = jnp.split(
            projected,
            [key_cols, 2 * key_cols, 3 * key_cols, 3 * key_cols + value_cols],
            axis=1,
        )
        decay = jnp.exp(jax.nn.log_sigmoid(logits) / SOFTNESS + decay_offset[layer])
        per_key, per_value = (rows, heads, head_key), (rows, heads, value_channels)
        fresh = (
            decay.reshape(per_key)[..., None] * state[layer]
            + (key * head_key ** (-0.5)).reshape(per_key)[..., None]
            * value.reshape(per_value)[:, :, None, :]
        )
        got = jnp.sum(query.reshape(per_key)[..., None] * fresh, axis=2)
        got = got * lax.rsqrt(jnp.mean(got * got, axis=2, keepdims=True) + EPSILON)
        got = got * out_gain[layer].reshape(heads, value_channels)[None]
        gated = (got * jax.nn.silu(gate.reshape(per_value))).reshape(rows, value_cols).astype(BF16)
        mixed = jnp.dot(
            lax.all_gather(gated, "dp", axis=0, tiled=True), w_out[layer],
            preferred_element_type=F32,
        ).astype(BF16)
        mine = lax.psum_scatter(mixed, "tp", scatter_dimension=0, tiled=True).astype(F32)
        current = (current.astype(F32) + mine).astype(BF16)
        states.append(fresh)
    return current, jnp.stack(states)


def solution(mesh):
    n_tp, n_dp = mesh.shape["tp"], mesh.shape["dp"]

    def per_device(hidden_in, *rest):
        state = rest[-1]
        width, key_cols, value_cols = hidden_in.shape[1], rest[1].shape[2], rest[4].shape[2]
        layers, rows, heads = state.shape[:3]
        sized = key_cols == 512 and width % key_cols == 0 and value_cols % key_cols == 0
        shaped = hidden_in.shape[0] == rows == 12 and state.shape[4] == 128
        if n_tp == 4 and n_dp == 4 and layers > 1 and sized and shaped and heads % (value_cols // key_cols) == 0:
            return fused(n_tp, n_dp, hidden_in, *rest)
        return plain(hidden_in, *rest)

    return jax.shard_map(
        per_device,
        mesh=mesh,
        in_specs=(
            P(("grp", "tp"), "dp"),
            P(None, "dp"),
            P(None, "dp", "tp"),
            P(None, "dp", "tp"),
            P(None, "dp", "tp"),
            P(None, "dp", "tp"),
            P(None, "dp", "tp"),
            P(None, "tp"),
            P(None, "tp", "dp"),
            P(None, ("grp", "dp"), "tp"),
            P(None, ("grp", "dp"), "tp", None, None),
        ),
        out_specs=(P(("grp", "tp"), "dp"), P(None, ("grp", "dp"), "tp", None, None)),
        check_vma=False,
    )
```

```python
import functools

import jax
import jax.numpy as jnp
from jax import lax
from jax.experimental import pallas as pl
from jax.experimental.pallas import tpu as pltpu
from jax.sharding import PartitionSpec as P

EPSILON = 1e-06
SOFTNESS = 16.0
F32 = jnp.float32
BF16 = jnp.bfloat16


def swap(tiles):
    return pltpu.roll(tiles, 4, 0)


def first_half(shape):
    return lax.broadcasted_iota(jnp.int32, shape, 0) < 4


def fold(upper, lower, second):
    even = jnp.concatenate([lower[:, :128], lower[:, 256:384]], axis=1)
    odd = jnp.concatenate([lower[:, 128:256], lower[:, 384:]], axis=1)
    top = first_half(even.shape)
    first_form = jnp.where(top, even, swap(odd))
    second_form = jnp.where(top, swap(even), odd)
    if isinstance(second, int):
        folded = second_form if second else first_form
    else:
        folded = jnp.where(second == 1, second_form, first_form)
    return jnp.concatenate(
        [
            jnp.concatenate([upper[:, :256], folded[:, :128]], axis=1),
            jnp.concatenate([upper[:, 256:], folded[:, 128:]], axis=1),
        ],
        axis=0,
    )


def unfold(block):
    upper = jnp.concatenate([block[:8, :256], block[8:, :256]], axis=1)
    left, right = block[:8, 256:], block[8:, 256:]
    lower = jnp.concatenate([left, swap(left), right, swap(right)], axis=1)
    return upper, lower


def unfold_rows(block):
    upper, lower = unfold(block)
    return jnp.concatenate([upper, jnp.where(first_half(lower.shape), lower, 0.0)], axis=0)


def stack_pair(one, two):
    lower = []
    for half in range(2):
        a, b = one[8 * half : 8 * half + 8, 256:], two[8 * half : 8 * half + 8, 256:]
        top = first_half(a.shape)
        lower += [jnp.where(top, a, swap(b)), jnp.where(top, swap(a), b)]
    return jnp.concatenate(
        [
            jnp.concatenate([one[:8, :256], one[8:, :256]], axis=1),
            jnp.concatenate([two[:8, :256], two[8:, :256]], axis=1),
            jnp.concatenate(lower, axis=1),
        ],
        axis=0,
    )


def block_kernel(
    n_tp, n_dp, d_model, head_key, value_channels, piece,
    hidden_hbm, gain_hbm, out_gain_hbm, offset_hbm,
    wq_hbm, wk_hbm, wd_hbm, wv_hbm, wg_hbm, wo_hbm, state_hbm,
    hidden_out_ref, new_state_ref,
    hidden, gain, out_gain, offset, proj, wo, state,
    gathered, product, partial, near, own, cross, far,
    sq_part, sq_near, sq_cross, sq_far,
    expand, values, fresh_columns, readout,
    gated_all, mix_part, mix_send, mix_recv, mix_last,
    small_sem, proj_sem, wo_sem, state_sem,
    gather_recv, near_recv, far_recv, sq_recv, gated_recv, mix_recv_sem, send_sem,
):
    layers, rows, heads = state.shape[0], state.shape[1], state.shape[2]
    pad = 16
    mix_pieces = mix_send.shape[1]
    pieces = proj.shape[1]
    key_cols = heads * head_key
    value_cols = heads * value_channels
    halves = value_cols // piece
    half_heads = heads // halves
    pairs = tuple((3 + 2 * half, 2) for half in range(halves))
    groups = ((0, 3),) + pairs
    parcels = ((0, 1), (1, 1), (2, 1)) + pairs
    tp = lax.axis_index("tp")
    dp = lax.axis_index("dp")
    chip, core = dp // 2, lax.rem(dp, 2)
    other_core = 1 - core
    other_chip = 1 - chip
    partner = 2 * chip + other_core
    across = 2 * other_chip + core
    diagonal = 2 * other_chip + other_core
    mesh_id = pl.DeviceIdType.MESH

    barrier = pltpu.get_barrier_semaphore()
    for j in range(1, n_tp):
        pl.semaphore_signal(
            barrier, inc=1, device_id={"tp": lax.rem(tp + j, n_tp)}, device_id_type=mesh_id
        )
    for j in range(1, n_dp):
        pl.semaphore_signal(
            barrier, inc=1, device_id={"dp": lax.rem(dp + j, n_dp)}, device_id_type=mesh_id
        )

    small = [
        pltpu.make_async_copy(source, target, small_sem.at[index])
        for index, (source, target) in enumerate(
            ((hidden_hbm, hidden), (gain_hbm, gain), (out_gain_hbm, out_gain), (offset_hbm, offset))
        )
    ]

    def load_proj(layer, i):
        if i < 3:
            source = (wd_hbm, wq_hbm, wk_hbm)[i].at[layer]
        else:
            half, which = divmod(i - 3, 2)
            source = (wv_hbm, wg_hbm)[which].at[layer, :, pl.ds(half * piece, piece)]
        return pltpu.make_async_copy(source, proj.at[layer, i], proj_sem.at[layer])

    def load_wo(layer):
        return pltpu.make_async_copy(wo_hbm.at[layer], wo.at[layer], wo_sem)

    def load_state(layer):
        return pltpu.make_async_copy(state_hbm.at[layer], state.at[layer], state_sem)

    for copy in small:
        copy.start()

    row_of = lax.broadcasted_iota(jnp.int32, (4 * pad, 2 * value_channels), 0)
    lane_of = lax.broadcasted_iota(jnp.int32, (4 * pad, 2 * value_channels), 1)
    for second in range(2):
        for pair in range(rows // 2):
            picked = pair * 2 + lane_of // value_channels
            inside = (row_of >= second * 2 * pad) & (row_of < (second + 1) * 2 * pad)
            hit = inside & (lax.rem(row_of, pad) == picked)
            expand[second, pair] = jnp.where(hit, 1.0, 0.0).astype(BF16)

    for copy in small:
        copy.wait()
    for layer in range(layers):
        for i in range(pieces):
            load_proj(layer, i).start()
        load_state(layer).start()
        load_wo(layer).start()

    upper = hidden[pl.ds(0, 8), :].astype(F32)
    lower = hidden[pl.ds(8, 4), :].astype(F32)
    lower = jnp.concatenate([lower, lower], axis=0)
    for p in range(mix_pieces):
        span = slice(p * piece, (p + 1) * piece)
        gathered[0, p, tp] = fold(upper[:, span], lower[:, span], 0).astype(BF16)
    pl.semaphore_wait(barrier, n_tp + n_dp - 2)

    def remote(src, dst, send, recv, axis, target):
        copy = pltpu.make_async_remote_copy(
            src_ref=src, dst_ref=dst, send_sem=send, recv_sem=recv,
            device_id={axis: target}, device_id_type=mesh_id,
        )
        copy.start()

    def await_bytes(ref, sem):
        pltpu.make_async_copy(ref, ref, sem).wait()

    above = tp // 2
    is_owner = (tp == 1) | (tp == 2)

    def tp_step(j):
        return j + above * (n_tp - 2 * j)

    def send_features(layer, p):
        for j in range(n_tp - 1, 0, -1):
            remote(
                gathered.at[layer, p, tp], gathered.at[layer, p, tp],
                send_sem.at[0], gather_recv.at[p],
                "tp", lax.rem(tp + tp_step(j), n_tp),
            )

    def await_features(layer, p):
        if layer == 0:
            await_bytes(gathered.at[layer, p, pl.ds(0, n_tp - 1)], gather_recv.at[p])
            return

        @pl.when(is_owner)
        def _():
            await_bytes(gathered.at[layer, p, pl.ds(0, 2)], gather_recv.at[p])

        @pl.when(jnp.logical_not(is_owner))
        def _():
            await_bytes(gathered.at[layer, p], gather_recv.at[p])

    def await_feature_sends(layer):
        if layer == 0:
            await_bytes(gathered.at[layer, :, pl.ds(0, n_tp - 1)], send_sem.at[0])
            return

        @pl.when(is_owner)
        def _():
            await_bytes(mix_recv.at[layer - 1], send_sem.at[0])

    def gated_pair(layer, half, which):
        return stack_pair(
            gated_all[layer, half, 2 * which].astype(F32),
            gated_all[layer, half, 2 * which + 1].astype(F32),
        ).astype(BF16)

    def mix(layer, p, which, result):
        for k in range(2):
            group = 2 * which + k
            mix_send[layer, p, group] = fold(
                result[8 * k : 8 * k + 8], result[16:], k
            ).astype(BF16)
        for k in range(2):
            group = 2 * which + k
            if layer == layers - 1:
                to = group
                target = mix_last.at[p, lax.rem(tp - to + n_tp - 1, n_tp)]
                arrival = mix_recv_sem.at[p, 0]
            else:
                to = 1 + which
                target = mix_recv.at[layer, p, k, tp - above]
                arrival = mix_recv_sem.at[p, k]

            @pl.when(tp != to)
            def _():
                remote(mix_send.at[layer, p, group], target, send_sem.at[5], arrival, "tp", to)

    def renew(layer, begin, end):
        for pair in range(begin, end):
            adds = jnp.dot(fresh_columns[...], expand[0, pair], preferred_element_type=F32)
            keeps = jnp.dot(fresh_columns[...], expand[1, pair], preferred_element_type=F32)
            for k in range(2):
                b = 2 * pair + k
                lanes = slice(k * value_channels, (k + 1) * value_channels)
                for h in range(heads):
                    part = slice(h * head_key, (h + 1) * head_key)
                    row = values[pl.ds(b, 1), pl.ds(h * value_channels, value_channels)]
                    new_state_ref[layer, b, h] = (
                        keeps[part, lanes] * state[layer, b, h] + adds[part, lanes] * row
                    )

    def await_mixed_sends(layer):
        if layer == layers - 1:
            await_bytes(mix_last, send_sem.at[5])
            return

        @pl.when(is_owner)
        def _():
            await_bytes(mix_send.at[layer, :, pl.ds(0, 2)], send_sem.at[5])

        @pl.when(jnp.logical_not(is_owner))
        def _():
            await_bytes(mix_send.at[layer], send_sem.at[5])

    def finish_middle(layer):
        for p in range(mix_pieces):
            for k in range(2):
                await_bytes(mix_recv.at[layer, p, k], mix_recv_sem.at[p, k])
                mine = 2 * (tp - 1) + k
                total = mix_send[layer, p, mine].astype(F32)
                for j in range(n_tp - 1):
                    total = total + mix_recv[layer, p, k, j].astype(F32)
                gathered[layer + 1, p, mine] = (
                    gathered[layer, p, mine].astype(F32) + total
                ).astype(BF16)
                block = gathered.at[layer + 1, p, mine]
                for to in (3 * (2 - tp), 3 - tp, 3 * (tp - 1)):
                    remote(block, block, send_sem.at[0], gather_recv.at[p], "tp", to)

    def store_partial(layer, i, result):
        for c in range(2):
            block = result[24 * c : 24 * c + 24]
            tail = jnp.concatenate([block[16:, :256], block[16:, 256:]], axis=0)
            partial[layer, c, i] = jnp.concatenate([block[:16], tail], axis=1).astype(BF16)

    def send_group(layer, number):
        these = pl.ds(*groups[number])
        remote(
            partial.at[layer, other_core, these], near.at[layer, these],
            send_sem.at[2], near_recv.at[number], "dp", partner,
        )

    def cross_first(layer):
        await_bytes(sq_near.at[layer], sq_recv.at[0])
        chip_squares = sq_part[layer, core] + sq_near[layer]
        sq_part[layer, core] = chip_squares
        sq_cross[layer] = jnp.concatenate(
            [jnp.where(chip == 0, chip_squares[8:16], chip_squares[:8]), chip_squares[16:]], axis=0
        )
        remote(
            sq_cross.at[layer], sq_far.at[layer], send_sem.at[6], sq_recv.at[1], "dp", across
        )
        cross_group(layer, 0)

    def cross_group(layer, number):
        begin, amount = groups[number]
        await_bytes(near.at[layer, pl.ds(begin, amount)], near_recv.at[number])
        for i in range(begin, begin + amount):
            both = partial[layer, core, i].astype(F32) + near[layer, i].astype(F32)
            tail = jnp.concatenate([both[:8, piece:], both[8:, piece:]], axis=1)
            zero, one = both[:8, :piece], both[8:, :piece]
            cross[layer, i] = fold(jnp.where(chip == 0, one, zero), tail, other_chip).astype(BF16)
            for parcel, (first, count) in enumerate(parcels):
                if i == first + count - 1:
                    these = pl.ds(first, count)
                    remote(
                        cross.at[layer, these], far.at[layer, these],
                        send_sem.at[3], far_recv.at[parcel], "dp", across,
                    )
            own[i] = fold(jnp.where(chip == 0, zero, one), tail, chip)

    def split(block):
        high = block.astype(BF16).astype(F32)
        return [high, block - high]

    def columns_of(parts):
        return jnp.concatenate(parts, axis=0).T.astype(BF16)

    for p in range(mix_pieces):
        send_features(0, p)

    for layer in range(layers):
        squares = jnp.zeros((n_tp * rows, 128), F32)
        scaled = []
        first, count = groups[0]
        for p in range(mix_pieces):
            await_features(layer, p)
            widened = jnp.concatenate(
                [
                    stack_pair(
                        gathered[layer, p, c].astype(F32), gathered[layer, p, 2 + c].astype(F32)
                    )
                    for c in range(2)
                ],
                axis=0,
            )
            span = pl.ds(p * piece, piece)
            scaled.append((widened * gain[layer, span][None, :]).astype(BF16))
            for lane in range(0, piece, 128):
                tile = widened[:, lane : lane + 128]
                squares = squares + tile * tile
            if p == 0:
                await_bytes(proj.at[layer], proj_sem.at[layer])
            if p == mix_pieces - 1:
                for c in range(2):
                    sq_part[layer, c] = squares[24 * c : 24 * c + 24]
                remote(
                    sq_part.at[layer, other_core], sq_near.at[layer],
                    send_sem.at[1], sq_recv.at[0], "dp", partner,
                )
            for i in range(first, first + count):
                result = jnp.dot(scaled[p], proj[layer, i, span, :], preferred_element_type=F32)
                if p > 0:
                    result = result + product[i]
                if p < mix_pieces - 1:
                    product[i] = result
                else:
                    store_partial(layer, i, result)
        send_group(layer, 0)
        pl.when(core == 0)(functools.partial(cross_first, layer))
        whole_rows = jnp.concatenate(scaled, axis=1)
        for number in range(1, len(groups)):
            first, count = groups[number]
            for i in range(first, first + count):
                store_partial(
                    layer, i, jnp.dot(whole_rows, proj[layer, i], preferred_element_type=F32)
                )
            send_group(layer, number)
            pl.when(core == 0)(functools.partial(cross_group, layer, number))

        @pl.when(core != 0)
        def _():
            cross_first(layer)
            for number in range(1, len(groups)):
                cross_group(layer, number)

        await_bytes(sq_far.at[layer], sq_recv.at[1])
        chip_squares = sq_part[layer, core]
        last = chip_squares[16:] + sq_far[layer, pl.ds(8, 8), :]
        total_squares = jnp.concatenate(
            [
                jnp.where(chip == 0, chip_squares[:8], chip_squares[8:16])
                + sq_far[layer, pl.ds(0, 8), :],
                jnp.where(chip == 0, last, swap(last)),
            ],
            axis=0,
        )
        inverse = lax.rsqrt(jnp.sum(total_squares, axis=1, keepdims=True) / d_model + EPSILON)

        def projected(i):
            for number, (first, count) in enumerate(parcels):
                if i == first:
                    await_bytes(far.at[layer, pl.ds(first, count)], far_recv.at[number])
            return unfold_rows(own[i] + far[layer, i].astype(F32)) * inverse

        if layer == 0:
            await_bytes(state, state_sem)
        logits = projected(0)
        log_sigmoid = jnp.minimum(logits, 0.0) - jnp.log(1.0 + jnp.exp(-jnp.abs(logits)))
        log_decay = log_sigmoid[:rows] / SOFTNESS + offset[:, layer, :]
        decay = jnp.exp(jnp.concatenate([log_decay, jnp.zeros((pad - rows, key_cols), F32)], axis=0))
        query = projected(1)
        read_columns = columns_of(split(query * decay))
        key = projected(2) * head_key ** (-0.5)
        both = query * key
        products = [
            jnp.sum(both[:, h * head_key : (h + 1) * head_key], axis=1, keepdims=True)
            for h in range(heads)
        ]

        for half in range(halves):
            base = half * half_heads
            columns = read_columns[base * head_key : (base + half_heads) * head_key]
            for pair in range(rows // 2):
                factors = jnp.dot(
                    columns, expand[0, pair, pl.ds(0, 2 * pad), :], preferred_element_type=F32
                )
                for k in range(2):
                    b = 2 * pair + k
                    for hh in range(half_heads):
                        factor = factors[
                            hh * head_key : (hh + 1) * head_key,
                            k * value_channels : (k + 1) * value_channels,
                        ]
                        readout[base + hh, pl.ds(b, 1), :] = jnp.sum(
                            factor * state[layer, b, base + hh], axis=0, keepdims=True
                        )
            value = projected(3 + 2 * half)
            gate_all = projected(4 + 2 * half)
            values[:, pl.ds(half * piece, piece)] = value
            gated_heads = []
            for hh in range(half_heads):
                h = base + hh
                span = slice(hh * value_channels, (hh + 1) * value_channels)
                got = readout[h] + products[h] * value[:, span]
                gate = gate_all[:, span]
                normed = got * lax.rsqrt(jnp.mean(got * got, axis=1, keepdims=True) + EPSILON)
                whole = pl.ds(h * value_channels, value_channels)
                normed = normed * out_gain[layer, whole][None, :]
                gated_heads.append(normed * (gate / (1.0 + jnp.exp(-gate))))
            gated = jnp.concatenate(gated_heads, axis=1)
            gated_all[layer, half, dp] = fold(gated[:8], gated[8:], 0).astype(BF16)
            block = gated_all.at[layer, half, dp]
            remote(block, block, send_sem.at[4], gated_recv.at[half], "dp", across)
            remote(block, block, send_sem.at[4], gated_recv.at[half], "dp", diagonal)
            remote(block, block, send_sem.at[4], gated_recv.at[halves], "dp", partner)

        fresh_columns[...] = columns_of(split(key) + split(decay))
        first_pairs = rows // 4
        renew(layer, 0, first_pairs)

        if layer == 0:
            await_bytes(wo, wo_sem)
        await_bytes(gated_all.at[layer, :, pl.ds(0, 1)], gated_recv.at[halves])
        gated = jnp.concatenate([gated_pair(layer, half, chip) for half in range(halves)], axis=1)
        for p in range(mix_pieces):
            columns = pl.ds(p * piece, piece)
            mix(layer, p, chip, jnp.dot(gated, wo[layer, :, columns], preferred_element_type=F32))

        for half in range(halves):
            await_bytes(gated_all.at[layer, half, pl.ds(0, 2)], gated_recv.at[half])
            gated = gated_pair(layer, half, other_chip)
            for p in range(mix_pieces):
                columns = pl.ds(p * piece, piece)
                result = jnp.dot(
                    gated, wo[layer, pl.ds(half * piece, piece), columns],
                    preferred_element_type=F32,
                )
                if half > 0:
                    result = result + mix_part[p]
                if half < halves - 1:
                    mix_part[p] = result
                else:
                    mix(layer, p, other_chip, result)
        renew(layer, first_pairs, rows // 2)

        await_feature_sends(layer)
        await_bytes(sq_near.at[layer], send_sem.at[1])
        await_bytes(sq_far.at[layer], send_sem.at[6])
        await_bytes(near.at[layer], send_sem.at[2])
        await_bytes(far.at[layer], send_sem.at[3])
        await_bytes(gated_all.at[layer, :, pl.ds(0, n_dp - 1)], send_sem.at[4])

        if layer + 1 < layers:
            pl.when(is_owner)(functools.partial(finish_middle, layer))
        else:
            for p in range(mix_pieces):
                await_bytes(mix_last.at[p], mix_recv_sem.at[p, 0])
                total = mix_send[layer, p, tp].astype(F32)
                for j in range(n_tp - 1):
                    total = total + mix_last[p, j].astype(F32)
                result = (gathered[layer, p, tp].astype(F32) + total).astype(BF16)
                span = slice(p * piece, (p + 1) * piece)
                hidden_out_ref[:, span] = unfold_rows(result.astype(F32))[:rows].astype(BF16)
        await_mixed_sends(layer)


def store_kernel(hidden_ref, state_ref, hidden_out, state_out, hidden_sem, state_sem):
    layers, rows, heads = state_ref.shape[:3]
    for layer in range(layers):
        for b in range(rows):
            for half in range(2):
                part = (layer, b, pl.ds(half * (heads // 2), heads // 2))
                pltpu.make_async_copy(state_ref.at[part], state_out.at[part], state_sem).start()
    store_hidden = pltpu.make_async_copy(hidden_ref, hidden_out, hidden_sem)
    store_hidden.start()
    store_hidden.wait()
    pltpu.make_async_copy(state_ref, state_out, state_sem).wait()


def fused(
    n_tp, n_dp, hidden_in, input_norm_gain, w_query, w_key, w_decay, w_value, w_gate,
    out_gain, w_out, decay_offset, state,
):
    layers, rows, heads, head_key, value_channels = state.shape
    width = hidden_in.shape[1]
    key_cols, value_cols = w_query.shape[2], w_value.shape[2]
    piece = key_cols
    halves = value_cols // piece
    pieces = 3 + 2 * halves
    mix_pieces = width // piece
    block = (16, piece // 4 * 3)
    vmem = pl.BlockSpec(memory_space=pltpu.VMEM)
    hbm = pl.BlockSpec(memory_space=pl.ANY)
    offsets = decay_offset.transpose(1, 0, 2)
    hidden, fresh = pl.pallas_call(
        functools.partial(
            block_kernel, n_tp, n_dp, width * n_dp, head_key, value_channels, piece
        ),
        out_shape=(
            pltpu.VMEM(hidden_in.shape, BF16),
            pltpu.VMEM(state.shape, F32),
        ),
        in_specs=[hbm] * 11,
        out_specs=(vmem, vmem),
        scratch_shapes=[
            pltpu.VMEM(hidden_in.shape, BF16),
            pltpu.VMEM(input_norm_gain.shape, F32),
            pltpu.VMEM(out_gain.shape, F32),
            pltpu.VMEM(offsets.shape, F32),
            pltpu.VMEM((layers, pieces, width, piece), BF16),
            pltpu.VMEM(w_out.shape, BF16),
            pltpu.VMEM(state.shape, F32),
            pltpu.VMEM((layers, mix_pieces, n_tp) + block, BF16),
            pltpu.VMEM((3, n_tp * rows, piece), F32),
            pltpu.VMEM((layers, 2, pieces, 16, piece // 2 * 3), BF16),
            pltpu.VMEM((layers, pieces, 16, piece // 2 * 3), BF16),
            pltpu.VMEM((pieces,) + block, F32),
            pltpu.VMEM((layers, pieces) + block, BF16),
            pltpu.VMEM((layers, pieces) + block, BF16),
            pltpu.VMEM((layers, 2, 2 * rows, 128), F32),
            pltpu.VMEM((layers, 2 * rows, 128), F32),
            pltpu.VMEM((layers, 16, 128), F32),
            pltpu.VMEM((layers, 16, 128), F32),
            pltpu.VMEM((2, rows // 2, 64, 2 * value_channels), BF16),
            pltpu.VMEM((16, value_cols), F32),
            pltpu.VMEM((key_cols, 64), BF16),
            pltpu.VMEM((heads, 16, value_channels), F32),
            pltpu.VMEM((layers, halves, n_dp) + block, BF16),
            pltpu.VMEM((mix_pieces, 2 * rows, piece), F32),
            pltpu.VMEM((layers, mix_pieces, n_tp) + block, BF16),
            pltpu.VMEM((layers - 1, mix_pieces, 2, n_tp - 1) + block, BF16),
            pltpu.VMEM((mix_pieces, n_tp - 1) + block, BF16),
            pltpu.SemaphoreType.DMA((4,)),
            pltpu.SemaphoreType.DMA((layers,)),
            pltpu.SemaphoreType.DMA,
            pltpu.SemaphoreType.DMA,
            pltpu.SemaphoreType.DMA((mix_pieces,)),
            pltpu.SemaphoreType.DMA((1 + halves,)),
            pltpu.SemaphoreType.DMA((3 + halves,)),
            pltpu.SemaphoreType.DMA((2,)),
            pltpu.SemaphoreType.DMA((halves + 1,)),
            pltpu.SemaphoreType.DMA((mix_pieces, 2)),
            pltpu.SemaphoreType.DMA((7,)),
        ],
        compiler_params=pltpu.CompilerParams(
            collective_id=0, has_side_effects=True, vmem_limit_bytes=48 * 1024 * 1024
        ),
    )(
        hidden_in, input_norm_gain, out_gain, offsets,
        w_query, w_key, w_decay, w_value, w_gate, w_out, state,
    )
    return pl.pallas_call(
        store_kernel,
        out_shape=(
            jax.ShapeDtypeStruct(hidden_in.shape, BF16),
            jax.ShapeDtypeStruct(state.shape, F32),
        ),
        in_specs=[vmem] * 2,
        out_specs=(hbm, hbm),
        scratch_shapes=[
            pltpu.SemaphoreType.DMA,
            pltpu.SemaphoreType.DMA,
        ],
        compiler_params=pltpu.CompilerParams(vmem_limit_bytes=1024 * 1024),
    )(hidden, fresh)


def plain(
    hidden_in, input_norm_gain, w_query, w_key, w_decay, w_value, w_gate,
    out_gain, w_out, decay_offset, state,
):
    layers, rows, heads, head_key, value_channels = state.shape
    key_cols, value_cols = w_query.shape[2], w_value.shape[2]
    d_model = hidden_in.shape[1] * lax.axis_size("dp")
    first = lax.axis_index("dp") * rows
    current, states = hidden_in, []
    for layer in range(layers):
        widened = lax.all_gather(current, "tp", axis=0, tiled=True).astype(F32)
        squares = lax.psum(jnp.sum(widened * widened, axis=1), "dp")
        scaled = (widened * input_norm_gain[layer][None, :]).astype(BF16)
        partial = jnp.concatenate(
            [
                jnp.dot(scaled, matrix[layer], preferred_element_type=F32)
                for matrix in (w_query, w_key, w_decay, w_value, w_gate)
            ],
            axis=1,
        ).astype(BF16)
        summed = lax.psum_scatter(partial, "dp", scatter_dimension=0, tiled=True).astype(F32)
        own = lax.dynamic_slice_in_dim(squares, first, rows)
        projected = summed * lax.rsqrt(own / d_model + EPSILON)[:, None]
        query, key, logits, value, gate = jnp.split(
            projected,
            [key_cols, 2 * key_cols, 3 * key_cols, 3 * key_cols + value_cols],
            axis=1,
        )
        decay = jnp.exp(jax.nn.log_sigmoid(logits) / SOFTNESS + decay_offset[layer])
        per_key, per_value = (rows, heads, head_key), (rows, heads, value_channels)
        fresh = (
            decay.reshape(per_key)[..., None] * state[layer]
            + (key * head_key ** (-0.5)).reshape(per_key)[..., None]
            * value.reshape(per_value)[:, :, None, :]
        )
        got = jnp.sum(query.reshape(per_key)[..., None] * fresh, axis=2)
        got = got * lax.rsqrt(jnp.mean(got * got, axis=2, keepdims=True) + EPSILON)
        got = got * out_gain[layer].reshape(heads, value_channels)[None]
        gated = (got * jax.nn.silu(gate.reshape(per_value))).reshape(rows, value_cols).astype(BF16)
        mixed = jnp.dot(
            lax.all_gather(gated, "dp", axis=0, tiled=True), w_out[layer],
            preferred_element_type=F32,
        ).astype(BF16)
        mine = lax.psum_scatter(mixed, "tp", scatter_dimension=0, tiled=True).astype(F32)
        current = (current.astype(F32) + mine).astype(BF16)
        states.append(fresh)
    return current, jnp.stack(states)


def solution(mesh):
    n_tp, n_dp = mesh.shape["tp"], mesh.shape["dp"]

    def per_device(hidden_in, *rest):
        state = rest[-1]
        width, key_cols, value_cols = hidden_in.shape[1], rest[1].shape[2], rest[4].shape[2]
        layers, rows, heads = state.shape[:3]
        sized = key_cols == 512 and width % key_cols == 0 and value_cols % key_cols == 0
        shaped = hidden_in.shape[0] == rows == 12 and state.shape[4] == 128
        if n_tp == 4 and n_dp == 4 and layers > 1 and sized and shaped and heads % (value_cols // key_cols) == 0:
            return fused(n_tp, n_dp, hidden_in, *rest)
        return plain(hidden_in, *rest)

    return jax.shard_map(
        per_device,
        mesh=mesh,
        in_specs=(
            P(("grp", "tp"), "dp"),
            P(None, "dp"),
            P(None, "dp", "tp"),
            P(None, "dp", "tp"),
            P(None, "dp", "tp"),
            P(None, "dp", "tp"),
            P(None, "dp", "tp"),
            P(None, "tp"),
            P(None, "tp", "dp"),
            P(None, ("grp", "dp"), "tp"),
            P(None, ("grp", "dp"), "tp", None, None),
        ),
        out_specs=(P(("grp", "tp"), "dp"), P(None, ("grp", "dp"), "tp", None, None)),
        check_vma=False,
    )
```

```python
import functools

import jax
import jax.numpy as jnp
from jax import lax
from jax.experimental import pallas as pl
from jax.experimental.pallas import tpu as pltpu
from jax.sharding import PartitionSpec as P

EPSILON = 1e-06
SOFTNESS = 16.0
F32 = jnp.float32
BF16 = jnp.bfloat16


def swap(tiles):
    return pltpu.roll(tiles, 4, 0)


def first_half(shape):
    return lax.broadcasted_iota(jnp.int32, shape, 0) < 4


def fold(upper, lower, second):
    even = jnp.concatenate([lower[:, :128], lower[:, 256:384]], axis=1)
    odd = jnp.concatenate([lower[:, 128:256], lower[:, 384:]], axis=1)
    top = first_half(even.shape)
    first_form = jnp.where(top, even, swap(odd))
    second_form = jnp.where(top, swap(even), odd)
    if isinstance(second, int):
        folded = second_form if second else first_form
    else:
        folded = jnp.where(second == 1, second_form, first_form)
    return jnp.concatenate(
        [
            jnp.concatenate([upper[:, :256], folded[:, :128]], axis=1),
            jnp.concatenate([upper[:, 256:], folded[:, 128:]], axis=1),
        ],
        axis=0,
    )


def unfold(block):
    upper = jnp.concatenate([block[:8, :256], block[8:, :256]], axis=1)
    left, right = block[:8, 256:], block[8:, 256:]
    lower = jnp.concatenate([left, swap(left), right, swap(right)], axis=1)
    return upper, lower


def unfold_rows(block):
    upper, lower = unfold(block)
    return jnp.concatenate([upper, jnp.where(first_half(lower.shape), lower, 0.0)], axis=0)


def stack_pair(one, two):
    lower = []
    for half in range(2):
        a, b = one[8 * half : 8 * half + 8, 256:], two[8 * half : 8 * half + 8, 256:]
        top = first_half(a.shape)
        lower += [jnp.where(top, a, swap(b)), jnp.where(top, swap(a), b)]
    return jnp.concatenate(
        [
            jnp.concatenate([one[:8, :256], one[8:, :256]], axis=1),
            jnp.concatenate([two[:8, :256], two[8:, :256]], axis=1),
            jnp.concatenate(lower, axis=1),
        ],
        axis=0,
    )


def block_kernel(
    n_tp, n_dp, d_model, head_key, value_channels, piece,
    hidden_hbm, gain_hbm, out_gain_hbm, offset_hbm,
    wq_hbm, wk_hbm, wd_hbm, wv_hbm, wg_hbm, wo_hbm, state_hbm,
    hidden_out_ref, new_state_ref,
    hidden, gain, out_gain, offset, proj, wo, state,
    gathered, product, partial, near, own, cross, far, direct, far_direct,
    sq_part, sq_near, sq_cross, sq_far,
    expand, values, fresh_columns, readout,
    gated_all, mix_part, mix_send, mix_recv, mix_last,
    small_sem, proj_sem, wo_sem, state_sem,
    gather_recv, near_recv, far_recv, sq_recv, gated_recv, mix_recv_sem, direct_recv, send_sem,
):
    layers, rows, heads = state.shape[0], state.shape[1], state.shape[2]
    pad = 16
    mix_pieces = mix_send.shape[1]
    pieces = proj.shape[1]
    key_cols = heads * head_key
    value_cols = heads * value_channels
    halves = value_cols // piece
    half_heads = heads // halves
    pairs = tuple((3 + 2 * half, 2) for half in range(halves))
    groups = ((0, 3),) + pairs
    tp = lax.axis_index("tp")
    dp = lax.axis_index("dp")
    chip, core = dp // 2, lax.rem(dp, 2)
    other_core = 1 - core
    other_chip = 1 - chip
    partner = 2 * chip + other_core
    across = 2 * other_chip + core
    diagonal = 2 * other_chip + other_core
    mesh_id = pl.DeviceIdType.MESH

    barrier = pltpu.get_barrier_semaphore()
    for j in range(1, n_tp):
        pl.semaphore_signal(
            barrier, inc=1, device_id={"tp": lax.rem(tp + j, n_tp)}, device_id_type=mesh_id
        )
    for j in range(1, n_dp):
        pl.semaphore_signal(
            barrier, inc=1, device_id={"dp": lax.rem(dp + j, n_dp)}, device_id_type=mesh_id
        )

    small = [
        pltpu.make_async_copy(source, target, small_sem.at[index])
        for index, (source, target) in enumerate(
            ((hidden_hbm, hidden), (gain_hbm, gain), (out_gain_hbm, out_gain), (offset_hbm, offset))
        )
    ]

    def load_proj(layer, i):
        if i < 3:
            source = (wd_hbm, wq_hbm, wk_hbm)[i].at[layer]
        else:
            half, which = divmod(i - 3, 2)
            source = (wv_hbm, wg_hbm)[which].at[layer, :, pl.ds(half * piece, piece)]
        return pltpu.make_async_copy(source, proj.at[layer, i], proj_sem.at[layer])

    def load_wo(layer):
        return pltpu.make_async_copy(wo_hbm.at[layer], wo.at[layer], wo_sem)

    def load_state(layer):
        return pltpu.make_async_copy(state_hbm.at[layer], state.at[layer], state_sem)

    for copy in small:
        copy.start()

    @pl.when(core == 0)
    def _():
        far_direct[...] = jnp.zeros_like(far_direct)

    row_of = lax.broadcasted_iota(jnp.int32, (4 * pad, 2 * value_channels), 0)
    lane_of = lax.broadcasted_iota(jnp.int32, (4 * pad, 2 * value_channels), 1)
    for second in range(2):
        for pair in range(rows // 2):
            picked = pair * 2 + lane_of // value_channels
            inside = (row_of >= second * 2 * pad) & (row_of < (second + 1) * 2 * pad)
            hit = inside & (lax.rem(row_of, pad) == picked)
            expand[second, pair] = jnp.where(hit, 1.0, 0.0).astype(BF16)

    for copy in small:
        copy.wait()
    for layer in range(layers):
        for i in range(pieces):
            load_proj(layer, i).start()
        load_state(layer).start()
        load_wo(layer).start()

    upper = hidden[pl.ds(0, 8), :].astype(F32)
    lower = hidden[pl.ds(8, 4), :].astype(F32)
    lower = jnp.concatenate([lower, lower], axis=0)
    for p in range(mix_pieces):
        span = slice(p * piece, (p + 1) * piece)
        gathered[0, p, tp] = fold(upper[:, span], lower[:, span], 0).astype(BF16)
    pl.semaphore_wait(barrier, n_tp + n_dp - 2)

    def remote(src, dst, send, recv, axis, target):
        copy = pltpu.make_async_remote_copy(
            src_ref=src, dst_ref=dst, send_sem=send, recv_sem=recv,
            device_id={axis: target}, device_id_type=mesh_id,
        )
        copy.start()

    def await_bytes(ref, sem):
        pltpu.make_async_copy(ref, ref, sem).wait()

    above = tp // 2
    is_owner = (tp == 1) | (tp == 2)

    def tp_step(j):
        return j + above * (n_tp - 2 * j)

    def send_features(layer, p):
        for j in range(n_tp - 1, 0, -1):
            remote(
                gathered.at[layer, p, tp], gathered.at[layer, p, tp],
                send_sem.at[0], gather_recv.at[p],
                "tp", lax.rem(tp + tp_step(j), n_tp),
            )

    def await_features(layer, p):
        if layer == 0:
            await_bytes(gathered.at[layer, p, pl.ds(0, n_tp - 1)], gather_recv.at[p])
            return

        @pl.when(is_owner)
        def _():
            await_bytes(gathered.at[layer, p, pl.ds(0, 2)], gather_recv.at[p])

        @pl.when(jnp.logical_not(is_owner))
        def _():
            await_bytes(gathered.at[layer, p], gather_recv.at[p])

    def await_feature_sends(layer):
        if layer == 0:
            await_bytes(gathered.at[layer, :, pl.ds(0, n_tp - 1)], send_sem.at[0])
            return

        @pl.when(is_owner)
        def _():
            await_bytes(mix_recv.at[layer - 1], send_sem.at[0])

    def gated_pair(layer, half, which):
        return stack_pair(
            gated_all[layer, half, 2 * which].astype(F32),
            gated_all[layer, half, 2 * which + 1].astype(F32),
        ).astype(BF16)

    def mix(layer, p, which, result):
        for k in range(2):
            group = 2 * which + k
            mix_send[layer, p, group] = fold(
                result[8 * k : 8 * k + 8], result[16:], k
            ).astype(BF16)
        for k in range(2):
            group = 2 * which + k
            if layer == layers - 1:
                continue
            to = 1 + which

            @pl.when(tp != to)
            def _():
                remote(
                    mix_send.at[layer, p, group], mix_recv.at[layer, p, k, tp - above],
                    send_sem.at[5], mix_recv_sem.at[p, k], "tp", to,
                )

    def send_last(layer, which):
        for k in range(2):
            to = 2 * which + k

            @pl.when(tp != to)
            def _():
                for p in range(mix_pieces):
                    remote(
                        mix_send.at[layer, p, to],
                        mix_last.at[p, lax.rem(tp - to + n_tp - 1, n_tp)],
                        send_sem.at[5], mix_recv_sem.at[p, 0], "tp", to,
                    )

    def project_out(layer, which, arrivals, senders):
        for half in range(halves):
            await_bytes(
                gated_all.at[layer, half, pl.ds(0, senders)], gated_recv.at[arrivals + half]
            )
            gated = gated_pair(layer, half, which)
            for p in range(mix_pieces):
                columns = pl.ds(p * piece, piece)
                result = jnp.dot(
                    gated, wo[layer, pl.ds(half * piece, piece), columns],
                    preferred_element_type=F32,
                )
                if half > 0:
                    result = result + mix_part[p]
                if half < halves - 1:
                    mix_part[p] = result
                else:
                    mix(layer, p, which, result)

    def renew(layer, begin, end):
        for pair in range(begin, end):
            adds = jnp.dot(fresh_columns[...], expand[0, pair], preferred_element_type=F32)
            keeps = jnp.dot(fresh_columns[...], expand[1, pair], preferred_element_type=F32)
            for k in range(2):
                b = 2 * pair + k
                lanes = slice(k * value_channels, (k + 1) * value_channels)
                for h in range(heads):
                    part = slice(h * head_key, (h + 1) * head_key)
                    row = values[pl.ds(b, 1), pl.ds(h * value_channels, value_channels)]
                    new_state_ref[layer, b, h] = (
                        keeps[part, lanes] * state[layer, b, h] + adds[part, lanes] * row
                    )

    def await_mixed_sends(layer):
        if layer == layers - 1:
            await_bytes(mix_last, send_sem.at[5])
            return

        @pl.when(is_owner)
        def _():
            await_bytes(mix_send.at[layer, :, pl.ds(0, 2)], send_sem.at[5])

        @pl.when(jnp.logical_not(is_owner))
        def _():
            await_bytes(mix_send.at[layer], send_sem.at[5])

    def finish_middle(layer):
        for p in range(mix_pieces):
            for k in range(2):
                await_bytes(mix_recv.at[layer, p, k], mix_recv_sem.at[p, k])
                mine = 2 * (tp - 1) + k
                total = mix_send[layer, p, mine].astype(F32)
                for j in range(n_tp - 1):
                    total = total + mix_recv[layer, p, k, j].astype(F32)
                gathered[layer + 1, p, mine] = (
                    gathered[layer, p, mine].astype(F32) + total
                ).astype(BF16)
                block = gathered.at[layer + 1, p, mine]
                for to in (3 * (2 - tp), 3 - tp, 3 * (tp - 1)):
                    remote(block, block, send_sem.at[0], gather_recv.at[p], "tp", to)

    def store_partial(layer, i, result):
        for c in range(2):
            block = result[24 * c : 24 * c + 24]
            tail = jnp.concatenate([block[16:, :256], block[16:, 256:]], axis=0)
            partial[layer, c, i] = jnp.concatenate([block[:16], tail], axis=1).astype(BF16)

    def send_group(layer, number):
        these = pl.ds(*groups[number])
        remote(
            partial.at[layer, other_core, these], near.at[layer, these],
            send_sem.at[2], near_recv.at[number], "dp", partner,
        )

    def halves_of(block):
        tail = jnp.concatenate([block[:8, piece:], block[8:, piece:]], axis=1)
        return block[:8, :piece], block[8:, :piece], tail

    def of_other_chip(block):
        zero, one, tail = halves_of(block)
        return fold(jnp.where(chip == 0, one, zero), tail, other_chip).astype(BF16)

    def of_this_chip(block):
        zero, one, tail = halves_of(block)
        return fold(jnp.where(chip == 0, zero, one), tail, chip)

    def chip_sum(layer, i):
        return partial[layer, core, i].astype(F32) + near[layer, i].astype(F32)

    def send_cross(layer, number):
        these = pl.ds(*groups[number])
        remote(
            cross.at[layer, these], far.at[layer, these],
            send_sem.at[3], far_recv.at[number], "dp", across,
        )

    def cross_squares(layer):
        await_bytes(sq_near.at[layer], sq_recv.at[0])
        chip_squares = sq_part[layer, core] + sq_near[layer]
        sq_part[layer, core] = chip_squares
        sq_cross[layer] = jnp.concatenate(
            [jnp.where(chip == 0, chip_squares[8:16], chip_squares[:8]), chip_squares[16:]], axis=0
        )
        remote(
            sq_cross.at[layer], sq_far.at[layer], send_sem.at[6], sq_recv.at[1], "dp", across
        )

    def first_of_core_0(layer):
        cross_squares(layer)
        begin, amount = groups[0]
        await_bytes(near.at[layer, pl.ds(begin, amount)], near_recv.at[0])
        for i in range(begin, begin + amount):
            cross[layer, i] = of_other_chip(chip_sum(layer, i))
        send_cross(layer, 0)
        for i in range(begin, begin + amount):
            direct[layer, i] = of_other_chip(partial[layer, 1, i].astype(F32))
        remote(
            direct.at[layer], far_direct.at[layer],
            send_sem.at[7], direct_recv, "dp", diagonal,
        )
        for i in range(begin, begin + amount):
            own[i] = of_this_chip(chip_sum(layer, i))

    def send_direct_of_core_1(layer):
        begin, amount = groups[0]
        for i in range(begin, begin + amount):
            cross[layer, i] = of_other_chip(partial[layer, 1, i].astype(F32))
        send_cross(layer, 0)

    def first_of_core_1(layer):
        cross_squares(layer)
        begin, amount = groups[0]
        await_bytes(near.at[layer, pl.ds(begin, amount)], near_recv.at[0])
        for i in range(begin, begin + amount):
            own[i] = of_this_chip(chip_sum(layer, i))

    def cross_group(layer, number):
        begin, amount = groups[number]
        await_bytes(near.at[layer, pl.ds(begin, amount)], near_recv.at[number])
        for i in range(begin, begin + amount):
            cross[layer, i] = of_other_chip(chip_sum(layer, i))
        send_cross(layer, number)
        for i in range(begin, begin + amount):
            own[i] = of_this_chip(chip_sum(layer, i))

    def split(block):
        high = block.astype(BF16).astype(F32)
        return [high, block - high]

    def columns_of(parts):
        return jnp.concatenate(parts, axis=0).T.astype(BF16)

    for p in range(mix_pieces):
        send_features(0, p)

    for layer in range(layers):
        squares = jnp.zeros((n_tp * rows, 128), F32)
        scaled = []
        first, count = groups[0]
        for p in range(mix_pieces):
            await_features(layer, p)
            widened = jnp.concatenate(
                [
                    stack_pair(
                        gathered[layer, p, c].astype(F32), gathered[layer, p, 2 + c].astype(F32)
                    )
                    for c in range(2)
                ],
                axis=0,
            )
            span = pl.ds(p * piece, piece)
            scaled.append((widened * gain[layer, span][None, :]).astype(BF16))
            for lane in range(0, piece, 128):
                tile = widened[:, lane : lane + 128]
                squares = squares + tile * tile
            if p == 0:
                await_bytes(proj.at[layer], proj_sem.at[layer])
            if p == mix_pieces - 1:
                for c in range(2):
                    sq_part[layer, c] = squares[24 * c : 24 * c + 24]
                remote(
                    sq_part.at[layer, other_core], sq_near.at[layer],
                    send_sem.at[1], sq_recv.at[0], "dp", partner,
                )
            for i in range(first, first + count):
                result = jnp.dot(scaled[p], proj[layer, i, span, :], preferred_element_type=F32)
                if p > 0:
                    result = result + product[i]
                if p < mix_pieces - 1:
                    product[i] = result
                else:
                    store_partial(layer, i, result)
        send_group(layer, 0)
        pl.when(core == 0)(functools.partial(first_of_core_0, layer))
        pl.when(core != 0)(functools.partial(send_direct_of_core_1, layer))
        whole_rows = jnp.concatenate(scaled, axis=1)
        for number in range(1, len(groups)):
            first, count = groups[number]
            for i in range(first, first + count):
                store_partial(
                    layer, i, jnp.dot(whole_rows, proj[layer, i], preferred_element_type=F32)
                )
            send_group(layer, number)
            pl.when(core == 0)(functools.partial(cross_group, layer, number))

        @pl.when(core != 0)
        def _():
            first_of_core_1(layer)
            for number in range(1, len(groups)):
                cross_group(layer, number)

        await_bytes(sq_far.at[layer], sq_recv.at[1])
        chip_squares = sq_part[layer, core]
        last = chip_squares[16:] + sq_far[layer, pl.ds(8, 8), :]
        total_squares = jnp.concatenate(
            [
                jnp.where(chip == 0, chip_squares[:8], chip_squares[8:16])
                + sq_far[layer, pl.ds(0, 8), :],
                jnp.where(chip == 0, last, swap(last)),
            ],
            axis=0,
        )
        inverse = lax.rsqrt(jnp.sum(total_squares, axis=1, keepdims=True) / d_model + EPSILON)

        def projected(i):
            for number, (first, count) in enumerate(groups):
                if i == first:
                    await_bytes(far.at[layer, pl.ds(first, count)], far_recv.at[number])
            total = own[i] + far[layer, i].astype(F32)
            if i < groups[0][1]:
                total = total + far_direct[layer, i].astype(F32)
            return unfold_rows(total) * inverse

        if layer == 0:
            await_bytes(state, state_sem)

        @pl.when(core != 0)
        def _():
            await_bytes(far_direct.at[layer], direct_recv)

        logits = projected(0)
        log_sigmoid = jnp.minimum(logits, 0.0) - jnp.log(1.0 + jnp.exp(-jnp.abs(logits)))
        log_decay = log_sigmoid[:rows] / SOFTNESS + offset[:, layer, :]
        decay = jnp.exp(jnp.concatenate([log_decay, jnp.zeros((pad - rows, key_cols), F32)], axis=0))
        query = projected(1)
        read_columns = columns_of(split(query * decay))
        key = projected(2) * head_key ** (-0.5)
        both = query * key
        products = [
            jnp.sum(both[:, h * head_key : (h + 1) * head_key], axis=1, keepdims=True)
            for h in range(heads)
        ]

        for half in range(halves):
            base = half * half_heads
            columns = read_columns[base * head_key : (base + half_heads) * head_key]
            for pair in range(rows // 2):
                factors = jnp.dot(
                    columns, expand[0, pair, pl.ds(0, 2 * pad), :], preferred_element_type=F32
                )
                for k in range(2):
                    b = 2 * pair + k
                    for hh in range(half_heads):
                        factor = factors[
                            hh * head_key : (hh + 1) * head_key,
                            k * value_channels : (k + 1) * value_channels,
                        ]
                        readout[base + hh, pl.ds(b, 1), :] = jnp.sum(
                            factor * state[layer, b, base + hh], axis=0, keepdims=True
                        )
            value = projected(3 + 2 * half)
            gate_all = projected(4 + 2 * half)
            values[:, pl.ds(half * piece, piece)] = value
            gated_heads = []
            for hh in range(half_heads):
                h = base + hh
                span = slice(hh * value_channels, (hh + 1) * value_channels)
                got = readout[h] + products[h] * value[:, span]
                gate = gate_all[:, span]
                normed = got * lax.rsqrt(jnp.mean(got * got, axis=1, keepdims=True) + EPSILON)
                whole = pl.ds(h * value_channels, value_channels)
                normed = normed * out_gain[layer, whole][None, :]
                gated_heads.append(normed * (gate / (1.0 + jnp.exp(-gate))))
            gated = jnp.concatenate(gated_heads, axis=1)
            gated_all[layer, half, dp] = fold(gated[:8], gated[8:], 0).astype(BF16)
            block = gated_all.at[layer, half, dp]
            remote(block, block, send_sem.at[4], gated_recv.at[half], "dp", across)
            remote(block, block, send_sem.at[4], gated_recv.at[half], "dp", diagonal)
            remote(block, block, send_sem.at[4], gated_recv.at[halves + half], "dp", partner)

        fresh_columns[...] = columns_of(split(key) + split(decay))
        first_pairs = rows // 4
        renew(layer, 0, first_pairs)

        if layer == 0:
            await_bytes(wo, wo_sem)
        project_out(layer, chip, halves, 1)
        if layer == layers - 1:
            send_last(layer, chip)
        project_out(layer, other_chip, 0, 2)
        if layer == layers - 1:
            send_last(layer, other_chip)
        renew(layer, first_pairs, rows // 2)

        await_feature_sends(layer)
        await_bytes(sq_near.at[layer], send_sem.at[1])
        await_bytes(sq_far.at[layer], send_sem.at[6])
        await_bytes(near.at[layer], send_sem.at[2])
        await_bytes(far.at[layer], send_sem.at[3])

        @pl.when(core == 0)
        def _():
            await_bytes(direct.at[layer], send_sem.at[7])

        await_bytes(gated_all.at[layer, :, pl.ds(0, n_dp - 1)], send_sem.at[4])

        if layer + 1 < layers:
            pl.when(is_owner)(functools.partial(finish_middle, layer))
        else:
            for p in range(mix_pieces):
                await_bytes(mix_last.at[p], mix_recv_sem.at[p, 0])
                total = mix_send[layer, p, tp].astype(F32)
                for j in range(n_tp - 1):
                    total = total + mix_last[p, j].astype(F32)
                result = (gathered[layer, p, tp].astype(F32) + total).astype(BF16)
                span = slice(p * piece, (p + 1) * piece)
                hidden_out_ref[:, span] = unfold_rows(result.astype(F32))[:rows].astype(BF16)
        await_mixed_sends(layer)


def store_kernel(hidden_ref, state_ref, hidden_out, state_out, hidden_sem, state_sem):
    layers, rows, heads = state_ref.shape[:3]
    for layer in range(layers):
        for b in range(rows):
            for half in range(2):
                part = (layer, b, pl.ds(half * (heads // 2), heads // 2))
                pltpu.make_async_copy(state_ref.at[part], state_out.at[part], state_sem).start()
    store_hidden = pltpu.make_async_copy(hidden_ref, hidden_out, hidden_sem)
    store_hidden.start()
    store_hidden.wait()
    pltpu.make_async_copy(state_ref, state_out, state_sem).wait()


def fused(
    n_tp, n_dp, hidden_in, input_norm_gain, w_query, w_key, w_decay, w_value, w_gate,
    out_gain, w_out, decay_offset, state,
):
    layers, rows, heads, head_key, value_channels = state.shape
    width = hidden_in.shape[1]
    key_cols, value_cols = w_query.shape[2], w_value.shape[2]
    piece = key_cols
    halves = value_cols // piece
    pieces = 3 + 2 * halves
    mix_pieces = width // piece
    block = (16, piece // 4 * 3)
    vmem = pl.BlockSpec(memory_space=pltpu.VMEM)
    hbm = pl.BlockSpec(memory_space=pl.ANY)
    offsets = decay_offset.transpose(1, 0, 2)
    hidden, fresh = pl.pallas_call(
        functools.partial(
            block_kernel, n_tp, n_dp, width * n_dp, head_key, value_channels, piece
        ),
        out_shape=(
            pltpu.VMEM(hidden_in.shape, BF16),
            pltpu.VMEM(state.shape, F32),
        ),
        in_specs=[hbm] * 11,
        out_specs=(vmem, vmem),
        scratch_shapes=[
            pltpu.VMEM(hidden_in.shape, BF16),
            pltpu.VMEM(input_norm_gain.shape, F32),
            pltpu.VMEM(out_gain.shape, F32),
            pltpu.VMEM(offsets.shape, F32),
            pltpu.VMEM((layers, pieces, width, piece), BF16),
            pltpu.VMEM(w_out.shape, BF16),
            pltpu.VMEM(state.shape, F32),
            pltpu.VMEM((layers, mix_pieces, n_tp) + block, BF16),
            pltpu.VMEM((3, n_tp * rows, piece), F32),
            pltpu.VMEM((layers, 2, pieces, 16, piece // 2 * 3), BF16),
            pltpu.VMEM((layers, pieces, 16, piece // 2 * 3), BF16),
            pltpu.VMEM((pieces,) + block, F32),
            pltpu.VMEM((layers, pieces) + block, BF16),
            pltpu.VMEM((layers, pieces) + block, BF16),
            pltpu.VMEM((layers, 3) + block, BF16),
            pltpu.VMEM((layers, 3) + block, BF16),
            pltpu.VMEM((layers, 2, 2 * rows, 128), F32),
            pltpu.VMEM((layers, 2 * rows, 128), F32),
            pltpu.VMEM((layers, 16, 128), F32),
            pltpu.VMEM((layers, 16, 128), F32),
            pltpu.VMEM((2, rows // 2, 64, 2 * value_channels), BF16),
            pltpu.VMEM((16, value_cols), F32),
            pltpu.VMEM((key_cols, 64), BF16),
            pltpu.VMEM((heads, 16, value_channels), F32),
            pltpu.VMEM((layers, halves, n_dp) + block, BF16),
            pltpu.VMEM((mix_pieces, 2 * rows, piece), F32),
            pltpu.VMEM((layers, mix_pieces, n_tp) + block, BF16),
            pltpu.VMEM((layers - 1, mix_pieces, 2, n_tp - 1) + block, BF16),
            pltpu.VMEM((mix_pieces, n_tp - 1) + block, BF16),
            pltpu.SemaphoreType.DMA((4,)),
            pltpu.SemaphoreType.DMA((layers,)),
            pltpu.SemaphoreType.DMA,
            pltpu.SemaphoreType.DMA,
            pltpu.SemaphoreType.DMA((mix_pieces,)),
            pltpu.SemaphoreType.DMA((1 + halves,)),
            pltpu.SemaphoreType.DMA((1 + halves,)),
            pltpu.SemaphoreType.DMA((2,)),
            pltpu.SemaphoreType.DMA((2 * halves,)),
            pltpu.SemaphoreType.DMA((mix_pieces, 2)),
            pltpu.SemaphoreType.DMA,
            pltpu.SemaphoreType.DMA((8,)),
        ],
        compiler_params=pltpu.CompilerParams(
            collective_id=0, has_side_effects=True, vmem_limit_bytes=48 * 1024 * 1024
        ),
    )(
        hidden_in, input_norm_gain, out_gain, offsets,
        w_query, w_key, w_decay, w_value, w_gate, w_out, state,
    )
    return pl.pallas_call(
        store_kernel,
        out_shape=(
            jax.ShapeDtypeStruct(hidden_in.shape, BF16),
            jax.ShapeDtypeStruct(state.shape, F32),
        ),
        in_specs=[vmem] * 2,
        out_specs=(hbm, hbm),
        scratch_shapes=[
            pltpu.SemaphoreType.DMA,
            pltpu.SemaphoreType.DMA,
        ],
        compiler_params=pltpu.CompilerParams(vmem_limit_bytes=1024 * 1024),
    )(hidden, fresh)


def plain(
    hidden_in, input_norm_gain, w_query, w_key, w_decay, w_value, w_gate,
    out_gain, w_out, decay_offset, state,
):
    layers, rows, heads, head_key, value_channels = state.shape
    key_cols, value_cols = w_query.shape[2], w_value.shape[2]
    d_model = hidden_in.shape[1] * lax.axis_size("dp")
    first = lax.axis_index("dp") * rows
    current, states = hidden_in, []
    for layer in range(layers):
        widened = lax.all_gather(current, "tp", axis=0, tiled=True).astype(F32)
        squares = lax.psum(jnp.sum(widened * widened, axis=1), "dp")
        scaled = (widened * input_norm_gain[layer][None, :]).astype(BF16)
        partial = jnp.concatenate(
            [
                jnp.dot(scaled, matrix[layer], preferred_element_type=F32)
                for matrix in (w_query, w_key, w_decay, w_value, w_gate)
            ],
            axis=1,
        ).astype(BF16)
        summed = lax.psum_scatter(partial, "dp", scatter_dimension=0, tiled=True).astype(F32)
        own = lax.dynamic_slice_in_dim(squares, first, rows)
        projected = summed * lax.rsqrt(own / d_model + EPSILON)[:, None]
        query, key, logits, value, gate = jnp.split(
            projected,
            [key_cols, 2 * key_cols, 3 * key_cols, 3 * key_cols + value_cols],
            axis=1,
        )
        decay = jnp.exp(jax.nn.log_sigmoid(logits) / SOFTNESS + decay_offset[layer])
        per_key, per_value = (rows, heads, head_key), (rows, heads, value_channels)
        fresh = (
            decay.reshape(per_key)[..., None] * state[layer]
            + (key * head_key ** (-0.5)).reshape(per_key)[..., None]
            * value.reshape(per_value)[:, :, None, :]
        )
        got = jnp.sum(query.reshape(per_key)[..., None] * fresh, axis=2)
        got = got * lax.rsqrt(jnp.mean(got * got, axis=2, keepdims=True) + EPSILON)
        got = got * out_gain[layer].reshape(heads, value_channels)[None]
        gated = (got * jax.nn.silu(gate.reshape(per_value))).reshape(rows, value_cols).astype(BF16)
        mixed = jnp.dot(
            lax.all_gather(gated, "dp", axis=0, tiled=True), w_out[layer],
            preferred_element_type=F32,
        ).astype(BF16)
        mine = lax.psum_scatter(mixed, "tp", scatter_dimension=0, tiled=True).astype(F32)
        current = (current.astype(F32) + mine).astype(BF16)
        states.append(fresh)
    return current, jnp.stack(states)


def solution(mesh):
    n_tp, n_dp = mesh.shape["tp"], mesh.shape["dp"]

    def per_device(hidden_in, *rest):
        state = rest[-1]
        width, key_cols, value_cols = hidden_in.shape[1], rest[1].shape[2], rest[4].shape[2]
        layers, rows, heads = state.shape[:3]
        sized = key_cols == 512 and width % key_cols == 0 and value_cols % key_cols == 0
        shaped = hidden_in.shape[0] == rows == 12 and state.shape[4] == 128
        if n_tp == 4 and n_dp == 4 and layers > 1 and sized and shaped and heads % (value_cols // key_cols) == 0:
            return fused(n_tp, n_dp, hidden_in, *rest)
        return plain(hidden_in, *rest)

    return jax.shard_map(
        per_device,
        mesh=mesh,
        in_specs=(
            P(("grp", "tp"), "dp"),
            P(None, "dp"),
            P(None, "dp", "tp"),
            P(None, "dp", "tp"),
            P(None, "dp", "tp"),
            P(None, "dp", "tp"),
            P(None, "dp", "tp"),
            P(None, "tp"),
            P(None, "tp", "dp"),
            P(None, ("grp", "dp"), "tp"),
            P(None, ("grp", "dp"), "tp", None, None),
        ),
        out_specs=(P(("grp", "tp"), "dp"), P(None, ("grp", "dp"), "tp", None, None)),
        check_vma=False,
    )
```

```python
import functools

import jax
import jax.numpy as jnp
from jax import lax
from jax.experimental import pallas as pl
from jax.experimental.pallas import tpu as pltpu
from jax.sharding import PartitionSpec as P

EPSILON = 1e-06
SOFTNESS = 16.0
F32 = jnp.float32
BF16 = jnp.bfloat16


def swap(tiles):
    return pltpu.roll(tiles, 4, 0)


def first_half(shape):
    return lax.broadcasted_iota(jnp.int32, shape, 0) < 4


def fold(upper, lower, second):
    even = jnp.concatenate([lower[:, :128], lower[:, 256:384]], axis=1)
    odd = jnp.concatenate([lower[:, 128:256], lower[:, 384:]], axis=1)
    top = first_half(even.shape)
    first_form = jnp.where(top, even, swap(odd))
    second_form = jnp.where(top, swap(even), odd)
    if isinstance(second, int):
        folded = second_form if second else first_form
    else:
        folded = jnp.where(second == 1, second_form, first_form)
    return jnp.concatenate(
        [
            jnp.concatenate([upper[:, :256], folded[:, :128]], axis=1),
            jnp.concatenate([upper[:, 256:], folded[:, 128:]], axis=1),
        ],
        axis=0,
    )


def unfold(block):
    upper = jnp.concatenate([block[:8, :256], block[8:, :256]], axis=1)
    left, right = block[:8, 256:], block[8:, 256:]
    lower = jnp.concatenate([left, swap(left), right, swap(right)], axis=1)
    return upper, lower


def unfold_rows(block):
    upper, lower = unfold(block)
    return jnp.concatenate([upper, jnp.where(first_half(lower.shape), lower, 0.0)], axis=0)


def stack_pair(one, two):
    lower = []
    for half in range(2):
        a, b = one[8 * half : 8 * half + 8, 256:], two[8 * half : 8 * half + 8, 256:]
        top = first_half(a.shape)
        lower += [jnp.where(top, a, swap(b)), jnp.where(top, swap(a), b)]
    return jnp.concatenate(
        [
            jnp.concatenate([one[:8, :256], one[8:, :256]], axis=1),
            jnp.concatenate([two[:8, :256], two[8:, :256]], axis=1),
            jnp.concatenate(lower, axis=1),
        ],
        axis=0,
    )


def block_kernel(
    n_tp, n_dp, d_model, head_key, value_channels, piece,
    hidden_hbm, gain_hbm, out_gain_hbm, offset_hbm,
    wq_hbm, wk_hbm, wd_hbm, wv_hbm, wg_hbm, wo_hbm, state_hbm,
    hidden_out_ref, new_state_ref,
    hidden, gain, out_gain, offset, proj, wo, state,
    gathered, product, partial, near, own, cross, far, direct, far_direct,
    sq_part, sq_near, sq_cross, sq_far,
    expand, values, fresh_columns, readout,
    gated_all, mix_part, mix_send, mix_recv, mix_other, mix_last, lent, handed,
    small_sem, proj_sem, wo_sem, state_sem,
    gather_recv, near_recv, far_recv, sq_recv, gated_recv, mix_recv_sem, direct_recv, lent_sem, send_sem,
):
    layers, rows, heads = state.shape[0], state.shape[1], state.shape[2]
    pad = 16
    mix_pieces = mix_send.shape[1]
    pieces = proj.shape[1]
    key_cols = heads * head_key
    value_cols = heads * value_channels
    halves = value_cols // piece
    half_heads = heads // halves
    pairs = tuple((3 + 2 * half, 2) for half in range(halves))
    groups = ((0, 3),) + pairs
    tp = lax.axis_index("tp")
    dp = lax.axis_index("dp")
    chip, core = dp // 2, lax.rem(dp, 2)
    other_core = 1 - core
    other_chip = 1 - chip
    partner = 2 * chip + other_core
    across = 2 * other_chip + core
    diagonal = 2 * other_chip + other_core
    mesh_id = pl.DeviceIdType.MESH

    barrier = pltpu.get_barrier_semaphore()
    for j in range(1, n_tp):
        pl.semaphore_signal(
            barrier, inc=1, device_id={"tp": lax.rem(tp + j, n_tp)}, device_id_type=mesh_id
        )
    for j in range(1, n_dp):
        pl.semaphore_signal(
            barrier, inc=1, device_id={"dp": lax.rem(dp + j, n_dp)}, device_id_type=mesh_id
        )

    for j in range(1, n_tp):
        pl.semaphore_signal(
            barrier, inc=1, device_id={"tp": lax.rem(tp + j, n_tp), "dp": partner},
            device_id_type=mesh_id,
        )

    small = [
        pltpu.make_async_copy(source, target, small_sem.at[index])
        for index, (source, target) in enumerate(
            ((hidden_hbm, hidden), (gain_hbm, gain), (out_gain_hbm, out_gain), (offset_hbm, offset))
        )
    ]

    def load_proj(layer, i):
        if i < 3:
            source = (wd_hbm, wq_hbm, wk_hbm)[i].at[layer]
        else:
            half, which = divmod(i - 3, 2)
            source = (wv_hbm, wg_hbm)[which].at[layer, :, pl.ds(half * piece, piece)]
        return pltpu.make_async_copy(source, proj.at[layer, i], proj_sem.at[layer])

    def load_wo(layer):
        return pltpu.make_async_copy(wo_hbm.at[layer], wo.at[layer], wo_sem)

    def load_state(layer):
        return pltpu.make_async_copy(state_hbm.at[layer], state.at[layer], state_sem)

    for copy in small:
        copy.start()

    @pl.when(core == 0)
    def _():
        far_direct[...] = jnp.zeros_like(far_direct)

    row_of = lax.broadcasted_iota(jnp.int32, (4 * pad, 2 * value_channels), 0)
    lane_of = lax.broadcasted_iota(jnp.int32, (4 * pad, 2 * value_channels), 1)
    for second in range(2):
        for pair in range(rows // 2):
            picked = pair * 2 + lane_of // value_channels
            inside = (row_of >= second * 2 * pad) & (row_of < (second + 1) * 2 * pad)
            hit = inside & (lax.rem(row_of, pad) == picked)
            expand[second, pair] = jnp.where(hit, 1.0, 0.0).astype(BF16)

    for copy in small:
        copy.wait()
    for layer in range(layers):
        for i in range(pieces):
            load_proj(layer, i).start()
        load_state(layer).start()
        load_wo(layer).start()

    upper = hidden[pl.ds(0, 8), :].astype(F32)
    lower = hidden[pl.ds(8, 4), :].astype(F32)
    lower = jnp.concatenate([lower, lower], axis=0)
    for p in range(mix_pieces):
        span = slice(p * piece, (p + 1) * piece)
        gathered[0, p, tp] = fold(upper[:, span], lower[:, span], 0).astype(BF16)
    pl.semaphore_wait(barrier, 2 * n_tp + n_dp - 3)

    def remote(src, dst, send, recv, axis, target):
        remote_to(src, dst, send, recv, {axis: target})

    def remote_to(src, dst, send, recv, device):
        copy = pltpu.make_async_remote_copy(
            src_ref=src, dst_ref=dst, send_sem=send, recv_sem=recv,
            device_id=device, device_id_type=mesh_id,
        )
        copy.start()

    def await_bytes(ref, sem):
        pltpu.make_async_copy(ref, ref, sem).wait()

    above = tp // 2
    middle = (tp == 1) | (tp == 2)
    is_owner = middle & (core == 1)
    lender = middle & (core == 0)
    even_dp, odd_dp = 2 * chip, 2 * chip + 1

    def tp_step(j):
        return j + above * (n_tp - 2 * j)

    def send_features(layer, p):
        for j in range(n_tp - 1, 0, -1):
            remote(
                gathered.at[layer, p, tp], gathered.at[layer, p, tp],
                send_sem.at[0], gather_recv.at[p],
                "tp", lax.rem(tp + tp_step(j), n_tp),
            )

    def await_features(layer, p):
        if layer == 0:
            await_bytes(gathered.at[layer, p, pl.ds(0, n_tp - 1)], gather_recv.at[p])
            return

        @pl.when(is_owner)
        def _():
            await_bytes(gathered.at[layer, p, pl.ds(0, 2)], gather_recv.at[p])

        @pl.when(jnp.logical_not(is_owner))
        def _():
            await_bytes(gathered.at[layer, p], gather_recv.at[p])

    def await_feature_sends(layer):
        if layer == 0:
            await_bytes(gathered.at[layer, :, pl.ds(0, n_tp - 1)], send_sem.at[0])
            return

        @pl.when(is_owner)
        def _():
            await_bytes(mix_recv.at[layer - 1], send_sem.at[0])
            await_bytes(mix_other.at[layer - 1], send_sem.at[8])

    def gated_pair(layer, half, which):
        return stack_pair(
            gated_all[layer, half, 2 * which].astype(F32),
            gated_all[layer, half, 2 * which + 1].astype(F32),
        ).astype(BF16)

    def mix(layer, p, which, result):
        for k in range(2):
            group = 2 * which + k
            mix_send[layer, p, group] = fold(
                result[8 * k : 8 * k + 8], result[16:], k
            ).astype(BF16)
        for k in range(2):
            group = 2 * which + k
            if layer == layers - 1:
                continue
            to = 1 + which

            @pl.when((core == 1) & (tp != to))
            def _():
                remote(
                    mix_send.at[layer, p, group], mix_recv.at[layer, p, k, tp - above],
                    send_sem.at[5], mix_recv_sem.at[0, p, k], "tp", to,
                )

            @pl.when(core == 0)
            def _():
                remote_to(
                    mix_send.at[layer, p, group], mix_other.at[layer, p, k, tp],
                    send_sem.at[5], mix_recv_sem.at[1, p, k], {"tp": to, "dp": odd_dp},
                )

    def send_last(layer, which):
        for k in range(2):
            to = 2 * which + k

            @pl.when(tp != to)
            def _():
                for p in range(mix_pieces):
                    remote(
                        mix_send.at[layer, p, to],
                        mix_last.at[p, lax.rem(tp - to + n_tp - 1, n_tp)],
                        send_sem.at[5], mix_recv_sem.at[0, p, 0], "tp", to,
                    )

    def project_out(layer, which, arrivals, senders):
        for half in range(halves):
            await_bytes(
                gated_all.at[layer, half, pl.ds(0, senders)], gated_recv.at[arrivals + half]
            )
            gated = gated_pair(layer, half, which)
            for p in range(mix_pieces):
                columns = pl.ds(p * piece, piece)
                result = jnp.dot(
                    gated, wo[layer, pl.ds(half * piece, piece), columns],
                    preferred_element_type=F32,
                )
                if half > 0:
                    result = result + mix_part[p]
                if half < halves - 1:
                    mix_part[p] = result
                else:
                    mix(layer, p, which, result)

    def renew(layer, begin, end):
        for pair in range(begin, end):
            adds = jnp.dot(fresh_columns[...], expand[0, pair], preferred_element_type=F32)
            keeps = jnp.dot(fresh_columns[...], expand[1, pair], preferred_element_type=F32)
            for k in range(2):
                b = 2 * pair + k
                lanes = slice(k * value_channels, (k + 1) * value_channels)
                for h in range(heads):
                    part = slice(h * head_key, (h + 1) * head_key)
                    row = values[pl.ds(b, 1), pl.ds(h * value_channels, value_channels)]
                    new_state_ref[layer, b, h] = (
                        keeps[part, lanes] * state[layer, b, h] + adds[part, lanes] * row
                    )

    def await_mixed_sends(layer):
        if layer == layers - 1:
            await_bytes(mix_last, send_sem.at[5])
            return

        @pl.when(is_owner)
        def _():
            await_bytes(mix_send.at[layer, :, pl.ds(0, 2)], send_sem.at[5])

        @pl.when(jnp.logical_not(is_owner))
        def _():
            await_bytes(mix_send.at[layer], send_sem.at[5])

    def lend_residual(layer):
        block = gathered.at[layer, :, pl.ds(2 * (tp - 1), 2)]
        remote(block, lent.at[layer], send_sem.at[9], lent_sem, "dp", partner)

    def finish_middle(layer):
        near_end, far_end = 3 * (tp - 1), 3 * (2 - tp)
        units = [(p, k) for p in range(mix_pieces) for k in range(2)]
        for p, k in units:
            await_bytes(mix_recv.at[layer, p, k], mix_recv_sem.at[0, p, k])
            mine = 2 * (tp - 1) + k
            total = mix_send[layer, p, mine].astype(F32)
            for j in range(n_tp - 1):
                total = total + mix_recv[layer, p, k, j].astype(F32)
            gathered[layer + 1, p, mine] = (
                gathered[layer, p, mine].astype(F32) + total
            ).astype(BF16)
            block = gathered.at[layer + 1, p, mine]
            for to in (far_end, 3 - tp, near_end):
                remote(block, block, send_sem.at[0], gather_recv.at[p], "tp", to)
        await_bytes(lent.at[layer], lent_sem)
        for p, k in units:
            await_bytes(mix_other.at[layer, p, k], mix_recv_sem.at[1, p, k])
            mine = 2 * (tp - 1) + k
            total = mix_other[layer, p, k, 0].astype(F32)
            for j in range(1, n_tp):
                total = total + mix_other[layer, p, k, j].astype(F32)
            handed[layer, p, k] = (lent[layer, p, k].astype(F32) + total).astype(BF16)
            for to in (far_end, 3 - tp, near_end, tp):
                remote_to(
                    handed.at[layer, p, k], gathered.at[layer + 1, p, mine],
                    send_sem.at[8], gather_recv.at[p], {"tp": to, "dp": even_dp},
                )

    def store_partial(layer, i, result):
        for c in range(2):
            block = result[24 * c : 24 * c + 24]
            tail = jnp.concatenate([block[16:, :256], block[16:, 256:]], axis=0)
            partial[layer, c, i] = jnp.concatenate([block[:16], tail], axis=1).astype(BF16)

    def send_group(layer, number):
        these = pl.ds(*groups[number])
        remote(
            partial.at[layer, other_core, these], near.at[layer, these],
            send_sem.at[2], near_recv.at[number], "dp", partner,
        )

    def halves_of(block):
        tail = jnp.concatenate([block[:8, piece:], block[8:, piece:]], axis=1)
        return block[:8, :piece], block[8:, :piece], tail

    def of_other_chip(block):
        zero, one, tail = halves_of(block)
        return fold(jnp.where(chip == 0, one, zero), tail, other_chip).astype(BF16)

    def of_this_chip(block):
        zero, one, tail = halves_of(block)
        return fold(jnp.where(chip == 0, zero, one), tail, chip)

    def chip_sum(layer, i):
        return partial[layer, core, i].astype(F32) + near[layer, i].astype(F32)

    def send_cross(layer, number):
        these = pl.ds(*groups[number])
        remote(
            cross.at[layer, these], far.at[layer, these],
            send_sem.at[3], far_recv.at[number], "dp", across,
        )

    def cross_squares(layer):
        await_bytes(sq_near.at[layer], sq_recv.at[0])
        chip_squares = sq_part[layer, core] + sq_near[layer]
        sq_part[layer, core] = chip_squares
        sq_cross[layer] = jnp.concatenate(
            [jnp.where(chip == 0, chip_squares[8:16], chip_squares[:8]), chip_squares[16:]], axis=0
        )
        remote(
            sq_cross.at[layer], sq_far.at[layer], send_sem.at[6], sq_recv.at[1], "dp", across
        )

    def first_of_core_0(layer):
        cross_squares(layer)
        begin, amount = groups[0]
        await_bytes(near.at[layer, pl.ds(begin, amount)], near_recv.at[0])
        for i in range(begin, begin + amount):
            cross[layer, i] = of_other_chip(chip_sum(layer, i))
        send_cross(layer, 0)
        for i in range(begin, begin + amount):
            direct[layer, i] = of_other_chip(partial[layer, 1, i].astype(F32))
        remote(
            direct.at[layer], far_direct.at[layer],
            send_sem.at[7], direct_recv, "dp", diagonal,
        )
        for i in range(begin, begin + amount):
            own[i] = of_this_chip(chip_sum(layer, i))

    def send_direct_of_core_1(layer):
        begin, amount = groups[0]
        for i in range(begin, begin + amount):
            cross[layer, i] = of_other_chip(partial[layer, 1, i].astype(F32))
        send_cross(layer, 0)

    def first_of_core_1(layer):
        cross_squares(layer)
        begin, amount = groups[0]
        await_bytes(near.at[layer, pl.ds(begin, amount)], near_recv.at[0])
        for i in range(begin, begin + amount):
            own[i] = of_this_chip(chip_sum(layer, i))

    def cross_group(layer, number):
        begin, amount = groups[number]
        await_bytes(near.at[layer, pl.ds(begin, amount)], near_recv.at[number])
        for i in range(begin, begin + amount):
            cross[layer, i] = of_other_chip(chip_sum(layer, i))
        send_cross(layer, number)
        for i in range(begin, begin + amount):
            own[i] = of_this_chip(chip_sum(layer, i))

    def split(block):
        high = block.astype(BF16).astype(F32)
        return [high, block - high]

    def columns_of(parts):
        return jnp.concatenate(parts, axis=0).T.astype(BF16)

    for p in range(mix_pieces):
        send_features(0, p)

    for layer in range(layers):
        squares = jnp.zeros((n_tp * rows, 128), F32)
        scaled = []
        first, count = groups[0]
        for p in range(mix_pieces):
            await_features(layer, p)
            widened = jnp.concatenate(
                [
                    stack_pair(
                        gathered[layer, p, c].astype(F32), gathered[layer, p, 2 + c].astype(F32)
                    )
                    for c in range(2)
                ],
                axis=0,
            )
            span = pl.ds(p * piece, piece)
            scaled.append((widened * gain[layer, span][None, :]).astype(BF16))
            for lane in range(0, piece, 128):
                tile = widened[:, lane : lane + 128]
                squares = squares + tile * tile
            if p == 0:
                await_bytes(proj.at[layer], proj_sem.at[layer])
            if p == mix_pieces - 1:
                for c in range(2):
                    sq_part[layer, c] = squares[24 * c : 24 * c + 24]
                remote(
                    sq_part.at[layer, other_core], sq_near.at[layer],
                    send_sem.at[1], sq_recv.at[0], "dp", partner,
                )
            for i in range(first, first + count):
                result = jnp.dot(scaled[p], proj[layer, i, span, :], preferred_element_type=F32)
                if p > 0:
                    result = result + product[i]
                if p < mix_pieces - 1:
                    product[i] = result
                else:
                    store_partial(layer, i, result)
        send_group(layer, 0)
        pl.when(core == 0)(functools.partial(first_of_core_0, layer))
        pl.when(core != 0)(functools.partial(send_direct_of_core_1, layer))
        whole_rows = jnp.concatenate(scaled, axis=1)
        for number in range(1, len(groups)):
            first, count = groups[number]
            for i in range(first, first + count):
                store_partial(
                    layer, i, jnp.dot(whole_rows, proj[layer, i], preferred_element_type=F32)
                )
            send_group(layer, number)
            pl.when(core == 0)(functools.partial(cross_group, layer, number))

        @pl.when(core != 0)
        def _():
            first_of_core_1(layer)
            for number in range(1, len(groups)):
                cross_group(layer, number)

        if layer + 1 < layers:
            pl.when(lender)(functools.partial(lend_residual, layer))
        await_bytes(sq_far.at[layer], sq_recv.at[1])
        chip_squares = sq_part[layer, core]
        last = chip_squares[16:] + sq_far[layer, pl.ds(8, 8), :]
        total_squares = jnp.concatenate(
            [
                jnp.where(chip == 0, chip_squares[:8], chip_squares[8:16])
                + sq_far[layer, pl.ds(0, 8), :],
                jnp.where(chip == 0, last, swap(last)),
            ],
            axis=0,
        )
        inverse = lax.rsqrt(jnp.sum(total_squares, axis=1, keepdims=True) / d_model + EPSILON)

        def projected(i):
            for number, (first, count) in enumerate(groups):
                if i == first:
                    await_bytes(far.at[layer, pl.ds(first, count)], far_recv.at[number])
            total = own[i] + far[layer, i].astype(F32)
            if i < groups[0][1]:
                total = total + far_direct[layer, i].astype(F32)
            return unfold_rows(total) * inverse

        if layer == 0:
            await_bytes(state, state_sem)

        @pl.when(core != 0)
        def _():
            await_bytes(far_direct.at[layer], direct_recv)

        logits = projected(0)
        log_sigmoid = jnp.minimum(logits, 0.0) - jnp.log(1.0 + jnp.exp(-jnp.abs(logits)))
        log_decay = log_sigmoid[:rows] / SOFTNESS + offset[:, layer, :]
        decay = jnp.exp(jnp.concatenate([log_decay, jnp.zeros((pad - rows, key_cols), F32)], axis=0))
        query = projected(1)
        read_columns = columns_of(split(query * decay))
        key = projected(2) * head_key ** (-0.5)
        both = query * key
        products = [
            jnp.sum(both[:, h * head_key : (h + 1) * head_key], axis=1, keepdims=True)
            for h in range(heads)
        ]

        for half in range(halves):
            base = half * half_heads
            columns = read_columns[base * head_key : (base + half_heads) * head_key]
            for pair in range(rows // 2):
                factors = jnp.dot(
                    columns, expand[0, pair, pl.ds(0, 2 * pad), :], preferred_element_type=F32
                )
                for k in range(2):
                    b = 2 * pair + k
                    for hh in range(half_heads):
                        factor = factors[
                            hh * head_key : (hh + 1) * head_key,
                            k * value_channels : (k + 1) * value_channels,
                        ]
                        readout[base + hh, pl.ds(b, 1), :] = jnp.sum(
                            factor * state[layer, b, base + hh], axis=0, keepdims=True
                        )
            value = projected(3 + 2 * half)
            gate_all = projected(4 + 2 * half)
            values[:, pl.ds(half * piece, piece)] = value
            gated_heads = []
            for hh in range(half_heads):
                h = base + hh
                span = slice(hh * value_channels, (hh + 1) * value_channels)
                got = readout[h] + products[h] * value[:, span]
                gate = gate_all[:, span]
                normed = got * lax.rsqrt(jnp.mean(got * got, axis=1, keepdims=True) + EPSILON)
                whole = pl.ds(h * value_channels, value_channels)
                normed = normed * out_gain[layer, whole][None, :]
                gated_heads.append(normed * (gate / (1.0 + jnp.exp(-gate))))
            gated = jnp.concatenate(gated_heads, axis=1)
            gated_all[layer, half, dp] = fold(gated[:8], gated[8:], 0).astype(BF16)
            block = gated_all.at[layer, half, dp]
            remote(block, block, send_sem.at[4], gated_recv.at[half], "dp", across)
            remote(block, block, send_sem.at[4], gated_recv.at[half], "dp", diagonal)
            remote(block, block, send_sem.at[4], gated_recv.at[halves + half], "dp", partner)

        fresh_columns[...] = columns_of(split(key) + split(decay))
        first_pairs = rows // 4
        renew(layer, 0, first_pairs)

        if layer == 0:
            await_bytes(wo, wo_sem)
        project_out(layer, chip, halves, 1)
        if layer == layers - 1:
            send_last(layer, chip)
        project_out(layer, other_chip, 0, 2)
        if layer == layers - 1:
            send_last(layer, other_chip)
        renew(layer, first_pairs, rows // 2)

        await_feature_sends(layer)
        if layer + 1 < layers:

            @pl.when(lender)
            def _():
                await_bytes(lent.at[layer], send_sem.at[9])

        await_bytes(sq_near.at[layer], send_sem.at[1])
        await_bytes(sq_far.at[layer], send_sem.at[6])
        await_bytes(near.at[layer], send_sem.at[2])
        await_bytes(far.at[layer], send_sem.at[3])

        @pl.when(core == 0)
        def _():
            await_bytes(direct.at[layer], send_sem.at[7])

        await_bytes(gated_all.at[layer, :, pl.ds(0, n_dp - 1)], send_sem.at[4])

        if layer + 1 < layers:
            pl.when(is_owner)(functools.partial(finish_middle, layer))
        else:
            for p in range(mix_pieces):
                await_bytes(mix_last.at[p], mix_recv_sem.at[0, p, 0])
                total = mix_send[layer, p, tp].astype(F32)
                for j in range(n_tp - 1):
                    total = total + mix_last[p, j].astype(F32)
                result = (gathered[layer, p, tp].astype(F32) + total).astype(BF16)
                span = slice(p * piece, (p + 1) * piece)
                hidden_out_ref[:, span] = unfold_rows(result.astype(F32))[:rows].astype(BF16)
        await_mixed_sends(layer)


def store_kernel(hidden_ref, state_ref, hidden_out, state_out, hidden_sem, state_sem):
    layers, rows, heads = state_ref.shape[:3]
    for layer in range(layers):
        for b in range(rows):
            for half in range(2):
                part = (layer, b, pl.ds(half * (heads // 2), heads // 2))
                pltpu.make_async_copy(state_ref.at[part], state_out.at[part], state_sem).start()
    store_hidden = pltpu.make_async_copy(hidden_ref, hidden_out, hidden_sem)
    store_hidden.start()
    store_hidden.wait()
    pltpu.make_async_copy(state_ref, state_out, state_sem).wait()


def fused(
    n_tp, n_dp, hidden_in, input_norm_gain, w_query, w_key, w_decay, w_value, w_gate,
    out_gain, w_out, decay_offset, state,
):
    layers, rows, heads, head_key, value_channels = state.shape
    width = hidden_in.shape[1]
    key_cols, value_cols = w_query.shape[2], w_value.shape[2]
    piece = key_cols
    halves = value_cols // piece
    pieces = 3 + 2 * halves
    mix_pieces = width // piece
    block = (16, piece // 4 * 3)
    vmem = pl.BlockSpec(memory_space=pltpu.VMEM)
    hbm = pl.BlockSpec(memory_space=pl.ANY)
    offsets = decay_offset.transpose(1, 0, 2)
    hidden, fresh = pl.pallas_call(
        functools.partial(
            block_kernel, n_tp, n_dp, width * n_dp, head_key, value_channels, piece
        ),
        out_shape=(
            pltpu.VMEM(hidden_in.shape, BF16),
            pltpu.VMEM(state.shape, F32),
        ),
        in_specs=[hbm] * 11,
        out_specs=(vmem, vmem),
        scratch_shapes=[
            pltpu.VMEM(hidden_in.shape, BF16),
            pltpu.VMEM(input_norm_gain.shape, F32),
            pltpu.VMEM(out_gain.shape, F32),
            pltpu.VMEM(offsets.shape, F32),
            pltpu.VMEM((layers, pieces, width, piece), BF16),
            pltpu.VMEM(w_out.shape, BF16),
            pltpu.VMEM(state.shape, F32),
            pltpu.VMEM((layers, mix_pieces, n_tp) + block, BF16),
            pltpu.VMEM((3, n_tp * rows, piece), F32),
            pltpu.VMEM((layers, 2, pieces, 16, piece // 2 * 3), BF16),
            pltpu.VMEM((layers, pieces, 16, piece // 2 * 3), BF16),
            pltpu.VMEM((pieces,) + block, F32),
            pltpu.VMEM((layers, pieces) + block, BF16),
            pltpu.VMEM((layers, pieces) + block, BF16),
            pltpu.VMEM((layers, 3) + block, BF16),
            pltpu.VMEM((layers, 3) + block, BF16),
            pltpu.VMEM((layers, 2, 2 * rows, 128), F32),
            pltpu.VMEM((layers, 2 * rows, 128), F32),
            pltpu.VMEM((layers, 16, 128), F32),
            pltpu.VMEM((layers, 16, 128), F32),
            pltpu.VMEM((2, rows // 2, 64, 2 * value_channels), BF16),
            pltpu.VMEM((16, value_cols), F32),
            pltpu.VMEM((key_cols, 64), BF16),
            pltpu.VMEM((heads, 16, value_channels), F32),
            pltpu.VMEM((layers, halves, n_dp) + block, BF16),
            pltpu.VMEM((mix_pieces, 2 * rows, piece), F32),
            pltpu.VMEM((layers, mix_pieces, n_tp) + block, BF16),
            pltpu.VMEM((layers - 1, mix_pieces, 2, n_tp - 1) + block, BF16),
            pltpu.VMEM((layers - 1, mix_pieces, 2, n_tp) + block, BF16),
            pltpu.VMEM((mix_pieces, n_tp - 1) + block, BF16),
            pltpu.VMEM((layers - 1, mix_pieces, 2) + block, BF16),
            pltpu.VMEM((layers - 1, mix_pieces, 2) + block, BF16),
            pltpu.SemaphoreType.DMA((4,)),
            pltpu.SemaphoreType.DMA((layers,)),
            pltpu.SemaphoreType.DMA,
            pltpu.SemaphoreType.DMA,
            pltpu.SemaphoreType.DMA((mix_pieces,)),
            pltpu.SemaphoreType.DMA((1 + halves,)),
            pltpu.SemaphoreType.DMA((1 + halves,)),
            pltpu.SemaphoreType.DMA((2,)),
            pltpu.SemaphoreType.DMA((2 * halves,)),
            pltpu.SemaphoreType.DMA((2, mix_pieces, 2)),
            pltpu.SemaphoreType.DMA,
            pltpu.SemaphoreType.DMA,
            pltpu.SemaphoreType.DMA((10,)),
        ],
        compiler_params=pltpu.CompilerParams(
            collective_id=0, has_side_effects=True, vmem_limit_bytes=48 * 1024 * 1024
        ),
    )(
        hidden_in, input_norm_gain, out_gain, offsets,
        w_query, w_key, w_decay, w_value, w_gate, w_out, state,
    )
    return pl.pallas_call(
        store_kernel,
        out_shape=(
            jax.ShapeDtypeStruct(hidden_in.shape, BF16),
            jax.ShapeDtypeStruct(state.shape, F32),
        ),
        in_specs=[vmem] * 2,
        out_specs=(hbm, hbm),
        scratch_shapes=[
            pltpu.SemaphoreType.DMA,
            pltpu.SemaphoreType.DMA,
        ],
        compiler_params=pltpu.CompilerParams(vmem_limit_bytes=1024 * 1024),
    )(hidden, fresh)


def plain(
    hidden_in, input_norm_gain, w_query, w_key, w_decay, w_value, w_gate,
    out_gain, w_out, decay_offset, state,
):
    layers, rows, heads, head_key, value_channels = state.shape
    key_cols, value_cols = w_query.shape[2], w_value.shape[2]
    d_model = hidden_in.shape[1] * lax.axis_size("dp")
    first = lax.axis_index("dp") * rows
    current, states = hidden_in, []
    for layer in range(layers):
        widened = lax.all_gather(current, "tp", axis=0, tiled=True).astype(F32)
        squares = lax.psum(jnp.sum(widened * widened, axis=1), "dp")
        scaled = (widened * input_norm_gain[layer][None, :]).astype(BF16)
        partial = jnp.concatenate(
            [
                jnp.dot(scaled, matrix[layer], preferred_element_type=F32)
                for matrix in (w_query, w_key, w_decay, w_value, w_gate)
            ],
            axis=1,
        ).astype(BF16)
        summed = lax.psum_scatter(partial, "dp", scatter_dimension=0, tiled=True).astype(F32)
        own = lax.dynamic_slice_in_dim(squares, first, rows)
        projected = summed * lax.rsqrt(own / d_model + EPSILON)[:, None]
        query, key, logits, value, gate = jnp.split(
            projected,
            [key_cols, 2 * key_cols, 3 * key_cols, 3 * key_cols + value_cols],
            axis=1,
        )
        decay = jnp.exp(jax.nn.log_sigmoid(logits) / SOFTNESS + decay_offset[layer])
        per_key, per_value = (rows, heads, head_key), (rows, heads, value_channels)
        fresh = (
            decay.reshape(per_key)[..., None] * state[layer]
            + (key * head_key ** (-0.5)).reshape(per_key)[..., None]
            * value.reshape(per_value)[:, :, None, :]
        )
        got = jnp.sum(query.reshape(per_key)[..., None] * fresh, axis=2)
        got = got * lax.rsqrt(jnp.mean(got * got, axis=2, keepdims=True) + EPSILON)
        got = got * out_gain[layer].reshape(heads, value_channels)[None]
        gated = (got * jax.nn.silu(gate.reshape(per_value))).reshape(rows, value_cols).astype(BF16)
        mixed = jnp.dot(
            lax.all_gather(gated, "dp", axis=0, tiled=True), w_out[layer],
            preferred_element_type=F32,
        ).astype(BF16)
        mine = lax.psum_scatter(mixed, "tp", scatter_dimension=0, tiled=True).astype(F32)
        current = (current.astype(F32) + mine).astype(BF16)
        states.append(fresh)
    return current, jnp.stack(states)


def solution(mesh):
    n_tp, n_dp = mesh.shape["tp"], mesh.shape["dp"]

    def per_device(hidden_in, *rest):
        state = rest[-1]
        width, key_cols, value_cols = hidden_in.shape[1], rest[1].shape[2], rest[4].shape[2]
        layers, rows, heads = state.shape[:3]
        sized = key_cols == 512 and width % key_cols == 0 and value_cols % key_cols == 0
        shaped = hidden_in.shape[0] == rows == 12 and state.shape[4] == 128
        if n_tp == 4 and n_dp == 4 and layers > 1 and sized and shaped and heads % (value_cols // key_cols) == 0:
            return fused(n_tp, n_dp, hidden_in, *rest)
        return plain(hidden_in, *rest)

    return jax.shard_map(
        per_device,
        mesh=mesh,
        in_specs=(
            P(("grp", "tp"), "dp"),
            P(None, "dp"),
            P(None, "dp", "tp"),
            P(None, "dp", "tp"),
            P(None, "dp", "tp"),
            P(None, "dp", "tp"),
            P(None, "dp", "tp"),
            P(None, "tp"),
            P(None, "tp", "dp"),
            P(None, ("grp", "dp"), "tp"),
            P(None, ("grp", "dp"), "tp", None, None),
        ),
        out_specs=(P(("grp", "tp"), "dp"), P(None, ("grp", "dp"), "tp", None, None)),
        check_vma=False,
    )
```

```python
import functools

import jax
import jax.numpy as jnp
from jax import lax
from jax.experimental import pallas as pl
from jax.experimental.pallas import tpu as pltpu
from jax.sharding import PartitionSpec as P

EPSILON = 1e-06
SOFTNESS = 16.0
F32 = jnp.float32
BF16 = jnp.bfloat16


def swap(tiles):
    return pltpu.roll(tiles, 4, 0)


def first_half(shape):
    return lax.broadcasted_iota(jnp.int32, shape, 0) < 4


def fold(upper, lower, second):
    even = jnp.concatenate([lower[:, :128], lower[:, 256:384]], axis=1)
    odd = jnp.concatenate([lower[:, 128:256], lower[:, 384:]], axis=1)
    top = first_half(even.shape)
    first_form = jnp.where(top, even, swap(odd))
    second_form = jnp.where(top, swap(even), odd)
    if isinstance(second, int):
        folded = second_form if second else first_form
    else:
        folded = jnp.where(second == 1, second_form, first_form)
    return jnp.concatenate(
        [
            jnp.concatenate([upper[:, :256], folded[:, :128]], axis=1),
            jnp.concatenate([upper[:, 256:], folded[:, 128:]], axis=1),
        ],
        axis=0,
    )


def unfold(block):
    upper = jnp.concatenate([block[:8, :256], block[8:, :256]], axis=1)
    left, right = block[:8, 256:], block[8:, 256:]
    lower = jnp.concatenate([left, swap(left), right, swap(right)], axis=1)
    return upper, lower


def unfold_rows(block):
    upper, lower = unfold(block)
    return jnp.concatenate([upper, jnp.where(first_half(lower.shape), lower, 0.0)], axis=0)


def stack_pair(one, two):
    lower = []
    for half in range(2):
        a, b = one[8 * half : 8 * half + 8, 256:], two[8 * half : 8 * half + 8, 256:]
        top = first_half(a.shape)
        lower += [jnp.where(top, a, swap(b)), jnp.where(top, swap(a), b)]
    return jnp.concatenate(
        [
            jnp.concatenate([one[:8, :256], one[8:, :256]], axis=1),
            jnp.concatenate([two[:8, :256], two[8:, :256]], axis=1),
            jnp.concatenate(lower, axis=1),
        ],
        axis=0,
    )


def block_kernel(
    n_tp, n_dp, d_model, head_key, value_channels, piece,
    hidden_hbm, gain_hbm, out_gain_hbm, offset_hbm,
    wq_hbm, wk_hbm, wd_hbm, wv_hbm, wg_hbm, wo_hbm, state_hbm,
    hidden_out_ref, new_state_ref,
    hidden, gain, out_gain, offset, proj, wo, state,
    gathered, product, partial, near, own, cross, far, direct, far_direct,
    sq_part, sq_near, sq_cross, sq_far,
    expand, values, fresh_columns, readout,
    gated_all, mix_part, mix_send, mix_recv, mix_other, mix_last, lent, handed,
    small_sem, proj_sem, wo_sem, state_sem,
    gather_recv, near_recv, far_recv, sq_recv, gated_recv, mix_recv_sem, direct_recv, lent_sem, send_sem,
):
    layers, rows, heads = state.shape[0], state.shape[1], state.shape[2]
    pad = 16
    mix_pieces = mix_send.shape[1]
    pieces = proj.shape[1]
    key_cols = heads * head_key
    value_cols = heads * value_channels
    halves = value_cols // piece
    half_heads = heads // halves
    pairs = tuple((3 + 2 * half, 2) for half in range(halves))
    groups = ((0, 3),) + pairs
    tp = lax.axis_index("tp")
    dp = lax.axis_index("dp")
    chip, core = dp // 2, lax.rem(dp, 2)
    other_core = 1 - core
    other_chip = 1 - chip
    partner = 2 * chip + other_core
    across = 2 * other_chip + core
    diagonal = 2 * other_chip + other_core
    mesh_id = pl.DeviceIdType.MESH

    barrier = pltpu.get_barrier_semaphore()
    for j in range(1, n_tp):
        pl.semaphore_signal(
            barrier, inc=1, device_id={"tp": lax.rem(tp + j, n_tp)}, device_id_type=mesh_id
        )
    for j in range(1, n_dp):
        pl.semaphore_signal(
            barrier, inc=1, device_id={"dp": lax.rem(dp + j, n_dp)}, device_id_type=mesh_id
        )

    for j in range(1, n_tp):
        pl.semaphore_signal(
            barrier, inc=1, device_id={"tp": lax.rem(tp + j, n_tp), "dp": partner},
            device_id_type=mesh_id,
        )

    small = [
        pltpu.make_async_copy(source, target, small_sem.at[index])
        for index, (source, target) in enumerate(
            ((hidden_hbm, hidden), (gain_hbm, gain), (out_gain_hbm, out_gain), (offset_hbm, offset))
        )
    ]

    def load_proj(layer, i):
        if i < 3:
            source = (wd_hbm, wq_hbm, wk_hbm)[i].at[layer]
        else:
            half, which = divmod(i - 3, 2)
            source = (wv_hbm, wg_hbm)[which].at[layer, :, pl.ds(half * piece, piece)]
        return pltpu.make_async_copy(source, proj.at[layer, i], proj_sem.at[layer])

    def load_wo(layer):
        return pltpu.make_async_copy(wo_hbm.at[layer], wo.at[layer], wo_sem)

    def load_state(layer):
        return pltpu.make_async_copy(state_hbm.at[layer], state.at[layer], state_sem)

    for copy in small:
        copy.start()

    @pl.when(core == 0)
    def _():
        far_direct[...] = jnp.zeros_like(far_direct)

    row_of = lax.broadcasted_iota(jnp.int32, (4 * pad, 2 * value_channels), 0)
    lane_of = lax.broadcasted_iota(jnp.int32, (4 * pad, 2 * value_channels), 1)
    for second in range(2):
        for pair in range(rows // 2):
            picked = pair * 2 + lane_of // value_channels
            inside = (row_of >= second * 2 * pad) & (row_of < (second + 1) * 2 * pad)
            hit = inside & (lax.rem(row_of, pad) == picked)
            expand[second, pair] = jnp.where(hit, 1.0, 0.0).astype(BF16)

    for copy in small:
        copy.wait()
    for layer in range(layers):
        for i in range(pieces):
            load_proj(layer, i).start()
        load_state(layer).start()
        load_wo(layer).start()

    upper = hidden[pl.ds(0, 8), :].astype(F32)
    lower = hidden[pl.ds(8, 4), :].astype(F32)
    lower = jnp.concatenate([lower, lower], axis=0)
    for p in range(mix_pieces):
        span = slice(p * piece, (p + 1) * piece)
        gathered[0, p, tp] = fold(upper[:, span], lower[:, span], 0).astype(BF16)
    pl.semaphore_wait(barrier, 2 * n_tp + n_dp - 3)

    def remote(src, dst, send, recv, axis, target):
        remote_to(src, dst, send, recv, {axis: target})

    def remote_to(src, dst, send, recv, device):
        copy = pltpu.make_async_remote_copy(
            src_ref=src, dst_ref=dst, send_sem=send, recv_sem=recv,
            device_id=device, device_id_type=mesh_id,
        )
        copy.start()

    def await_bytes(ref, sem):
        pltpu.make_async_copy(ref, ref, sem).wait()

    above = tp // 2
    middle = (tp == 1) | (tp == 2)
    is_owner = middle & (core == 1)
    lender = middle & (core == 0)
    even_dp, odd_dp = 2 * chip, 2 * chip + 1

    def tp_step(j):
        return j + above * (n_tp - 2 * j)

    def send_features(layer, p):
        for j in range(n_tp - 1, 0, -1):
            remote(
                gathered.at[layer, p, tp], gathered.at[layer, p, tp],
                send_sem.at[0], gather_recv.at[p],
                "tp", lax.rem(tp + tp_step(j), n_tp),
            )

    def await_features(layer, p):
        if layer == 0:
            await_bytes(gathered.at[layer, p, pl.ds(0, n_tp - 1)], gather_recv.at[p])
            return

        @pl.when(is_owner)
        def _():
            await_bytes(gathered.at[layer, p, pl.ds(0, 2)], gather_recv.at[p])

        @pl.when(jnp.logical_not(is_owner))
        def _():
            await_bytes(gathered.at[layer, p], gather_recv.at[p])

    def await_feature_sends(layer):
        if layer == 0:
            await_bytes(gathered.at[layer, :, pl.ds(0, n_tp - 1)], send_sem.at[0])
            return

        @pl.when(is_owner)
        def _():
            await_bytes(mix_recv.at[layer - 1], send_sem.at[0])
            await_bytes(mix_other.at[layer - 1], send_sem.at[5])

    def gated_pair(layer, half, which):
        return stack_pair(
            gated_all[layer, half, 2 * which].astype(F32),
            gated_all[layer, half, 2 * which + 1].astype(F32),
        ).astype(BF16)

    def mix(layer, p, which, result):
        for k in range(2):
            group = 2 * which + k
            mix_send[layer, p, group] = fold(
                result[8 * k : 8 * k + 8], result[16:], k
            ).astype(BF16)
        for k in range(2):
            group = 2 * which + k
            if layer == layers - 1:
                continue
            to = 1 + which

            @pl.when((core == 1) & (tp != to))
            def _():
                remote(
                    mix_send.at[layer, p, group], mix_recv.at[layer, p, k, tp - above],
                    send_sem.at[2], mix_recv_sem.at[0, p, k], "tp", to,
                )

            @pl.when(core == 0)
            def _():
                remote_to(
                    mix_send.at[layer, p, group], mix_other.at[layer, p, k, tp],
                    send_sem.at[2], mix_recv_sem.at[1, p, k], {"tp": to, "dp": odd_dp},
                )

    def send_last(layer, which):
        for k in range(2):
            to = 2 * which + k

            @pl.when(tp != to)
            def _():
                for p in range(mix_pieces):
                    remote(
                        mix_send.at[layer, p, to],
                        mix_last.at[p, lax.rem(tp - to + n_tp - 1, n_tp)],
                        send_sem.at[2], mix_recv_sem.at[0, p, 0], "tp", to,
                    )

    def project_out(layer, which, arrivals, senders):
        for half in range(halves):
            await_bytes(
                gated_all.at[layer, half, pl.ds(0, senders)], gated_recv.at[arrivals + half]
            )
            gated = gated_pair(layer, half, which)
            for p in range(mix_pieces):
                columns = pl.ds(p * piece, piece)
                result = jnp.dot(
                    gated, wo[layer, pl.ds(half * piece, piece), columns],
                    preferred_element_type=F32,
                )
                if half > 0:
                    result = result + mix_part[p]
                if half < halves - 1:
                    mix_part[p] = result
                else:
                    mix(layer, p, which, result)

    def renew(layer, begin, end):
        for pair in range(begin, end):
            adds = jnp.dot(fresh_columns[...], expand[0, pair], preferred_element_type=F32)
            keeps = jnp.dot(fresh_columns[...], expand[1, pair], preferred_element_type=F32)
            for k in range(2):
                b = 2 * pair + k
                lanes = slice(k * value_channels, (k + 1) * value_channels)
                for h in range(heads):
                    part = slice(h * head_key, (h + 1) * head_key)
                    row = values[pl.ds(b, 1), pl.ds(h * value_channels, value_channels)]
                    new_state_ref[layer, b, h] = (
                        keeps[part, lanes] * state[layer, b, h] + adds[part, lanes] * row
                    )

    def await_mixed_sends(layer):
        if layer == layers - 1:
            await_bytes(mix_last, send_sem.at[2])
            return

        @pl.when(is_owner)
        def _():
            await_bytes(mix_send.at[layer, :, pl.ds(0, 2)], send_sem.at[2])

        @pl.when(jnp.logical_not(is_owner))
        def _():
            await_bytes(mix_send.at[layer], send_sem.at[2])

    def lend_residual(layer):
        block = gathered.at[layer, :, pl.ds(2 * (tp - 1), 2)]
        remote(block, lent.at[layer], send_sem.at[6], lent_sem, "dp", partner)

    def finish_middle(layer):
        near_end, far_end = 3 * (tp - 1), 3 * (2 - tp)
        units = [(p, k) for p in range(mix_pieces) for k in range(2)]
        for p, k in units:
            await_bytes(mix_recv.at[layer, p, k], mix_recv_sem.at[0, p, k])
            mine = 2 * (tp - 1) + k
            total = mix_send[layer, p, mine].astype(F32)
            for j in range(n_tp - 1):
                total = total + mix_recv[layer, p, k, j].astype(F32)
            gathered[layer + 1, p, mine] = (
                gathered[layer, p, mine].astype(F32) + total
            ).astype(BF16)
            block = gathered.at[layer + 1, p, mine]
            for to in (far_end, 3 - tp, near_end):
                remote(block, block, send_sem.at[0], gather_recv.at[p], "tp", to)
        await_bytes(lent.at[layer], lent_sem)
        for p, k in units:
            await_bytes(mix_other.at[layer, p, k], mix_recv_sem.at[1, p, k])
            mine = 2 * (tp - 1) + k
            total = mix_other[layer, p, k, 0].astype(F32)
            for j in range(1, n_tp):
                total = total + mix_other[layer, p, k, j].astype(F32)
            handed[layer, p, k] = (lent[layer, p, k].astype(F32) + total).astype(BF16)
            for to in (far_end, 3 - tp, near_end, tp):
                remote_to(
                    handed.at[layer, p, k], gathered.at[layer + 1, p, mine],
                    send_sem.at[5], gather_recv.at[p], {"tp": to, "dp": even_dp},
                )

    def store_partial(layer, i, result):
        for c in range(2):
            block = result[24 * c : 24 * c + 24]
            tail = jnp.concatenate([block[16:, :256], block[16:, 256:]], axis=0)
            partial[layer, c, i] = jnp.concatenate([block[:16], tail], axis=1).astype(BF16)

    def send_group(layer, number):
        these = pl.ds(*groups[number])
        remote(
            partial.at[layer, other_core, these], near.at[layer, these],
            send_sem.at[1], near_recv.at[number], "dp", partner,
        )

    def halves_of(block):
        tail = jnp.concatenate([block[:8, piece:], block[8:, piece:]], axis=1)
        return block[:8, :piece], block[8:, :piece], tail

    def of_other_chip(block):
        zero, one, tail = halves_of(block)
        return fold(jnp.where(chip == 0, one, zero), tail, other_chip).astype(BF16)

    def of_this_chip(block):
        zero, one, tail = halves_of(block)
        return fold(jnp.where(chip == 0, zero, one), tail, chip)

    def chip_sum(layer, i):
        return partial[layer, core, i].astype(F32) + near[layer, i].astype(F32)

    def send_cross(layer, number):
        these = pl.ds(*groups[number])
        remote(
            cross.at[layer, these], far.at[layer, these],
            send_sem.at[1], far_recv.at[number], "dp", across,
        )

    def cross_squares(layer):
        await_bytes(sq_near.at[layer], sq_recv.at[0])
        chip_squares = sq_part[layer, core] + sq_near[layer]
        sq_part[layer, core] = chip_squares
        sq_cross[layer] = jnp.concatenate(
            [jnp.where(chip == 0, chip_squares[8:16], chip_squares[:8]), chip_squares[16:]], axis=0
        )
        remote(
            sq_cross.at[layer], sq_far.at[layer], send_sem.at[3], sq_recv.at[1], "dp", across
        )

    def first_of_core_0(layer):
        cross_squares(layer)
        begin, amount = groups[0]
        await_bytes(near.at[layer, pl.ds(begin, amount)], near_recv.at[0])
        for i in range(begin, begin + amount):
            cross[layer, i] = of_other_chip(chip_sum(layer, i))
        send_cross(layer, 0)
        for i in range(begin, begin + amount):
            direct[layer, i] = of_other_chip(partial[layer, 1, i].astype(F32))
        remote(
            direct.at[layer], far_direct.at[layer],
            send_sem.at[4], direct_recv, "dp", diagonal,
        )
        for i in range(begin, begin + amount):
            own[i] = of_this_chip(chip_sum(layer, i))

    def send_direct_of_core_1(layer):
        begin, amount = groups[0]
        for i in range(begin, begin + amount):
            cross[layer, i] = of_other_chip(partial[layer, 1, i].astype(F32))
        send_cross(layer, 0)

    def first_of_core_1(layer):
        cross_squares(layer)
        begin, amount = groups[0]
        await_bytes(near.at[layer, pl.ds(begin, amount)], near_recv.at[0])
        for i in range(begin, begin + amount):
            own[i] = of_this_chip(chip_sum(layer, i))

    def cross_group(layer, number):
        begin, amount = groups[number]
        await_bytes(near.at[layer, pl.ds(begin, amount)], near_recv.at[number])
        for i in range(begin, begin + amount):
            cross[layer, i] = of_other_chip(chip_sum(layer, i))
        send_cross(layer, number)
        for i in range(begin, begin + amount):
            own[i] = of_this_chip(chip_sum(layer, i))

    def split(block):
        high = block.astype(BF16).astype(F32)
        return [high, block - high]

    def columns_of(parts):
        return jnp.concatenate(parts, axis=0).T.astype(BF16)

    for p in range(mix_pieces):
        send_features(0, p)

    for layer in range(layers):
        squares = jnp.zeros((n_tp * rows, 128), F32)
        scaled = []
        first, count = groups[0]
        for p in range(mix_pieces):
            await_features(layer, p)
            widened = jnp.concatenate(
                [
                    stack_pair(
                        gathered[layer, p, c].astype(F32), gathered[layer, p, 2 + c].astype(F32)
                    )
                    for c in range(2)
                ],
                axis=0,
            )
            span = pl.ds(p * piece, piece)
            scaled.append((widened * gain[layer, span][None, :]).astype(BF16))
            for lane in range(0, piece, 128):
                tile = widened[:, lane : lane + 128]
                squares = squares + tile * tile
            if p == 0:
                await_bytes(proj.at[layer], proj_sem.at[layer])
            if p == mix_pieces - 1:
                for c in range(2):
                    sq_part[layer, c] = squares[24 * c : 24 * c + 24]
                remote(
                    sq_part.at[layer, other_core], sq_near.at[layer],
                    send_sem.at[1], sq_recv.at[0], "dp", partner,
                )
            for i in range(first, first + count):
                result = jnp.dot(scaled[p], proj[layer, i, span, :], preferred_element_type=F32)
                if p > 0:
                    result = result + product[i]
                if p < mix_pieces - 1:
                    product[i] = result
                else:
                    store_partial(layer, i, result)
        send_group(layer, 0)
        pl.when(core == 0)(functools.partial(first_of_core_0, layer))
        pl.when(core != 0)(functools.partial(send_direct_of_core_1, layer))
        whole_rows = jnp.concatenate(scaled, axis=1)
        for number in range(1, len(groups)):
            first, count = groups[number]
            for i in range(first, first + count):
                store_partial(
                    layer, i, jnp.dot(whole_rows, proj[layer, i], preferred_element_type=F32)
                )
            send_group(layer, number)
            pl.when(core == 0)(functools.partial(cross_group, layer, number))

        @pl.when(core != 0)
        def _():
            first_of_core_1(layer)
            for number in range(1, len(groups)):
                cross_group(layer, number)

        if layer + 1 < layers:
            pl.when(lender)(functools.partial(lend_residual, layer))
        await_bytes(sq_far.at[layer], sq_recv.at[1])
        chip_squares = sq_part[layer, core]
        last = chip_squares[16:] + sq_far[layer, pl.ds(8, 8), :]
        total_squares = jnp.concatenate(
            [
                jnp.where(chip == 0, chip_squares[:8], chip_squares[8:16])
                + sq_far[layer, pl.ds(0, 8), :],
                jnp.where(chip == 0, last, swap(last)),
            ],
            axis=0,
        )
        inverse = lax.rsqrt(jnp.sum(total_squares, axis=1, keepdims=True) / d_model + EPSILON)

        def projected(i):
            for number, (first, count) in enumerate(groups):
                if i == first:
                    await_bytes(far.at[layer, pl.ds(first, count)], far_recv.at[number])
            total = own[i] + far[layer, i].astype(F32)
            if i < groups[0][1]:
                total = total + far_direct[layer, i].astype(F32)
            return unfold_rows(total) * inverse

        if layer == 0:
            await_bytes(state, state_sem)

        @pl.when(core != 0)
        def _():
            await_bytes(far_direct.at[layer], direct_recv)

        logits = projected(0)
        log_sigmoid = jnp.minimum(logits, 0.0) - jnp.log(1.0 + jnp.exp(-jnp.abs(logits)))
        log_decay = log_sigmoid[:rows] / SOFTNESS + offset[:, layer, :]
        decay = jnp.exp(jnp.concatenate([log_decay, jnp.zeros((pad - rows, key_cols), F32)], axis=0))
        query = projected(1)
        read_columns = columns_of(split(query * decay))
        key = projected(2) * head_key ** (-0.5)
        both = query * key
        products = [
            jnp.sum(both[:, h * head_key : (h + 1) * head_key], axis=1, keepdims=True)
            for h in range(heads)
        ]

        for base in range(0, heads, half_heads):
            columns = read_columns[base * head_key : (base + half_heads) * head_key]
            for pair in range(rows // 2):
                factors = jnp.dot(
                    columns, expand[0, pair, pl.ds(0, 2 * pad), :], preferred_element_type=F32
                )
                for k in range(2):
                    b = 2 * pair + k
                    for hh in range(half_heads):
                        factor = factors[
                            hh * head_key : (hh + 1) * head_key,
                            k * value_channels : (k + 1) * value_channels,
                        ]
                        readout[base + hh, pl.ds(b, 1), :] = jnp.sum(
                            factor * state[layer, b, base + hh], axis=0, keepdims=True
                        )

        for half in range(halves):
            base = half * half_heads
            value = projected(3 + 2 * half)
            gate_all = projected(4 + 2 * half)
            values[:, pl.ds(half * piece, piece)] = value
            gated_heads = []
            for hh in range(half_heads):
                h = base + hh
                span = slice(hh * value_channels, (hh + 1) * value_channels)
                got = readout[h] + products[h] * value[:, span]
                gate = gate_all[:, span]
                normed = got * lax.rsqrt(jnp.mean(got * got, axis=1, keepdims=True) + EPSILON)
                whole = pl.ds(h * value_channels, value_channels)
                normed = normed * out_gain[layer, whole][None, :]
                gated_heads.append(normed * (gate / (1.0 + jnp.exp(-gate))))
            gated = jnp.concatenate(gated_heads, axis=1)
            gated_all[layer, half, dp] = fold(gated[:8], gated[8:], 0).astype(BF16)
            block = gated_all.at[layer, half, dp]
            remote(block, block, send_sem.at[1], gated_recv.at[half], "dp", across)
            remote(block, block, send_sem.at[1], gated_recv.at[half], "dp", diagonal)
            remote(block, block, send_sem.at[1], gated_recv.at[halves + half], "dp", partner)

        fresh_columns[...] = columns_of(split(key) + split(decay))
        first_pairs = rows // 4
        renew(layer, 0, first_pairs)

        if layer == 0:
            await_bytes(wo, wo_sem)
        project_out(layer, chip, halves, 1)
        if layer == layers - 1:
            send_last(layer, chip)
        project_out(layer, other_chip, 0, 2)
        if layer == layers - 1:
            send_last(layer, other_chip)
        renew(layer, first_pairs, rows // 2)

        await_feature_sends(layer)
        if layer + 1 < layers:

            @pl.when(lender)
            def _():
                await_bytes(lent.at[layer], send_sem.at[6])

        await_bytes(sq_far.at[layer], send_sem.at[3])
        await_bytes(partial.at[layer], send_sem.at[1])

        @pl.when(core == 0)
        def _():
            await_bytes(direct.at[layer], send_sem.at[4])


        if layer + 1 < layers:
            pl.when(is_owner)(functools.partial(finish_middle, layer))
        else:
            for p in range(mix_pieces):
                await_bytes(mix_last.at[p], mix_recv_sem.at[0, p, 0])
                total = mix_send[layer, p, tp].astype(F32)
                for j in range(n_tp - 1):
                    total = total + mix_last[p, j].astype(F32)
                result = (gathered[layer, p, tp].astype(F32) + total).astype(BF16)
                span = slice(p * piece, (p + 1) * piece)
                hidden_out_ref[:, span] = unfold_rows(result.astype(F32))[:rows].astype(BF16)
        await_mixed_sends(layer)


def store_kernel(hidden_ref, state_ref, hidden_out, state_out, hidden_sem, state_sem):
    layers, rows, heads = state_ref.shape[:3]
    for layer in range(layers):
        for b in range(rows):
            for half in range(2):
                part = (layer, b, pl.ds(half * (heads // 2), heads // 2))
                pltpu.make_async_copy(state_ref.at[part], state_out.at[part], state_sem).start()
    store_hidden = pltpu.make_async_copy(hidden_ref, hidden_out, hidden_sem)
    store_hidden.start()
    store_hidden.wait()
    pltpu.make_async_copy(state_ref, state_out, state_sem).wait()


def fused(
    n_tp, n_dp, hidden_in, input_norm_gain, w_query, w_key, w_decay, w_value, w_gate,
    out_gain, w_out, decay_offset, state,
):
    layers, rows, heads, head_key, value_channels = state.shape
    width = hidden_in.shape[1]
    key_cols, value_cols = w_query.shape[2], w_value.shape[2]
    piece = key_cols
    halves = value_cols // piece
    pieces = 3 + 2 * halves
    mix_pieces = width // piece
    block = (16, piece // 4 * 3)
    vmem = pl.BlockSpec(memory_space=pltpu.VMEM)
    hbm = pl.BlockSpec(memory_space=pl.ANY)
    offsets = decay_offset.transpose(1, 0, 2)
    hidden, fresh = pl.pallas_call(
        functools.partial(
            block_kernel, n_tp, n_dp, width * n_dp, head_key, value_channels, piece
        ),
        out_shape=(
            pltpu.VMEM(hidden_in.shape, BF16),
            pltpu.VMEM(state.shape, F32),
        ),
        in_specs=[hbm] * 11,
        out_specs=(vmem, vmem),
        scratch_shapes=[
            pltpu.VMEM(hidden_in.shape, BF16),
            pltpu.VMEM(input_norm_gain.shape, F32),
            pltpu.VMEM(out_gain.shape, F32),
            pltpu.VMEM(offsets.shape, F32),
            pltpu.VMEM((layers, pieces, width, piece), BF16),
            pltpu.VMEM(w_out.shape, BF16),
            pltpu.VMEM(state.shape, F32),
            pltpu.VMEM((layers, mix_pieces, n_tp) + block, BF16),
            pltpu.VMEM((3, n_tp * rows, piece), F32),
            pltpu.VMEM((layers, 2, pieces, 16, piece // 2 * 3), BF16),
            pltpu.VMEM((layers, pieces, 16, piece // 2 * 3), BF16),
            pltpu.VMEM((pieces,) + block, F32),
            pltpu.VMEM((layers, pieces) + block, BF16),
            pltpu.VMEM((layers, pieces) + block, BF16),
            pltpu.VMEM((layers, 3) + block, BF16),
            pltpu.VMEM((layers, 3) + block, BF16),
            pltpu.VMEM((layers, 2, 2 * rows, 128), F32),
            pltpu.VMEM((layers, 2 * rows, 128), F32),
            pltpu.VMEM((layers, 16, 128), F32),
            pltpu.VMEM((layers, 16, 128), F32),
            pltpu.VMEM((2, rows // 2, 64, 2 * value_channels), BF16),
            pltpu.VMEM((16, value_cols), F32),
            pltpu.VMEM((key_cols, 64), BF16),
            pltpu.VMEM((heads, 16, value_channels), F32),
            pltpu.VMEM((layers, halves, n_dp) + block, BF16),
            pltpu.VMEM((mix_pieces, 2 * rows, piece), F32),
            pltpu.VMEM((layers, mix_pieces, n_tp) + block, BF16),
            pltpu.VMEM((layers - 1, mix_pieces, 2, n_tp - 1) + block, BF16),
            pltpu.VMEM((layers - 1, mix_pieces, 2, n_tp) + block, BF16),
            pltpu.VMEM((mix_pieces, n_tp - 1) + block, BF16),
            pltpu.VMEM((layers - 1, mix_pieces, 2) + block, BF16),
            pltpu.VMEM((layers - 1, mix_pieces, 2) + block, BF16),
            pltpu.SemaphoreType.DMA((4,)),
            pltpu.SemaphoreType.DMA((layers,)),
            pltpu.SemaphoreType.DMA,
            pltpu.SemaphoreType.DMA,
            pltpu.SemaphoreType.DMA((mix_pieces,)),
            pltpu.SemaphoreType.DMA((1 + halves,)),
            pltpu.SemaphoreType.DMA((1 + halves,)),
            pltpu.SemaphoreType.DMA((2,)),
            pltpu.SemaphoreType.DMA((2 * halves,)),
            pltpu.SemaphoreType.DMA((2, mix_pieces, 2)),
            pltpu.SemaphoreType.DMA,
            pltpu.SemaphoreType.DMA,
            pltpu.SemaphoreType.DMA((7,)),
        ],
        compiler_params=pltpu.CompilerParams(
            collective_id=0, has_side_effects=True, vmem_limit_bytes=48 * 1024 * 1024
        ),
    )(
        hidden_in, input_norm_gain, out_gain, offsets,
        w_query, w_key, w_decay, w_value, w_gate, w_out, state,
    )
    return pl.pallas_call(
        store_kernel,
        out_shape=(
            jax.ShapeDtypeStruct(hidden_in.shape, BF16),
            jax.ShapeDtypeStruct(state.shape, F32),
        ),
        in_specs=[vmem] * 2,
        out_specs=(hbm, hbm),
        scratch_shapes=[
            pltpu.SemaphoreType.DMA,
            pltpu.SemaphoreType.DMA,
        ],
        compiler_params=pltpu.CompilerParams(vmem_limit_bytes=1024 * 1024),
    )(hidden, fresh)


def plain(
    hidden_in, input_norm_gain, w_query, w_key, w_decay, w_value, w_gate,
    out_gain, w_out, decay_offset, state,
):
    layers, rows, heads, head_key, value_channels = state.shape
    key_cols, value_cols = w_query.shape[2], w_value.shape[2]
    d_model = hidden_in.shape[1] * lax.axis_size("dp")
    first = lax.axis_index("dp") * rows
    current, states = hidden_in, []
    for layer in range(layers):
        widened = lax.all_gather(current, "tp", axis=0, tiled=True).astype(F32)
        squares = lax.psum(jnp.sum(widened * widened, axis=1), "dp")
        scaled = (widened * input_norm_gain[layer][None, :]).astype(BF16)
        partial = jnp.concatenate(
            [
                jnp.dot(scaled, matrix[layer], preferred_element_type=F32)
                for matrix in (w_query, w_key, w_decay, w_value, w_gate)
            ],
            axis=1,
        ).astype(BF16)
        summed = lax.psum_scatter(partial, "dp", scatter_dimension=0, tiled=True).astype(F32)
        own = lax.dynamic_slice_in_dim(squares, first, rows)
        projected = summed * lax.rsqrt(own / d_model + EPSILON)[:, None]
        query, key, logits, value, gate = jnp.split(
            projected,
            [key_cols, 2 * key_cols, 3 * key_cols, 3 * key_cols + value_cols],
            axis=1,
        )
        decay = jnp.exp(jax.nn.log_sigmoid(logits) / SOFTNESS + decay_offset[layer])
        per_key, per_value = (rows, heads, head_key), (rows, heads, value_channels)
        fresh = (
            decay.reshape(per_key)[..., None] * state[layer]
            + (key * head_key ** (-0.5)).reshape(per_key)[..., None]
            * value.reshape(per_value)[:, :, None, :]
        )
        got = jnp.sum(query.reshape(per_key)[..., None] * fresh, axis=2)
        got = got * lax.rsqrt(jnp.mean(got * got, axis=2, keepdims=True) + EPSILON)
        got = got * out_gain[layer].reshape(heads, value_channels)[None]
        gated = (got * jax.nn.silu(gate.reshape(per_value))).reshape(rows, value_cols).astype(BF16)
        mixed = jnp.dot(
            lax.all_gather(gated, "dp", axis=0, tiled=True), w_out[layer],
            preferred_element_type=F32,
        ).astype(BF16)
        mine = lax.psum_scatter(mixed, "tp", scatter_dimension=0, tiled=True).astype(F32)
        current = (current.astype(F32) + mine).astype(BF16)
        states.append(fresh)
    return current, jnp.stack(states)


def solution(mesh):
    n_tp, n_dp = mesh.shape["tp"], mesh.shape["dp"]

    def per_device(hidden_in, *rest):
        state = rest[-1]
        width, key_cols, value_cols = hidden_in.shape[1], rest[1].shape[2], rest[4].shape[2]
        layers, rows, heads = state.shape[:3]
        sized = key_cols == 512 and width % key_cols == 0 and value_cols % key_cols == 0
        shaped = hidden_in.shape[0] == rows == 12 and state.shape[4] == 128
        if n_tp == 4 and n_dp == 4 and layers > 1 and sized and shaped and heads % (value_cols // key_cols) == 0:
            return fused(n_tp, n_dp, hidden_in, *rest)
        return plain(hidden_in, *rest)

    return jax.shard_map(
        per_device,
        mesh=mesh,
        in_specs=(
            P(("grp", "tp"), "dp"),
            P(None, "dp"),
            P(None, "dp", "tp"),
            P(None, "dp", "tp"),
            P(None, "dp", "tp"),
            P(None, "dp", "tp"),
            P(None, "dp", "tp"),
            P(None, "tp"),
            P(None, "tp", "dp"),
            P(None, ("grp", "dp"), "tp"),
            P(None, ("grp", "dp"), "tp", None, None),
        ),
        out_specs=(P(("grp", "tp"), "dp"), P(None, ("grp", "dp"), "tp", None, None)),
        check_vma=False,
    )
```
